512 devices in a mesh: row: 64 (over z, y), col: 8 (over x, core).
Axes of the slice: x: 4, y: 8, z: 8, core: 2. Of those that a mesh axis runs over, the one named last changes fastest.
Arguments:
- tokens: bfloat16 [2, 8192, 2048], P(None, 'row'), may hold values from -6 to 6
- w_value: bfloat16 [2048, 1024], P(None, 'col'), may hold values from -0.125 to 0.125
- w_first: bfloat16 [2048, 1024], P(None, 'col'), may hold values from -0.125 to 0.125
- w_second: bfloat16 [2048, 1024], P(None, 'col'), may hold values from -0.125 to 0.125
- short_taps: float32 [3, 3, 1024], P(None, None, 'col'), may hold values from -3.5 to 3.5
- filter_in: float32 [33, 64], replicated, may hold values from -2 to 2
- filter_mid: float32 [64, 64], replicated, may hold values from -1.5 to 1.5
- filter_out: float32 [64, 2, 2, 1024], P(None, None, None, 'col'), may hold values from -0.75 to 0.75
- decay_rate: float32 [1024], P('col'), may hold values from 0 to 1, as said below
- skip_gain: float32 [2, 1024], P(None, 'col'), may hold values from -4 to 4
- w_output: bfloat16 [1024, 2048], P(None, 'col'), may hold values from -0.1875 to 0.1875
Outputs:
- mixed_out: bfloat16 [2, 8192, 2048], P(None, 'row', 'col')
The draws below stay inside these ranges and needn't reach their ends.
Inputs may be any that keep to these rules, and one draw needn't show every extreme that they name: `decay_rate`: Per-position decay rates of the channels' filters; all positive.
All inputs are finite; a program needn't handle non-finite values.
Results may differ from the reference program's by a relative error of at most 0.007.
Values may be sent and summed in bfloat16 or wider, within the bound.
No kernel may reach another device: no remote copies, remote signals or barrier semaphores. Data moves between devices by JAX's collectives and lax.ppermute only.
A program may use at most 64 MiB of HBM per device.

```python
import math
import jax
import jax.numpy as jnp
from jax import lax

WIDTH = 2048
CHANNELS = 1024
FEATS = 33
FILTER_UNITS = 64
SEQS = 2
LENGTH = 8192


def draw_decay_rate(key, part):
    base = jax.random.fold_in(key, 71)
    pick_key, slow_key, fast_key = jax.random.split(base, 3)
    slow_share = 0.5
    chooser = jax.random.uniform(pick_key, (CHANNELS,), jnp.float32)
    slow_log = jax.random.uniform(slow_key, (CHANNELS,), jnp.float32, jnp.log(0.05 / LENGTH), jnp.log(2.0 / LENGTH))
    fast_log = jax.random.uniform(fast_key, (CHANNELS,), jnp.float32, jnp.log(1.0 / 100.0), jnp.log(1.0 / 30.0))
    return jnp.where(chooser < slow_share, jnp.exp(slow_log), jnp.exp(fast_log)).astype(jnp.float32)


def shard_levels(key, shape, cuts, low, high):
    factor_of = 1.0
    for position, blocks in cuts:
        heights = jax.random.uniform(jax.random.fold_in(jax.random.fold_in(key, 6), position), (blocks,), jnp.float32, low / len(cuts), high / len(cuts))
        factor_of = factor_of * jnp.repeat(jnp.exp(heights), shape[position] // blocks).reshape((-1,) + (1,) * (len(shape) - 1 - position))
    return factor_of


def scatter_about(own_key, dims, scale, reach, cuts=(), kind=jnp.bfloat16):
    gain = shard_levels(own_key, dims, cuts, -0.22, 0.18) if cuts else 1.0
    result = jax.random.normal(own_key, dims, jnp.float32) * scale * gain
    return jnp.minimum(jnp.maximum(result, -reach), reach).astype(kind)


def setup_inputs(seed: int = 0) -> dict:
    key_of = jax.random.split(jax.random.key(seed), 12)
    return {
        "tokens": scatter_about(key_of[0], (SEQS, LENGTH, WIDTH), 1.0, 6.0, ((1, 64),)),
        "w_value": scatter_about(key_of[1], (WIDTH, CHANNELS), WIDTH ** -0.5, 0.125, ((1, 8),)),
        "w_first": scatter_about(key_of[2], (WIDTH, CHANNELS), WIDTH ** -0.5, 0.125, ((1, 8),)),
        "w_second": scatter_about(key_of[3], (WIDTH, CHANNELS), WIDTH ** -0.5, 0.125, ((1, 8),)),
        "short_taps": scatter_about(key_of[4], (3, 3, CHANNELS), 3 ** -0.5, 3.5, ((2, 8),), jnp.float32),
        "filter_in": jnp.clip(jax.random.uniform(key_of[5], (FEATS, FILTER_UNITS), jnp.float32, -2.0, 2.0), -2.0, 2.0),
        "filter_mid": jnp.clip(jax.random.uniform(key_of[6], (FILTER_UNITS, FILTER_UNITS), jnp.float32, -1.5, 1.5), -1.5, 1.5),
        "filter_out": scatter_about(key_of[7], (FILTER_UNITS, 2, 2, CHANNELS), FILTER_UNITS ** -0.5, 0.75, ((3, 8),), jnp.float32),
        "decay_rate": draw_decay_rate(jax.random.fold_in(key_of[11], 71), 0),
        "skip_gain": scatter_about(key_of[9], (2, CHANNELS), 1.0, 4.0, ((1, 8),), jnp.float32),
        "w_output": scatter_about(key_of[10], (CHANNELS, WIDTH), CHANNELS ** -0.5, 0.1875, ((1, 8),)),
    }


def position_features(length, band_count):
    lag_index = jnp.arange(length, dtype=jnp.float32)
    ramp_line = lag_index / (length - 1)
    omega_step = 2.0 * math.pi / length * lag_index
    band_freq = jnp.linspace(0.0001, band_count - 1, band_count, dtype=jnp.float32)
    angle = omega_step[:, None] * band_freq[None, :]
    return jnp.concatenate([ramp_line[:, None], jnp.cos(angle), -jnp.sin(angle)], axis=1)

def make_kernel(hidden, out_block, rate_block, length):
    shaped = jnp.einsum('lh,hsoc->solc', hidden, out_block, precision=lax.Precision.HIGHEST)
    lag_index = jnp.arange(length, dtype=jnp.float32)
    shaped = shaped * jnp.exp(-lag_index[:, None] * rate_block[None, :])
    ahead_half = shaped[0]
    behind_half = shaped[1]
    zero_col = jnp.zeros((2, 1, ahead_half.shape[2]), jnp.float32)
    kernel = jnp.concatenate([ahead_half, zero_col, behind_half[:, 1:][:, ::-1]], axis=1)
    return kernel * lax.rsqrt(lax.optimization_barrier(jnp.sum(kernel * kernel, axis=1, keepdims=True)) + 1e-06)

def one_sequence(tokens, w_value, w_first, w_second, short_taps, filter_in, filter_mid, filter_out, decay_rate, skip_gain, w_output):
    length = tokens.shape[0]
    channel_count = w_value.shape[1]
    stacked = jnp.stack([jnp.dot(tokens, weight, preferred_element_type=jnp.float32).astype(jnp.bfloat16) for weight in (w_value, w_first, w_second)])
    stacked = lax.optimization_barrier(stacked).astype(jnp.float32)
    padded = jnp.pad(stacked, ((0, 0), (1, 1), (0, 0)))
    smoothed = short_taps[0][:, None, :] * padded[:, :length] + short_taps[1][:, None, :] * padded[:, 1:length + 1] + short_taps[2][:, None, :] * padded[:, 2:]
    band_count = (filter_in.shape[0] - 1) // 2
    features = position_features(length, band_count)
    hidden = jnp.sin(jnp.dot(features, filter_in, precision=lax.Precision.HIGHEST))
    hidden = jnp.sin(jnp.dot(hidden, filter_mid, precision=lax.Precision.HIGHEST))
    block_count = channel_count // 128
    blocks_in = smoothed.reshape(3, length, block_count, 128).transpose(2, 0, 1, 3)
    out_blocks = filter_out.reshape(filter_out.shape[0], 2, 2, block_count, 128).transpose(3, 0, 1, 2, 4)
    rate_blocks = decay_rate.reshape(block_count, 128)
    gain_blocks = skip_gain.reshape(2, block_count, 128).transpose(1, 0, 2)

    def one_block(packed):
        parts, out_block, rate_block, gain_block = packed
        kernel = make_kernel(hidden, out_block, rate_block, length)
        spectrum = jnp.fft.rfft(kernel, axis=1)
        carried = parts[0]
        for order_idx in range(2):
            state_spec = jnp.fft.rfft(carried, n=2 * length, axis=0)
            reach_term = jnp.fft.irfft(state_spec * spectrum[order_idx], n=2 * length, axis=0)[:length]
            carried = parts[order_idx + 1] * (reach_term + gain_block[order_idx][None, :] * carried)
        return carried.astype(jnp.bfloat16)
    gated_blocks = lax.map(one_block, (blocks_in, out_blocks, rate_blocks, gain_blocks))
    gated_out = gated_blocks.transpose(1, 0, 2).reshape(length, channel_count)
    return jnp.dot(gated_out, w_output, preferred_element_type=jnp.float32).astype(jnp.bfloat16)

def reference(tokens, w_value, w_first, w_second, short_taps, filter_in, filter_mid, filter_out, decay_rate, skip_gain, w_output):

    def run_one(sequence):
        return one_sequence(sequence, w_value, w_first, w_second, short_taps, filter_in, filter_mid, filter_out, decay_rate, skip_gain, w_output)
    return lax.map(run_one, tokens)
```

```python
import functools
import math

import jax
import jax.numpy as jnp
import numpy as np
from jax import lax
from jax.experimental import pallas as pl
from jax.experimental.pallas import tpu as pltpu
from jax.sharding import Mesh
from jax.sharding import PartitionSpec as P

ROW = ("row_0", "row_1")
COL = ("x", "core")
SIDE = 128
HALF = SIDE // 2
BF = jnp.bfloat16
F32 = jnp.float32


def halves(table):
    table = np.asarray(table, np.float32)
    top = table.astype(jnp.bfloat16)
    return top, (table - top.astype(np.float32)).astype(jnp.bfloat16)


@functools.lru_cache(None)
def tables(length, feats):
    bands = (feats - 1) // 2
    lag = np.arange(length, dtype=np.float64)
    freq = np.linspace(0.0001, bands - 1, bands)
    angle = (2.0 * math.pi / length) * lag[None, :] * freq[:, None]
    features = np.concatenate(
        [lag[None, :] / (length - 1), np.cos(angle), -np.sin(angle), np.zeros((40 - feats, length))]
    )
    index = np.arange(SIDE)
    turn = 2.0 * math.pi / SIDE * (index[:, None] * index[None, :] % SIDE)
    cos, sin = np.cos(turn), np.sin(turn)
    fine = 2.0 * math.pi / (SIDE * SIDE) * (index[:, None] * index[None, :])
    real_in = np.concatenate([cos[:, :HALF], -sin[:, :HALF]])
    pair_in = np.block([[cos[:, :HALF], sin[:, :HALF]], [-sin[:, :HALF], cos[:, :HALF]]])
    right = np.block([[cos, -sin], [sin, cos]])
    split = {}
    split["real_in"] = halves(real_in)
    split["pair_in"] = halves(pair_in)
    split["pair_out"] = halves(pair_in.T)
    split["right"] = halves(right)
    split["back"] = halves(right.T)
    split["spec_re"] = halves(np.concatenate([cos, sin]))
    split["spec_im"] = halves(np.concatenate([-sin, cos]))
    return np.asarray(features, np.float32), np.stack([np.cos(fine), np.sin(fine)]).astype(
        np.float32
    ), split


def hi_lo(value):
    top = value.astype(BF)
    return top, (value - top.astype(F32)).astype(BF)


def mm(a, b, dims=(((1,), (0,)), ((), ()))):
    return lax.dot_general(a, b, dims, preferred_element_type=F32)


def left_const(const_hi, const_lo, value):
    top, low = hi_lo(value)
    return mm(const_hi, top) + mm(const_lo, top) + mm(const_hi, low)


def right_const(value, const_hi, const_lo):
    top, low = hi_lo(value)
    return mm(top, const_hi) + mm(low, const_hi) + mm(top, const_lo)


def sine_of_turns(turns):
    big = 12582912.0
    moved = turns - 0.25
    moved = moved - ((moved + big) - big)
    quarter = 0.25 - jnp.abs(moved)
    square = quarter * quarter
    poly = -70.98993302 * square + 81.34038614
    poly = poly * square - 41.33713041
    poly = poly * square + 6.28316395
    return poly * quarter


def filter_kernel(
    features_ref, in_ref, mid_ref, out_ref, rate_ref, fine_ref,
    real_hi, real_lo, re_hi, re_lo, im_hi, im_lo,
    spec_re_ref, spec_im_ref, rows_ref,
):
    length = features_ref.shape[1]
    device = lax.axis_index("row_0") * lax.axis_size("row_1") + lax.axis_index("row_1")
    lane = lax.broadcasted_iota(jnp.int32, (8, SIDE), 1)
    row = lax.broadcasted_iota(jnp.int32, (8, SIDE), 0)
    mine = lane == 2 * device + row % 2
    last = (((1,), (1,)), ((), ()))
    first = (((0,), (0,)), ((), ()))
    out_hi = jnp.zeros((8, out_ref.shape[0]), F32)
    out_lo = jnp.zeros((8, out_ref.shape[0]), F32)
    for pair in range(4):
        pick = jnp.where(mine & (row // 2 == pair), 1.0, 0.0).astype(BF)
        top, low = hi_lo(out_ref[:, pair * SIDE : (pair + 1) * SIDE])
        out_hi += mm(pick, top, last)
        out_lo += mm(pick, low, last)
    out_hi, out_lo = out_hi.astype(BF), out_lo.astype(BF)
    rate = jnp.sum(jnp.where(mine, rate_ref[...], 0.0), axis=1, keepdims=True)
    scale = 1.0 / (2.0 * math.pi)
    in_hi, in_lo = hi_lo(in_ref[...] * scale)
    mid_hi, mid_lo = hi_lo(mid_ref[...] * scale)
    out_all = jnp.concatenate([out_hi, out_lo, out_hi], axis=1)
    mid_all = jnp.concatenate([mid_hi, mid_lo, mid_hi], axis=1)
    chunk = 1024
    squares = jnp.zeros((8, SIDE), F32)
    sign = jnp.where(lax.broadcasted_iota(jnp.int32, (8, SIDE), 0) < 4, 1.0, -1.0)
    for start in range(0, length, chunk):
        top, low = hi_lo(features_ref[:, start : start + chunk])
        turns = mm(in_hi, top) + mm(in_lo, top) + mm(in_hi, low)
        top, low = hi_lo(sine_of_turns(turns))
        turns = mm(mid_all, jnp.concatenate([top, top, low], axis=0))
        top, low = hi_lo(sine_of_turns(turns))
        shaped = mm(out_all, jnp.concatenate([top, top, low], axis=0))
        for piece in range(chunk // SIDE):
            base = start + piece * SIDE
            lag = (lane + base).astype(F32)
            part = shaped[:, piece * SIDE : (piece + 1) * SIDE] * jnp.exp(-rate * lag)
            if base == 0:
                part = jnp.where((row >= 4) & (lane == 0), 0.0, part)
            squares += part * part
            other = pltpu.roll(part, 4, 0)
            rows_ref[base // SIDE] = other + part * sign
    total = jnp.sum(squares + pltpu.roll(squares, 4, 0), axis=1, keepdims=True)
    factor = lax.rsqrt(total + 1e-06) * (1.0 / (SIDE * SIDE))
    grid = jnp.concatenate([rows_ref[:, j, :] * factor[j : j + 1, :] for j in range(8)], axis=1)
    grid = left_const(real_hi[...], real_lo[...], grid)
    cos, sin = fine_ref[0], fine_ref[1]

    def turned(j):
        real = grid[:SIDE, j * SIDE : (j + 1) * SIDE]
        imag = grid[SIDE:, j * SIDE : (j + 1) * SIDE]
        return jnp.concatenate([real * cos + imag * sin, imag * cos - real * sin], axis=1)

    for order in range(2):
        for channel in range(2):
            j = order * 2 + channel
            rows = pl.ds(channel * SIDE, SIDE)
            spec_re_ref[order, rows, :] = right_const(turned(j), re_hi[...], re_lo[...])
            spec_im_ref[order, rows, :] = right_const(turned(j + 4), im_hi[...], im_lo[...])


def conv_kernel(
    x_ref, taps_ref, gain_ref, spec_re_ref, spec_im_ref, fine_ref,
    in_hi, in_lo, out_hi, out_lo, right_hi, right_lo, back_hi, back_lo,
    o_ref, wide_ref, rows_ref,
):
    device = lax.axis_index("row_0") * lax.axis_size("row_1") + lax.axis_index("row_1")
    wide_ref[...] = x_ref[...].astype(F32)
    row = lax.broadcasted_iota(jnp.int32, (HALF, SIDE), 0)
    lane = lax.broadcasted_iota(jnp.int32, (HALF, SIDE), 1)

    def smoothed(p):
        seqs = []
        for s in range(2):
            chans = []
            for c in range(2):
                here = wide_ref[:, (p * 2 + s) * 2 + c, :]
                moved = pltpu.roll(here, 1, 1)
                prev = jnp.where(lane == 0, pltpu.roll(moved, 1, 0), moved)
                prev = jnp.where((lane == 0) & (row == 0), 0.0, prev)
                moved = pltpu.roll(here, SIDE - 1, 1)
                after = jnp.where(lane == SIDE - 1, pltpu.roll(moved, HALF - 1, 0), moved)
                after = jnp.where((lane == SIDE - 1) & (row == HALF - 1), 0.0, after)
                at = 2 * device + c
                chans.append(
                    taps_ref[p, at] * prev + taps_ref[3 + p, at] * here + taps_ref[6 + p, at] * after
                )
            seqs.append(jnp.concatenate(chans, axis=1))
        return jnp.concatenate(seqs, axis=0)

    cos, sin = fine_ref[0], fine_ref[1]
    cos2, sin2 = jnp.concatenate([cos, cos], axis=1), jnp.concatenate([sin, sin], axis=1)
    lane2 = lax.broadcasted_iota(jnp.int32, (1, 2 * SIDE), 1)
    state = smoothed(0)
    for order in range(2):
        grid = left_const(in_hi[...], in_lo[...], state)
        real, imag = grid[:SIDE], grid[SIDE:]
        real, imag = real * cos2 + imag * sin2, imag * cos2 - real * sin2
        grid = jnp.concatenate(
            [
                jnp.concatenate([real[:, :SIDE], imag[:, :SIDE]], axis=1),
                jnp.concatenate([real[:, SIDE:], imag[:, SIDE:]], axis=1),
            ],
            axis=0,
        )
        grid = right_const(grid, right_hi[...], right_lo[...])
        real, imag = grid[:, :SIDE], grid[:, SIDE:]
        k_re, k_im = spec_re_ref[order], spec_im_ref[order]
        grid = jnp.concatenate([real * k_re - imag * k_im, real * k_im + imag * k_re], axis=1)
        grid = right_const(grid, back_hi[...], back_lo[...])
        real = jnp.concatenate([grid[:SIDE, :SIDE], grid[SIDE:, :SIDE]], axis=1)
        imag = jnp.concatenate([grid[:SIDE, SIDE:], grid[SIDE:, SIDE:]], axis=1)
        grid = jnp.concatenate([real * cos2 - imag * sin2, real * sin2 + imag * cos2], axis=0)
        reach = left_const(out_hi[...], out_lo[...], grid)
        gain = jnp.where(lane2 < SIDE, gain_ref[order, 2 * device], gain_ref[order, 2 * device + 1])
        state = smoothed(order + 1) * (reach + gain * state)
    for s in range(2):
        for c in range(2):
            rows_ref[s, pl.ds(c, HALF, stride=2), :] = state[
                s * HALF : (s + 1) * HALF, c * SIDE : (c + 1) * SIDE
            ]
        o_ref[:, pl.ds(s * SIDE, SIDE)] = rows_ref[s].astype(BF)


def on_device(
    tokens,
    w_value,
    w_first,
    w_second,
    short_taps,
    filter_in,
    filter_mid,
    filter_out,
    decay_rate,
    skip_gain,
    w_output,
):
    seqs, tok_rows, _ = tokens.shape
    blocks = lax.axis_size(ROW)
    length = tok_rows * blocks
    feats = filter_in.shape[0]
    features, fine, split = tables(length, feats)
    projected = jnp.stack(
        [
            jnp.einsum("std,dc->sct", tokens, weight, preferred_element_type=F32).astype(BF)
            for weight in (w_value, w_first, w_second)
        ]
    )
    pieces = projected.reshape(3, seqs, blocks, 2, tok_rows).transpose(2, 0, 1, 3, 4)
    pieces = pieces.reshape(blocks, 12, tok_rows)
    arrived = lax.all_to_all(pieces, ROW, 0, 0, tiled=True)

    vmem = pl.BlockSpec(memory_space=pltpu.VMEM)
    smem = pl.BlockSpec(memory_space=pltpu.SMEM)
    fine = jnp.asarray(fine)
    spec = jax.ShapeDtypeStruct((2, 2 * SIDE, SIDE), F32)
    const = {k: tuple(jnp.asarray(h) for h in v) for k, v in split.items()}
    spec_re, spec_im = pl.pallas_call(
        filter_kernel,
        out_shape=(spec, spec),
        in_specs=[vmem] * 12,
        out_specs=(vmem, vmem),
        scratch_shapes=[pltpu.VMEM((HALF, 8, SIDE), F32)],
        cost_estimate=pl.CostEstimate(
            flops=4_000_000_000, bytes_accessed=3_000_000, transcendentals=0
        ),
        name="filter_spectra",
    )(
        jnp.asarray(features),
        jnp.pad(filter_in.T, ((0, 0), (0, 40 - feats))),
        filter_mid.T,
        filter_out.reshape(filter_out.shape[0], -1),
        decay_rate.reshape(1, -1),
        fine,
        *const["real_in"],
        *const["spec_re"],
        *const["spec_im"],
    )
    gated = pl.pallas_call(
        conv_kernel,
        out_shape=jax.ShapeDtypeStruct((2 * blocks, seqs * tok_rows), BF),
        in_specs=[vmem, smem, smem] + [vmem] * 11,
        out_specs=vmem,
        scratch_shapes=[
            pltpu.VMEM((HALF, 12, SIDE), F32),
            pltpu.VMEM((2, SIDE, SIDE), F32),
        ],
        cost_estimate=pl.CostEstimate(
            flops=4_000_000_000, bytes_accessed=2_000_000, transcendentals=0
        ),
        name="gated_conv",
    )(
        arrived,
        short_taps.reshape(9, -1),
        skip_gain,
        spec_re,
        spec_im,
        fine,
        *const["pair_in"],
        *const["pair_out"],
        *const["right"],
        *const["back"],
    )
    returned = lax.all_to_all(gated, ROW, 0, 0, tiled=True)
    everyone = lax.all_to_all(
        jnp.broadcast_to(returned[None], (lax.axis_size("x"), *returned.shape)), "x", 0, 0, tiled=True
    )
    everyone = lax.all_gather(everyone, "core", axis=1)
    everyone = everyone.reshape(-1, seqs * tok_rows)
    result = jnp.einsum("ct,cd->td", everyone, w_output, preferred_element_type=F32)
    return result.astype(BF).reshape(seqs, tok_rows, -1)


def solution(mesh):
    torus = Mesh(mesh.devices.reshape(8, 8, 4, 2), ("row_0", "row_1", "x", "core"))
    in_specs = (
        P(None, ROW, None),
        P(None, COL),
        P(None, COL),
        P(None, COL),
        P(None, None, COL),
        P(),
        P(),
        P(None, None, None, COL),
        P(COL),
        P(None, COL),
        P(None, COL),
    )
    out_specs = P(None, ROW, COL)
    return jax.shard_map(
        on_device, mesh=torus, in_specs=in_specs, out_specs=out_specs, check_vma=False
    )
```

```python
import functools
import math

import jax
import jax.numpy as jnp
import numpy as np
from jax import lax
from jax.experimental import pallas as pl
from jax.experimental.pallas import tpu as pltpu
from jax.sharding import Mesh
from jax.sharding import PartitionSpec as P

ROW = ("row_0", "row_1")
COL = ("x", "core")
SIDE = 128
HALF = SIDE // 2
BF = jnp.bfloat16
F32 = jnp.float32


def halves(table):
    table = np.asarray(table, np.float32)
    top = table.astype(jnp.bfloat16)
    return top, (table - top.astype(np.float32)).astype(jnp.bfloat16)


@functools.lru_cache(None)
def tables(length, feats):
    bands = (feats - 1) // 2
    freq = np.linspace(0.0001, bands - 1, bands)[:, None] * (2.0 * math.pi / length)
    coarse, near = freq * np.arange(SIDE) * SIDE, freq * np.arange(SIDE)
    waves = np.stack([np.cos(coarse), np.sin(coarse), np.cos(near), np.sin(near)])
    index = np.arange(SIDE)
    turn = 2.0 * math.pi / SIDE * (index[:, None] * index[None, :] % SIDE)
    cos, sin = np.cos(turn), np.sin(turn)
    fine = 2.0 * math.pi / (SIDE * SIDE) * (index[:, None] * index[None, :])
    pair_in = np.block([[cos[:, :HALF], sin[:, :HALF]], [-sin[:, :HALF], cos[:, :HALF]]])
    right = np.block([[cos, -sin], [sin, cos]])
    split = {}
    split["pair_in"] = halves(pair_in)
    split["pair_out"] = halves(pair_in.T)
    split["right"] = halves(right)
    split["back"] = halves(right.T)
    fine = np.stack([np.cos(fine), np.sin(fine)])
    return waves.astype(np.float32), fine.astype(np.float32), split


def hi_lo(value):
    top = value.astype(BF)
    return top, (value - top.astype(F32)).astype(BF)


def mm(a, b, dims=(((1,), (0,)), ((), ()))):
    return lax.dot_general(a, b, dims, preferred_element_type=F32)


def left_const(const_hi, const_lo, value):
    top, low = hi_lo(value)
    return mm(const_hi, top) + mm(const_lo, top) + mm(const_hi, low)


def right_const(value, const_hi, const_lo):
    top, low = hi_lo(value)
    return mm(top, const_hi) + mm(low, const_hi) + mm(top, const_lo)


def sine_of_turns(turns):
    big = 12582912.0
    moved = turns - 0.25
    moved = moved - ((moved + big) - big)
    quarter = 0.25 - jnp.abs(moved)
    square = quarter * quarter
    poly = -70.98993302 * square + 81.34038614
    poly = poly * square - 41.33713041
    poly = poly * square + 6.28316395
    return poly * quarter


def project_kernel(steps, tok_hbm, a_hbm, b_hbm, c_hbm, o_ref, tok, weights, flat_ref, wide_ref, sems):
    depth = tok.shape[2] // steps
    copies = []
    for step in range(steps):
        cut = pl.ds(step * depth, depth)
        group = [pltpu.make_async_copy(tok_hbm.at[:, :, cut], tok.at[:, :, cut], sems.at[step, 3])]
        for p, source in enumerate((a_hbm, b_hbm, c_hbm)):
            group.append(
                pltpu.make_async_copy(source.at[cut, :], weights.at[p, cut, :], sems.at[step, p])
            )
        for copy in group:
            copy.start()
        copies.append(group)
    sums = [[None] * 3, [None] * 3]
    for step in range(steps):
        for copy in copies[step]:
            copy.wait()
        cut = slice(step * depth, (step + 1) * depth)
        for s in range(2):
            for p in range(3):
                part = mm(tok[s, :, cut], weights[p, cut, :])
                sums[s][p] = part if step == 0 else sums[s][p] + part
    for s in range(2):
        for p in range(3):
            flat_ref[s * 3 + p] = sums[s][p].T
            for c in range(2):
                wide_ref[:, (p * 2 + s) * 2 + c, :] = flat_ref[s * 3 + p, pl.ds(c, HALF, stride=2), :]
    o_ref[...] = wide_ref[...].astype(BF)


def filter_kernel(
    waves_ref, in_ref, mid_ref, out_ref, rate_ref, fine_ref,
    in_hi_ref, in_lo_ref, right_hi, right_lo,
    spec_re_ref, spec_im_ref, rows_ref, pad_ref,
):
    length = HALF * SIDE
    device = lax.axis_index("row_0") * lax.axis_size("row_1") + lax.axis_index("row_1")
    lane = lax.broadcasted_iota(jnp.int32, (8, SIDE), 1)
    row = lax.broadcasted_iota(jnp.int32, (8, SIDE), 0)
    mine = lane == 2 * device + row % 2
    last = (((1,), (1,)), ((), ()))
    first = (((0,), (0,)), ((), ()))
    out_hi = jnp.zeros((8, out_ref.shape[0]), F32)
    out_lo = jnp.zeros((8, out_ref.shape[0]), F32)
    for pair in range(4):
        pick = jnp.where(mine & (row // 2 == pair), 1.0, 0.0).astype(BF)
        top, low = hi_lo(out_ref[:, pair // 2, pair % 2, :])
        out_hi += mm(pick, top, last)
        out_lo += mm(pick, low, last)
    out_hi, out_lo = out_hi.astype(BF), out_lo.astype(BF)
    rate = jnp.sum(jnp.where(mine, rate_ref[...], 0.0), axis=1, keepdims=True)
    scale = 1.0 / (2.0 * math.pi)
    pad_ref[...] = jnp.zeros_like(pad_ref)
    pad_ref[:32, :] = in_ref[1:33, :] * scale
    pad_ref[32:33, :] = in_ref[0:1, :] * scale
    in_hi, in_lo = hi_lo(pad_ref[...])
    in_all = jnp.concatenate([in_hi, in_lo, in_hi], axis=0)
    mid_hi, mid_lo = hi_lo(mid_ref[...] * scale)
    out_all = jnp.concatenate([out_hi, out_lo, out_hi], axis=1)
    mid_all = jnp.concatenate([mid_hi, mid_lo, mid_hi], axis=0)
    chunk = 1024
    cos_near, sin_near = waves_ref[2], waves_ref[3]
    wide_lane = lax.broadcasted_iota(jnp.int32, (16, SIDE), 1)
    top_row = lax.broadcasted_iota(jnp.int32, (16, SIDE), 0) == 0
    ramp_step = 1.0 / (length - 1)

    def features(block):
        cos_far = waves_ref[0, :, block : block + 1]
        sin_far = waves_ref[1, :, block : block + 1]
        ramp = jnp.where(top_row, (wide_lane + block * SIDE).astype(F32) * ramp_step, 0.0)
        return jnp.concatenate(
            [
                cos_far * cos_near - sin_far * sin_near,
                -(sin_far * cos_near + cos_far * sin_near),
                ramp,
            ],
            axis=0,
        )

    squares = jnp.zeros((8, SIDE), F32)
    sign = jnp.where(lax.broadcasted_iota(jnp.int32, (8, SIDE), 0) < 4, 1.0, -1.0)
    for start in range(0, length, chunk):
        top, low = hi_lo(
            jnp.concatenate(
                [features(b) for b in range(start // SIDE, (start + chunk) // SIDE)], axis=1
            )
        )
        turns = mm(in_all, jnp.concatenate([top, top, low], axis=0), first)
        top, low = hi_lo(sine_of_turns(turns))
        turns = mm(mid_all, jnp.concatenate([top, top, low], axis=0), first)
        top, low = hi_lo(sine_of_turns(turns))
        shaped = mm(out_all, jnp.concatenate([top, top, low], axis=0))
        for piece in range(chunk // SIDE):
            base = start + piece * SIDE
            lag = (lane + base).astype(F32)
            part = shaped[:, piece * SIDE : (piece + 1) * SIDE] * jnp.exp(-rate * lag)
            if base == 0:
                part = jnp.where((row >= 4) & (lane == 0), 0.0, part)
            squares += part * part
            other = pltpu.roll(part, 4, 0)
            rows_ref[base // SIDE] = other + part * sign
    total = jnp.sum(squares + pltpu.roll(squares, 4, 0), axis=1, keepdims=True)
    factor = lax.rsqrt(total + 1e-06) * (1.0 / (SIDE * SIDE))
    grid = jnp.concatenate([rows_ref[:, j, :] * factor[j : j + 1, :] for j in range(8)], axis=1)
    grid = left_const(in_hi_ref[:, :HALF], in_lo_ref[:, :HALF], grid)
    cos, sin = fine_ref[0], fine_ref[1]

    def turned(j):
        real = grid[:SIDE, j * SIDE : (j + 1) * SIDE]
        imag = grid[SIDE:, j * SIDE : (j + 1) * SIDE]
        return jnp.concatenate([real * cos + imag * sin, imag * cos - real * sin], axis=1)

    for order in range(2):
        for channel in range(2):
            j = order * 2 + channel
            rows = pl.ds(channel * SIDE, SIDE)
            spec_re_ref[order, rows, :] = right_const(
                turned(j), right_hi[:, :SIDE], right_lo[:, :SIDE]
            )
            spec_im_ref[order, rows, :] = right_const(
                turned(j + 4), right_hi[:, SIDE:], right_lo[:, SIDE:]
            )


def conv_kernel(
    x_ref, taps_ref, gain_ref, spec_re_ref, spec_im_ref, fine_ref,
    in_hi, in_lo, out_hi, out_lo, right_hi, right_lo, back_hi, back_lo,
    o_ref, wide_ref, rows_ref,
):
    device = lax.axis_index("row_0") * lax.axis_size("row_1") + lax.axis_index("row_1")
    wide_ref[...] = x_ref[...].astype(F32)
    row = lax.broadcasted_iota(jnp.int32, (HALF, SIDE), 0)
    lane = lax.broadcasted_iota(jnp.int32, (HALF, SIDE), 1)

    def smoothed(p):
        seqs = []
        for s in range(2):
            chans = []
            for c in range(2):
                here = wide_ref[:, (p * 2 + s) * 2 + c, :]
                moved = pltpu.roll(here, 1, 1)
                prev = jnp.where(lane == 0, pltpu.roll(moved, 1, 0), moved)
                prev = jnp.where((lane == 0) & (row == 0), 0.0, prev)
                moved = pltpu.roll(here, SIDE - 1, 1)
                after = jnp.where(lane == SIDE - 1, pltpu.roll(moved, HALF - 1, 0), moved)
                after = jnp.where((lane == SIDE - 1) & (row == HALF - 1), 0.0, after)
                at = 2 * device + c
                chans.append(
                    taps_ref[0, p, at] * prev + taps_ref[1, p, at] * here + taps_ref[2, p, at] * after
                )
            seqs.append(jnp.concatenate(chans, axis=1))
        return jnp.concatenate(seqs, axis=0)

    cos, sin = fine_ref[0], fine_ref[1]
    cos2, sin2 = jnp.concatenate([cos, cos], axis=1), jnp.concatenate([sin, sin], axis=1)
    lane2 = lax.broadcasted_iota(jnp.int32, (1, 2 * SIDE), 1)
    state = smoothed(0)
    for order in range(2):
        grid = left_const(in_hi[...], in_lo[...], state)
        real, imag = grid[:SIDE], grid[SIDE:]
        real, imag = real * cos2 + imag * sin2, imag * cos2 - real * sin2
        grid = jnp.concatenate(
            [
                jnp.concatenate([real[:, :SIDE], imag[:, :SIDE]], axis=1),
                jnp.concatenate([real[:, SIDE:], imag[:, SIDE:]], axis=1),
            ],
            axis=0,
        )
        grid = right_const(grid, right_hi[...], right_lo[...])
        real, imag = grid[:, :SIDE], grid[:, SIDE:]
        k_re, k_im = spec_re_ref[order], spec_im_ref[order]
        grid = jnp.concatenate([real * k_re - imag * k_im, real * k_im + imag * k_re], axis=1)
        grid = right_const(grid, back_hi[...], back_lo[...])
        real = jnp.concatenate([grid[:SIDE, :SIDE], grid[SIDE:, :SIDE]], axis=1)
        imag = jnp.concatenate([grid[:SIDE, SIDE:], grid[SIDE:, SIDE:]], axis=1)
        grid = jnp.concatenate([real * cos2 - imag * sin2, real * sin2 + imag * cos2], axis=0)
        reach = left_const(out_hi[...], out_lo[...], grid)
        gain = jnp.where(lane2 < SIDE, gain_ref[order, 2 * device], gain_ref[order, 2 * device + 1])
        state = smoothed(order + 1) * (reach + gain * state)
    for s in range(2):
        for c in range(2):
            rows_ref[:, c, pl.ds(s * SIDE, SIDE)] = state[
                s * HALF : (s + 1) * HALF, c * SIDE : (c + 1) * SIDE
            ]
    o_ref[...] = rows_ref[...].astype(BF)


def on_device(
    tokens,
    w_value,
    w_first,
    w_second,
    short_taps,
    filter_in,
    filter_mid,
    filter_out,
    decay_rate,
    skip_gain,
    w_output,
):
    seqs, tok_rows, _ = tokens.shape
    blocks = lax.axis_size(ROW)
    length = tok_rows * blocks
    feats = filter_in.shape[0]
    waves, fine, split = tables(length, feats)
    far = pl.BlockSpec(memory_space=pltpu.HBM)
    vmem = pl.BlockSpec(memory_space=pltpu.VMEM)
    smem = pl.BlockSpec(memory_space=pltpu.SMEM)
    steps = 4
    pieces = pl.pallas_call(
        functools.partial(project_kernel, steps),
        out_shape=jax.ShapeDtypeStruct((blocks, 12, tok_rows), BF),
        in_specs=[far] * 4,
        out_specs=vmem,
        scratch_shapes=[
            pltpu.VMEM(tokens.shape, BF),
            pltpu.VMEM((3, *w_value.shape), BF),
            pltpu.VMEM((6, SIDE, SIDE), F32),
            pltpu.VMEM((HALF, 12, SIDE), F32),
            pltpu.SemaphoreType.DMA((steps, 4)),
        ],
        compiler_params=pltpu.CompilerParams(vmem_limit_bytes=66_700_000),
        name="project",
    )(tokens, w_value, w_first, w_second)
    arrived = lax.all_to_all(pieces, ROW, 0, 0, tiled=True)

    fine = jnp.asarray(fine)
    spec = jax.ShapeDtypeStruct((2, 2 * SIDE, SIDE), F32)
    const = {k: tuple(jnp.asarray(h) for h in v) for k, v in split.items()}
    spec_re, spec_im = pl.pallas_call(
        filter_kernel,
        out_shape=(spec, spec),
        in_specs=[vmem] * 10,
        out_specs=(vmem, vmem),
        scratch_shapes=[
            pltpu.VMEM((HALF, 8, SIDE), F32),
            pltpu.VMEM((48, filter_in.shape[1]), F32),
        ],
        compiler_params=pltpu.CompilerParams(vmem_limit_bytes=16 * 2**20),
        cost_estimate=pl.CostEstimate(
            flops=4_000_000_000, bytes_accessed=3_000_000, transcendentals=0
        ),
        name="filter_spectra",
    )(
        jnp.asarray(waves),
        filter_in,
        filter_mid,
        filter_out,
        decay_rate.reshape(1, -1),
        fine,
        *const["pair_in"],
        *const["right"],
    )
    gated = pl.pallas_call(
        conv_kernel,
        out_shape=jax.ShapeDtypeStruct((blocks, 2, seqs * tok_rows), BF),
        in_specs=[vmem, smem, smem] + [vmem] * 11,
        out_specs=vmem,
        scratch_shapes=[
            pltpu.VMEM((HALF, 12, SIDE), F32),
            pltpu.VMEM((HALF, 2, 2 * SIDE), F32),
        ],
        compiler_params=pltpu.CompilerParams(vmem_limit_bytes=16 * 2**20),
        cost_estimate=pl.CostEstimate(
            flops=4_000_000_000, bytes_accessed=2_000_000, transcendentals=0
        ),
        name="gated_conv",
    )(
        arrived,
        short_taps,
        skip_gain,
        spec_re,
        spec_im,
        fine,
        *const["pair_in"],
        *const["pair_out"],
        *const["right"],
        *const["back"],
    )
    returned = lax.all_to_all(gated, ROW, 0, 0, tiled=True)
    returned = returned.reshape(2 * blocks, seqs * tok_rows)
    everyone = lax.all_to_all(
        jnp.broadcast_to(returned[None], (lax.axis_size("x"), *returned.shape)), "x", 0, 0, tiled=True
    )
    everyone = lax.all_gather(everyone, "core", axis=1)
    everyone = everyone.reshape(-1, seqs * tok_rows)
    result = jnp.einsum("ct,cd->td", everyone, w_output, preferred_element_type=F32)
    return result.astype(BF).reshape(seqs, tok_rows, -1)


def solution(mesh):
    torus = Mesh(mesh.devices.reshape(8, 8, 4, 2), ("row_0", "row_1", "x", "core"))
    in_specs = (
        P(None, ROW, None),
        P(None, COL),
        P(None, COL),
        P(None, COL),
        P(None, None, COL),
        P(),
        P(),
        P(None, None, None, COL),
        P(COL),
        P(None, COL),
        P(None, COL),
    )
    out_specs = P(None, ROW, COL)
    return jax.shard_map(
        on_device, mesh=torus, in_specs=in_specs, out_specs=out_specs, check_vma=False
    )
```

```python
import functools
import math

import jax
import jax.numpy as jnp
import numpy as np
from jax import lax
from jax.experimental import pallas as pl
from jax.experimental.pallas import tpu as pltpu
from jax.sharding import Mesh
from jax.sharding import PartitionSpec as P

ROW = ("row_0", "row_1")
COL = ("x", "core")
SIDE = 128
HALF = SIDE // 2
MAPS_FIRST = 6 * SIDE
BF = jnp.bfloat16
F32 = jnp.float32


def halves(table):
    table = np.asarray(table, np.float32)
    top = table.astype(jnp.bfloat16)
    return top, (table - top.astype(np.float32)).astype(jnp.bfloat16)


@functools.lru_cache(None)
def tables(length, feats):
    bands = (feats - 1) // 2
    freq = np.linspace(0.0001, bands - 1, bands)[:, None] * (2.0 * math.pi / length)
    coarse, near = freq * np.arange(SIDE) * SIDE, freq * np.arange(SIDE)
    waves = np.stack([np.cos(coarse), np.sin(coarse), np.cos(near), np.sin(near)])
    index = np.arange(SIDE)
    turn = 2.0 * math.pi / SIDE * (index[:, None] * index[None, :] % SIDE)
    cos, sin = np.cos(turn), np.sin(turn)
    fine = 2.0 * math.pi / (SIDE * SIDE) * (index[:, None] * index[None, :])
    pair_in = np.block([[cos[:, :HALF], sin[:, :HALF]], [-sin[:, :HALF], cos[:, :HALF]]])
    right = np.block([[cos, -sin], [sin, cos]])
    in_hi, in_lo = halves(pair_in)
    out_hi, out_lo = halves(pair_in.T)
    right_hi, right_lo = halves(right)
    back_hi, back_lo = halves(right.T)
    maps = np.concatenate(
        [right_hi, right_lo, np.concatenate([in_hi, in_lo], axis=1), back_hi, back_lo, out_hi, out_lo]
    )
    angles = np.concatenate([np.cos(fine), np.sin(fine), *waves]).astype(np.float32)
    return angles, maps[:MAPS_FIRST], maps[MAPS_FIRST:]


def hi_lo(value):
    top = value.astype(BF)
    return top, (value - top.astype(F32)).astype(BF)


def mm(a, b, dims=(((1,), (0,)), ((), ()))):
    return lax.dot_general(a, b, dims, preferred_element_type=F32)


def left_const(const_hi, const_lo, value):
    top, low = hi_lo(value)
    return mm(const_hi, top) + mm(const_lo, top) + mm(const_hi, low)


def right_const(value, const_hi, const_lo):
    top, low = hi_lo(value)
    return mm(top, const_hi) + mm(low, const_hi) + mm(top, const_lo)


def sine_of_turns(turns):
    big = 12582912.0
    moved = turns - 0.25
    moved = moved - ((moved + big) - big)
    quarter = 0.25 - jnp.abs(moved)
    square = quarter * quarter
    poly = -70.98993302 * square + 81.34038614
    poly = poly * square - 41.33713041
    poly = poly * square + 6.28316395
    return poly * quarter


def project_kernel(
    steps, tok_hbm, a_hbm, b_hbm, c_hbm, o_ref, tok, weights, sum_ref, flat_ref, wide_ref, sems
):
    depth = tok.shape[1] // steps

    def group_of(step, cut):
        group = []
        for s in range(2):
            group.append((tok_hbm.at[s, :, cut], tok.at[pl.ds(s * SIDE, SIDE), cut]))
        for p, source in enumerate((a_hbm, b_hbm, c_hbm)):
            group.append((source.at[cut, :], weights.at[cut, pl.ds(p * SIDE, SIDE)]))
        return [
            pltpu.make_async_copy(near, far, sems.at[step, k]) for k, (near, far) in enumerate(group)
        ]

    for step in range(steps):
        for copy in group_of(step, pl.ds(step * depth, depth)):
            copy.start()
    sum_ref[...] = jnp.zeros_like(sum_ref)

    @pl.loop(0, steps)
    def _(step):
        cut = pl.ds(pl.multiple_of(step * depth, depth), depth)
        for copy in group_of(step, cut):
            copy.wait()
        sum_ref[...] += mm(tok[:, cut], weights[cut, :])

    @pl.loop(0, 3)
    def _(p):
        cut = pl.ds(pl.multiple_of(p * SIDE, SIDE), SIDE)
        for s in range(2):
            flat_ref[s] = sum_ref[s * SIDE : (s + 1) * SIDE, cut].T
            for c in range(2):
                wide_ref[:, s * 2 + c, :] = flat_ref[s, pl.ds(c, HALF, stride=2), :]
        o_ref[:, :, cut] = wide_ref[...].astype(BF)


def filter_kernel(
    angles_ref, maps_ref, in_ref, mid_ref, out_ref, rate_ref, taps_ref, gain_ref,
    spec_re_ref, spec_im_ref, coef_ref, rows_ref, pad_ref,
):
    length = HALF * SIDE
    device = lax.axis_index("row_0") * lax.axis_size("row_1") + lax.axis_index("row_1")
    lane = lax.broadcasted_iota(jnp.int32, (8, SIDE), 1)
    row = lax.broadcasted_iota(jnp.int32, (8, SIDE), 0)
    mine = lane == 2 * device + row % 2
    last = (((1,), (1,)), ((), ()))
    first = (((0,), (0,)), ((), ()))
    out_hi = jnp.zeros((8, out_ref.shape[0]), F32)
    out_lo = jnp.zeros((8, out_ref.shape[0]), F32)
    for pair in range(4):
        pick = jnp.where(mine & (row // 2 == pair), 1.0, 0.0).astype(BF)
        top, low = hi_lo(out_ref[:, pair // 2, pair % 2, :])
        out_hi += mm(pick, top, last)
        out_lo += mm(pick, low, last)
    out_hi, out_lo = out_hi.astype(BF), out_lo.astype(BF)
    rate = jnp.sum(jnp.where(mine, rate_ref[...], 0.0), axis=1, keepdims=True)
    for c in range(2):
        sources = [(tap, taps_ref[tap], 0) for tap in range(3)] + [(3, gain_ref[...], 1)]
        for at, source, shift in sources:
            count = source.shape[0]
            at_lane = lax.broadcasted_iota(jnp.int32, (count, SIDE), 1) == 2 * device + c
            value = jnp.sum(jnp.where(at_lane, source, 0.0), axis=1, keepdims=True)
            value = jnp.broadcast_to(value, (count, SIDE))
            for k in range(count):
                coef_ref[k + shift, at : at + 1, c * SIDE : (c + 1) * SIDE] = value[k : k + 1]
    scale = 1.0 / (2.0 * math.pi)
    pad_ref[...] = jnp.zeros_like(pad_ref)
    pad_ref[:32, :] = in_ref[1:33, :] * scale
    pad_ref[32:33, :] = in_ref[0:1, :] * scale
    in_hi, in_lo = hi_lo(pad_ref[...])
    in_all = jnp.concatenate([in_hi, in_lo, in_hi], axis=0)
    mid_hi, mid_lo = hi_lo(mid_ref[...] * scale)
    out_all = jnp.concatenate([out_hi, out_lo, out_hi], axis=1)
    mid_all = jnp.concatenate([mid_hi, mid_lo, mid_hi], axis=0)
    chunk = 1024
    blocks = chunk // SIDE
    sign = jnp.where(row < 4, 1.0, -1.0)
    cos_near, sin_near = (
        angles_ref[2 * SIDE + 16 * k : 2 * SIDE + 16 * (k + 1), :] for k in (2, 3)
    )
    top_row = lax.broadcasted_iota(jnp.int32, (16, SIDE), 0) == 0
    wide_lane = lax.broadcasted_iota(jnp.int32, (16, SIDE), 1)

    def one_chunk(step, squares):
        cos_far, sin_far = (
            pltpu.roll(
                angles_ref[2 * SIDE + 16 * k : 2 * SIDE + 16 * (k + 1), :], SIDE - step * blocks, 1
            )
            for k in (0, 1)
        )
        pieces = []
        for piece in range(blocks):
            far_c, far_s = cos_far[:, piece : piece + 1], sin_far[:, piece : piece + 1]
            lag = (wide_lane + (step * blocks + piece) * SIDE).astype(F32)
            pieces.append(
                jnp.concatenate(
                    [
                        far_c * cos_near - far_s * sin_near,
                        -(far_s * cos_near + far_c * sin_near),
                        jnp.where(top_row, lag * (1.0 / (length - 1)), 0.0),
                    ],
                    axis=0,
                )
            )
        top, low = hi_lo(jnp.concatenate(pieces, axis=1))
        turns = mm(in_all, jnp.concatenate([top, top, low], axis=0), first)
        top, low = hi_lo(sine_of_turns(turns))
        turns = mm(mid_all, jnp.concatenate([top, top, low], axis=0), first)
        top, low = hi_lo(sine_of_turns(turns))
        shaped = mm(out_all, jnp.concatenate([top, top, low], axis=0))
        for piece in range(blocks):
            lag = lane + (step * blocks + piece) * SIDE
            part = shaped[:, piece * SIDE : (piece + 1) * SIDE] * jnp.exp(-rate * lag.astype(F32))
            part = jnp.where((row >= 4) & (lag == 0), 0.0, part)
            squares += part * part
            rows_ref[step * blocks + piece] = pltpu.roll(part, 4, 0) + part * sign
        return squares

    squares = lax.fori_loop(0, length // chunk, one_chunk, jnp.zeros((8, SIDE), F32))
    total = jnp.sum(squares + pltpu.roll(squares, 4, 0), axis=1, keepdims=True)
    factor = lax.rsqrt(total + 1e-06) * (1.0 / (SIDE * SIDE))
    grid = jnp.concatenate([rows_ref[:, j, :] * factor[j : j + 1, :] for j in range(8)], axis=1)
    grid = left_const(
        maps_ref[4 * SIDE :, :HALF], maps_ref[4 * SIDE :, SIDE : SIDE + HALF], grid
    )
    cos, sin = angles_ref[:SIDE, :], angles_ref[SIDE : 2 * SIDE, :]

    def turned(j):
        real = grid[:SIDE, j * SIDE : (j + 1) * SIDE]
        imag = grid[SIDE:, j * SIDE : (j + 1) * SIDE]
        return jnp.concatenate([real * cos + imag * sin, imag * cos - real * sin], axis=1)

    for order in range(2):
        for channel in range(2):
            j = order * 2 + channel
            rows = pl.ds(channel * SIDE, SIDE)
            spec_re_ref[order, rows, :] = right_const(
                turned(j), maps_ref[: 2 * SIDE, :SIDE], maps_ref[2 * SIDE : 4 * SIDE, :SIDE]
            )
            spec_im_ref[order, rows, :] = right_const(
                turned(j + 4), maps_ref[: 2 * SIDE, SIDE:], maps_ref[2 * SIDE : 4 * SIDE, SIDE:]
            )


def conv_kernel(
    x_ref, coef_ref, spec_re_ref, spec_im_ref, angles_ref, maps_ref, more_ref,
    o_ref, wide_ref, rows_ref,
):
    wide_ref[...] = x_ref[...].astype(F32)
    row = lax.broadcasted_iota(jnp.int32, (HALF, SIDE), 0)
    lane = lax.broadcasted_iota(jnp.int32, (HALF, SIDE), 1)

    def smoothed(p):
        seqs = []
        cut = pl.ds(pl.multiple_of(p * SIDE, SIDE), SIDE)
        for s in range(2):
            chans = []
            for c in range(2):
                here = wide_ref[:, s * 2 + c, cut]
                moved = pltpu.roll(here, 1, 1)
                prev = jnp.where(lane == 0, pltpu.roll(moved, 1, 0), moved)
                prev = jnp.where((lane == 0) & (row == 0), 0.0, prev)
                moved = pltpu.roll(here, SIDE - 1, 1)
                after = jnp.where(lane == SIDE - 1, pltpu.roll(moved, HALF - 1, 0), moved)
                after = jnp.where((lane == SIDE - 1) & (row == HALF - 1), 0.0, after)
                first, second, third = (
                    coef_ref[p, tap : tap + 1, c * SIDE : (c + 1) * SIDE] for tap in range(3)
                )
                chans.append(first * prev + second * here + third * after)
            seqs.append(jnp.concatenate(chans, axis=1))
        return jnp.concatenate(seqs, axis=0)

    cos, sin = angles_ref[:SIDE, :], angles_ref[SIDE : 2 * SIDE, :]
    cos2, sin2 = jnp.concatenate([cos, cos], axis=1), jnp.concatenate([sin, sin], axis=1)

    def one_order(order, state):
        grid = left_const(maps_ref[4 * SIDE :, :SIDE], maps_ref[4 * SIDE :, SIDE:], state)
        real, imag = grid[:SIDE], grid[SIDE:]
        real, imag = real * cos2 + imag * sin2, imag * cos2 - real * sin2
        grid = jnp.concatenate(
            [
                jnp.concatenate([real[:, :SIDE], imag[:, :SIDE]], axis=1),
                jnp.concatenate([real[:, SIDE:], imag[:, SIDE:]], axis=1),
            ],
            axis=0,
        )
        grid = right_const(grid, maps_ref[: 2 * SIDE, :], maps_ref[2 * SIDE : 4 * SIDE, :])
        real, imag = grid[:, :SIDE], grid[:, SIDE:]
        k_re, k_im = spec_re_ref[order], spec_im_ref[order]
        grid = jnp.concatenate([real * k_re - imag * k_im, real * k_im + imag * k_re], axis=1)
        grid = right_const(grid, more_ref[: 2 * SIDE, :], more_ref[2 * SIDE : 4 * SIDE, :])
        real = jnp.concatenate([grid[:SIDE, :SIDE], grid[SIDE:, :SIDE]], axis=1)
        imag = jnp.concatenate([grid[:SIDE, SIDE:], grid[SIDE:, SIDE:]], axis=1)
        grid = jnp.concatenate([real * cos2 - imag * sin2, real * sin2 + imag * cos2], axis=0)
        reach = left_const(more_ref[4 * SIDE : 5 * SIDE, :], more_ref[5 * SIDE :, :], grid)
        return smoothed(order + 1) * (reach + coef_ref[order + 1, 3:4, :] * state)

    state = lax.fori_loop(0, 2, one_order, smoothed(0))
    for s in range(2):
        for c in range(2):
            rows_ref[:, c, pl.ds(s * SIDE, SIDE)] = state[
                s * HALF : (s + 1) * HALF, c * SIDE : (c + 1) * SIDE
            ]
    o_ref[...] = rows_ref[...].astype(BF)


def on_device(
    tokens,
    w_value,
    w_first,
    w_second,
    short_taps,
    filter_in,
    filter_mid,
    filter_out,
    decay_rate,
    skip_gain,
    w_output,
):
    seqs, tok_rows, _ = tokens.shape
    blocks = lax.axis_size(ROW)
    length = tok_rows * blocks
    feats = filter_in.shape[0]
    angles, maps, more = (jnp.asarray(t) for t in tables(length, feats))
    far = pl.BlockSpec(memory_space=pltpu.HBM)
    vmem = pl.BlockSpec(memory_space=pltpu.VMEM)
    steps = 4
    pieces = pl.pallas_call(
        functools.partial(project_kernel, steps),
        out_shape=jax.ShapeDtypeStruct((blocks, 4, 3 * tok_rows), BF),
        in_specs=[far] * 4,
        out_specs=vmem,
        scratch_shapes=[
            pltpu.VMEM((seqs * tok_rows, tokens.shape[2]), BF),
            pltpu.VMEM((tokens.shape[2], 3 * SIDE), BF),
            pltpu.VMEM((seqs * tok_rows, 3 * SIDE), F32),
            pltpu.VMEM((2, SIDE, SIDE), F32),
            pltpu.VMEM((HALF, 4, SIDE), F32),
            pltpu.SemaphoreType.DMA((steps, 5)),
        ],
        compiler_params=pltpu.CompilerParams(vmem_limit_bytes=66_700_000),
        name="project",
    )(tokens, w_value, w_first, w_second)
    arrived = lax.all_to_all(pieces, ROW, 0, 0, tiled=True)

    spec = jax.ShapeDtypeStruct((2, 2 * SIDE, SIDE), F32)
    spec_re, spec_im, coef = pl.pallas_call(
        filter_kernel,
        out_shape=(spec, spec, jax.ShapeDtypeStruct((3, 8, 2 * SIDE), F32)),
        in_specs=[vmem] * 8,
        out_specs=(vmem, vmem, vmem),
        scratch_shapes=[
            pltpu.VMEM((HALF, 8, SIDE), F32),
            pltpu.VMEM((48, filter_in.shape[1]), F32),
        ],
        compiler_params=pltpu.CompilerParams(vmem_limit_bytes=16 * 2**20),
        cost_estimate=pl.CostEstimate(
            flops=4_000_000_000, bytes_accessed=3_000_000, transcendentals=0
        ),
        name="filter_spectra",
    )(
        angles,
        maps,
        filter_in,
        filter_mid,
        filter_out,
        decay_rate.reshape(1, -1),
        short_taps,
        skip_gain,
    )
    gated = pl.pallas_call(
        conv_kernel,
        out_shape=jax.ShapeDtypeStruct((blocks, 2, seqs * tok_rows), BF),
        in_specs=[vmem] * 7,
        out_specs=vmem,
        scratch_shapes=[
            pltpu.VMEM((HALF, 4, 3 * SIDE), F32),
            pltpu.VMEM((HALF, 2, 2 * SIDE), F32),
        ],
        compiler_params=pltpu.CompilerParams(vmem_limit_bytes=16 * 2**20),
        cost_estimate=pl.CostEstimate(
            flops=4_000_000_000, bytes_accessed=2_000_000, transcendentals=0
        ),
        name="gated_conv",
    )(
        arrived,
        coef,
        spec_re,
        spec_im,
        angles,
        maps,
        more,
    )
    returned = lax.all_to_all(gated, ROW, 0, 0, tiled=True)
    returned = returned.reshape(2 * blocks, seqs * tok_rows)
    everyone = lax.all_to_all(
        jnp.broadcast_to(returned[None], (lax.axis_size("x"), *returned.shape)), "x", 0, 0, tiled=True
    )
    everyone = lax.all_gather(everyone, "core", axis=1)
    everyone = everyone.reshape(-1, seqs * tok_rows)
    result = jnp.einsum("ct,cd->td", everyone, w_output, preferred_element_type=F32)
    return result.astype(BF).reshape(seqs, tok_rows, -1)


def solution(mesh):
    torus = Mesh(mesh.devices.reshape(8, 8, 4, 2), ("row_0", "row_1", "x", "core"))
    in_specs = (
        P(None, ROW, None),
        P(None, COL),
        P(None, COL),
        P(None, COL),
        P(None, None, COL),
        P(),
        P(),
        P(None, None, None, COL),
        P(COL),
        P(None, COL),
        P(None, COL),
    )
    out_specs = P(None, ROW, COL)
    return jax.shard_map(
        on_device, mesh=torus, in_specs=in_specs, out_specs=out_specs, check_vma=False
    )
```

```python
import functools
import math

import jax
import jax.numpy as jnp
import numpy as np
from jax import lax
from jax.experimental import pallas as pl
from jax.experimental.pallas import tpu as pltpu
from jax.sharding import Mesh
from jax.sharding import PartitionSpec as P

ROW = ("row_0", "row_1")
COL = ("x", "core")
SIDE = 128
HALF = SIDE // 2
CHUNK = 4096
BF = jnp.bfloat16
F32 = jnp.float32


def halves(table):
    table = np.asarray(table, np.float32)
    top = table.astype(jnp.bfloat16)
    return top, (table - top.astype(np.float32)).astype(jnp.bfloat16)


@functools.lru_cache(None)
def tables(length, feats):
    bands = (feats - 1) // 2
    freq = np.linspace(0.0001, bands - 1, bands)[:, None] * (2.0 * math.pi / length)
    coarse, near = freq * np.arange(SIDE) * SIDE, freq * np.arange(SIDE)
    waves = np.stack([np.cos(coarse), np.sin(coarse), np.cos(near), np.sin(near)])
    index = np.arange(SIDE)
    turn = 2.0 * math.pi / SIDE * (index[:, None] * index[None, :] % SIDE)
    cos, sin = np.cos(turn), np.sin(turn)
    fine = 2.0 * math.pi / (SIDE * SIDE) * (index[:, None] * index[None, :])
    pair_in = np.block([[cos[:, :HALF], sin[:, :HALF]], [-sin[:, :HALF], cos[:, :HALF]]])
    right = np.block([[cos, -sin], [sin, cos]])
    in_hi, in_lo = halves(pair_in)
    out_hi, out_lo = halves(pair_in.T)
    right_hi, right_lo = halves(right)
    back_hi, back_lo = halves(right.T)
    real_hi, real_lo = in_hi[:, :HALF], in_lo[:, :HALF]
    real_all = np.concatenate([real_hi, real_lo, real_hi, np.zeros_like(real_hi)], axis=1)
    rights = np.concatenate([right_hi, right_lo])
    backs = np.concatenate([back_hi, back_lo])
    ends = np.concatenate([np.concatenate([in_hi, in_lo], axis=1), out_hi, out_lo])
    turns = np.concatenate([np.cos(fine), np.sin(fine)]).astype(np.float32)
    return np.concatenate(waves).astype(np.float32), turns, real_all, rights, backs, ends


def hi_lo(value):
    top = value.astype(BF)
    return top, (value - top.astype(F32)).astype(BF)


def mm(a, b, dims=(((1,), (0,)), ((), ()))):
    return lax.dot_general(a, b, dims, preferred_element_type=F32)


def left_const(const_hi, const_lo, value):
    top, low = hi_lo(value)
    return mm(const_hi, top) + mm(const_lo, top) + mm(const_hi, low)


def right_const(value, const_hi, const_lo):
    top, low = hi_lo(value)
    return mm(top, const_hi) + mm(low, const_hi) + mm(top, const_lo)


def sine_of_turns(moved):
    moved = moved - jnp.round(moved)
    quarter = 0.25 - jnp.abs(moved)
    square = quarter * quarter
    poly = -70.98993302 * square + 81.34038614
    poly = poly * square - 41.33713041
    poly = poly * square + 6.28316395
    return poly * quarter


def project_kernel(
    steps, tok_hbm, a_hbm, b_hbm, c_hbm, o_ref, tok, weights, sum_ref, flat_ref, wide_ref, sems
):
    depth = tok.shape[1] // steps

    def group_of(step, cut):
        group = []
        for s in range(2):
            group.append((tok_hbm.at[s, :, cut], tok.at[pl.ds(s * SIDE, SIDE), cut]))
        for p, source in enumerate((a_hbm, b_hbm, c_hbm)):
            group.append((source.at[cut, :], weights.at[cut, pl.ds(p * SIDE, SIDE)]))
        return [
            pltpu.make_async_copy(near, far, sems.at[step, k]) for k, (near, far) in enumerate(group)
        ]

    for step in range(steps):
        for copy in group_of(step, pl.ds(step * depth, depth)):
            copy.start()
    sum_ref[...] = jnp.zeros_like(sum_ref)

    @pl.loop(0, steps)
    def _(step):
        cut = pl.ds(pl.multiple_of(step * depth, depth), depth)
        for copy in group_of(step, cut):
            copy.wait()
        sum_ref[...] += mm(tok[:, cut], weights[cut, :])

    @pl.loop(0, 3)
    def _(p):
        cut = pl.ds(pl.multiple_of(p * SIDE, SIDE), SIDE)
        for s in range(2):
            flat_ref[s] = sum_ref[s * SIDE : (s + 1) * SIDE, cut].T
            for c in range(2):
                wide_ref[:, s * 2 + c, :] = flat_ref[s, pl.ds(c, HALF, stride=2), :]
        o_ref[:, :, cut] = wide_ref[...].astype(BF)


def network_kernel(
    waves_ref, in_ref, mid_ref, out_ref, rate_ref, rows_ref, factor_ref, side_ref
):
    length = HALF * SIDE
    device = lax.axis_index("row_0") * lax.axis_size("row_1") + lax.axis_index("row_1")
    lane = lax.broadcasted_iota(jnp.int32, (8, SIDE), 1)
    row = lax.broadcasted_iota(jnp.int32, (8, SIDE), 0)
    mine = lane == 2 * device + row % 2
    last = (((1,), (1,)), ((), ()))
    first = (((0,), (0,)), ((), ()))
    units = mid_ref.shape[0]
    out_hi = jnp.zeros((8, units), F32)
    out_lo = jnp.zeros((8, units), F32)
    for pair in range(4):
        pick = jnp.where(mine & (row // 2 == pair), 1.0, 0.0).astype(BF)
        top, low = hi_lo(out_ref[pl.ds(pair, units, stride=4), :])
        out_hi += mm(pick, top, last)
        out_lo += mm(pick, low, last)
    out_all = jnp.concatenate([out_hi.astype(BF), out_lo.astype(BF)], axis=1)
    rate = jnp.sum(jnp.where(mine, rate_ref[...], 0.0), axis=1, keepdims=True)
    scale = 1.0 / (2.0 * math.pi)
    side_ref[...] = jnp.zeros_like(side_ref)
    ramp_hi, ramp_lo = hi_lo(in_ref[0:1, :] * scale)
    side_ref[0:1, :] = ramp_hi.astype(F32)
    side_ref[1:2, :] = ramp_lo.astype(F32)
    side_ref[2:3, :] = ramp_hi.astype(F32)
    side_ref[3:4, :] = jnp.full((1, units), -0.25, F32)
    side_ref[16:17, :] = jnp.full((1, units), -0.25, F32)
    in_hi, in_lo = hi_lo(in_ref[1:33, :] * scale)
    in_all = jnp.concatenate([in_hi, in_lo, in_hi, side_ref[0:16, :].astype(BF)], axis=0)
    mid_hi, mid_lo = hi_lo(mid_ref[...] * scale)
    mid_all = jnp.concatenate([mid_hi, mid_lo, mid_hi, side_ref[16:32, :].astype(BF)], axis=0)
    chunk = CHUNK
    cos_far, sin_far, cos_near, sin_near = (
        waves_ref[16 * k : 16 * (k + 1), :] for k in range(4)
    )
    ones = jnp.ones((16, chunk), BF)
    sign = jnp.where(row < 4, 1.0, -1.0)
    squares = jnp.zeros((8, SIDE), F32)
    blocks = chunk // SIDE
    for start in range(0, HALF, blocks):
        pieces, sides = [], []
        for block in range(start, start + blocks):
            far_c, far_s = cos_far[:, block : block + 1], sin_far[:, block : block + 1]
            pieces.append(
                jnp.concatenate(
                    [
                        far_c * cos_near - far_s * sin_near,
                        -(far_s * cos_near + far_c * sin_near),
                    ],
                    axis=0,
                )
            )
            ramp = (lane + block * SIDE).astype(F32) * (1.0 / (length - 1))
            ramp_top = ramp.astype(BF).astype(F32)
            ramp = jnp.where(row == 2, ramp - ramp_top, jnp.where(row < 2, ramp_top, 1.0))
            sides.append(jnp.concatenate([ramp, jnp.zeros_like(ramp)], axis=0).astype(BF))
        top, low = hi_lo(jnp.concatenate(pieces, axis=1))
        side = jnp.concatenate(sides, axis=1)
        moved = mm(in_all, jnp.concatenate([top, top, low, side], axis=0), first)
        top, low = hi_lo(sine_of_turns(moved))
        moved = mm(mid_all, jnp.concatenate([top, top, low, ones], axis=0), first)
        top = sine_of_turns(moved).astype(BF)
        shaped = mm(out_all, jnp.concatenate([top, top], axis=0))
        for piece in range(blocks):
            block = start + piece
            lag = lane + block * SIDE
            part = shaped[:, piece * SIDE : (piece + 1) * SIDE] * jnp.exp(-rate * lag.astype(F32))
            if block == 0:
                part = jnp.where((row >= 4) & (lag == 0), 0.0, part)
            squares += part * part
            rows_ref[block * 8 : (block + 1) * 8, :] = pltpu.roll(part, 4, 0) + part * sign
    total = jnp.sum(squares + pltpu.roll(squares, 4, 0), axis=1, keepdims=True)
    factor = lax.rsqrt(total + 1e-06) * (1.0 / (SIDE * SIDE))
    factor_ref[...] = jnp.broadcast_to(factor, factor_ref.shape)


def spectra_kernel(
    rows_ref, factor_ref, turns_ref, real_ref, right_ref, taps_ref, gain_ref,
    spec_re_ref, spec_im_ref, coef_ref,
):
    device = lax.axis_index("row_0") * lax.axis_size("row_1") + lax.axis_index("row_1")
    sources = [(tap, taps_ref[tap], 0) for tap in range(3)] + [(3, gain_ref[...], 1)]
    for c in range(2):
        for at, source, shift in sources:
            count = source.shape[0]
            at_lane = lax.broadcasted_iota(jnp.int32, (count, SIDE), 1) == 2 * device + c
            value = jnp.sum(jnp.where(at_lane, source, 0.0), axis=1, keepdims=True)
            value = jnp.broadcast_to(value, (count, SIDE))
            for k in range(count):
                coef_ref[k + shift, at : at + 1, c * SIDE : (c + 1) * SIDE] = value[k : k + 1]
    pieces = []
    for j in range(8):
        pieces.append(rows_ref[pl.ds(j, HALF, stride=8), :] * factor_ref[j : j + 1, :])
    top, low = hi_lo(jnp.concatenate(pieces, axis=1))
    grid = mm(real_ref[:, : 3 * HALF], jnp.concatenate([top, top, low], axis=0))
    cos, sin = turns_ref[:SIDE, :], turns_ref[SIDE:, :]

    def turned(j):
        real = grid[:SIDE, j * SIDE : (j + 1) * SIDE]
        imag = grid[SIDE:, j * SIDE : (j + 1) * SIDE]
        return jnp.concatenate([real * cos + imag * sin, imag * cos - real * sin], axis=1)

    for j in range(4):
        rows = pl.ds(j % 2 * SIDE, SIDE)
        spec_re_ref[j // 2, rows, :] = right_const(
            turned(j), right_ref[: 2 * SIDE, :SIDE], right_ref[2 * SIDE :, :SIDE]
        )
        spec_im_ref[j // 2, rows, :] = right_const(
            turned(j + 4), right_ref[: 2 * SIDE, SIDE:], right_ref[2 * SIDE :, SIDE:]
        )


def conv_kernel(
    x_ref, coef_ref, spec_re_ref, spec_im_ref, turns_ref, right_ref, back_ref, ends_ref,
    o_ref, wide_ref, rows_ref,
):
    wide_ref[...] = x_ref[...].astype(F32)
    row = lax.broadcasted_iota(jnp.int32, (HALF, SIDE), 0)
    lane = lax.broadcasted_iota(jnp.int32, (HALF, SIDE), 1)

    def smoothed(p):
        seqs = []
        cut = pl.ds(pl.multiple_of(p * SIDE, SIDE), SIDE)
        for s in range(2):
            chans = []
            for c in range(2):
                here = wide_ref[:, s * 2 + c, cut]
                moved = pltpu.roll(here, 1, 1)
                prev = jnp.where(lane == 0, pltpu.roll(moved, 1, 0), moved)
                prev = jnp.where((lane == 0) & (row == 0), 0.0, prev)
                moved = pltpu.roll(here, SIDE - 1, 1)
                after = jnp.where(lane == SIDE - 1, pltpu.roll(moved, HALF - 1, 0), moved)
                after = jnp.where((lane == SIDE - 1) & (row == HALF - 1), 0.0, after)
                first, second, third = (
                    coef_ref[p, tap : tap + 1, c * SIDE : (c + 1) * SIDE] for tap in range(3)
                )
                chans.append(first * prev + second * here + third * after)
            seqs.append(jnp.concatenate(chans, axis=1))
        return jnp.concatenate(seqs, axis=0)

    cos, sin = turns_ref[:SIDE, :], turns_ref[SIDE:, :]
    cos2, sin2 = jnp.concatenate([cos, cos], axis=1), jnp.concatenate([sin, sin], axis=1)

    def one_order(order, state):
        grid = left_const(ends_ref[: 2 * SIDE, :SIDE], ends_ref[: 2 * SIDE, SIDE:], state)
        real, imag = grid[:SIDE], grid[SIDE:]
        real, imag = real * cos2 + imag * sin2, imag * cos2 - real * sin2
        grid = jnp.concatenate(
            [
                jnp.concatenate([real[:, :SIDE], imag[:, :SIDE]], axis=1),
                jnp.concatenate([real[:, SIDE:], imag[:, SIDE:]], axis=1),
            ],
            axis=0,
        )
        grid = right_const(grid, right_ref[: 2 * SIDE, :], right_ref[2 * SIDE :, :])
        real, imag = grid[:, :SIDE], grid[:, SIDE:]
        k_re, k_im = spec_re_ref[order], spec_im_ref[order]
        grid = jnp.concatenate([real * k_re - imag * k_im, real * k_im + imag * k_re], axis=1)
        grid = right_const(grid, back_ref[: 2 * SIDE, :], back_ref[2 * SIDE :, :])
        real = jnp.concatenate([grid[:SIDE, :SIDE], grid[SIDE:, :SIDE]], axis=1)
        imag = jnp.concatenate([grid[:SIDE, SIDE:], grid[SIDE:, SIDE:]], axis=1)
        grid = jnp.concatenate([real * cos2 - imag * sin2, real * sin2 + imag * cos2], axis=0)
        reach = left_const(ends_ref[2 * SIDE : 3 * SIDE, :], ends_ref[3 * SIDE :, :], grid)
        return smoothed(order + 1) * (reach + coef_ref[order + 1, 3:4, :] * state)

    state = lax.fori_loop(0, 2, one_order, smoothed(0))
    for s in range(2):
        for c in range(2):
            rows_ref[:, c, pl.ds(s * SIDE, SIDE)] = state[
                s * HALF : (s + 1) * HALF, c * SIDE : (c + 1) * SIDE
            ]
    o_ref[...] = rows_ref[...].astype(BF)


def on_device(
    tokens,
    w_value,
    w_first,
    w_second,
    short_taps,
    filter_in,
    filter_mid,
    filter_out,
    decay_rate,
    skip_gain,
    w_output,
):
    seqs, tok_rows, _ = tokens.shape
    blocks = lax.axis_size(ROW)
    length = tok_rows * blocks
    feats = filter_in.shape[0]
    waves, turns, real_all, rights, backs, ends = (jnp.asarray(t) for t in tables(length, feats))
    far = pl.BlockSpec(memory_space=pltpu.HBM)
    vmem = pl.BlockSpec(memory_space=pltpu.VMEM)
    steps = 4
    pieces = pl.pallas_call(
        functools.partial(project_kernel, steps),
        out_shape=jax.ShapeDtypeStruct((blocks, 4, 3 * tok_rows), BF),
        in_specs=[far] * 4,
        out_specs=vmem,
        scratch_shapes=[
            pltpu.VMEM((seqs * tok_rows, tokens.shape[2]), BF),
            pltpu.VMEM((tokens.shape[2], 3 * SIDE), BF),
            pltpu.VMEM((seqs * tok_rows, 3 * SIDE), F32),
            pltpu.VMEM((2, SIDE, SIDE), F32),
            pltpu.VMEM((HALF, 4, SIDE), F32),
            pltpu.SemaphoreType.DMA((steps, 5)),
        ],
        compiler_params=pltpu.CompilerParams(vmem_limit_bytes=66_700_000),
        name="project",
    )(tokens, w_value, w_first, w_second)
    arrived = lax.all_to_all(pieces, ROW, 0, 0, tiled=True)

    spec = jax.ShapeDtypeStruct((2, 2 * SIDE, SIDE), F32)
    units = filter_in.shape[1]
    rows, factor = pl.pallas_call(
        network_kernel,
        out_shape=(
            jax.ShapeDtypeStruct((8 * HALF, SIDE), F32),
            jax.ShapeDtypeStruct((8, SIDE), F32),
        ),
        in_specs=[vmem] * 5,
        out_specs=(vmem, vmem),
        scratch_shapes=[pltpu.VMEM((32, units), F32)],
        compiler_params=pltpu.CompilerParams(vmem_limit_bytes=16 * 2**20),
        cost_estimate=pl.CostEstimate(
            flops=4_000_000_000, bytes_accessed=1_000_000, transcendentals=0
        ),
        name="network",
    )(
        waves,
        filter_in,
        filter_mid,
        filter_out.reshape(4 * units, -1),
        decay_rate.reshape(1, -1),
    )
    spec_re, spec_im, coef = pl.pallas_call(
        spectra_kernel,
        out_shape=(spec, spec, jax.ShapeDtypeStruct((3, 8, 2 * SIDE), F32)),
        in_specs=[vmem] * 7,
        out_specs=(vmem,) * 3,
        compiler_params=pltpu.CompilerParams(vmem_limit_bytes=16 * 2**20),
        cost_estimate=pl.CostEstimate(
            flops=1_000_000_000, bytes_accessed=2_000_000, transcendentals=0
        ),
        name="spectra",
    )(rows, factor, turns, real_all, rights, short_taps, skip_gain)
    gated = pl.pallas_call(
        conv_kernel,
        out_shape=jax.ShapeDtypeStruct((blocks, 2, seqs * tok_rows), BF),
        in_specs=[vmem] * 8,
        out_specs=vmem,
        scratch_shapes=[
            pltpu.VMEM((HALF, 4, 3 * SIDE), F32),
            pltpu.VMEM((HALF, 2, 2 * SIDE), F32),
        ],
        compiler_params=pltpu.CompilerParams(vmem_limit_bytes=16 * 2**20),
        cost_estimate=pl.CostEstimate(
            flops=4_000_000_000, bytes_accessed=2_000_000, transcendentals=0
        ),
        name="gated_conv",
    )(
        arrived,
        coef,
        spec_re,
        spec_im,
        turns,
        rights,
        backs,
        ends,
    )
    returned = lax.all_to_all(gated, ROW, 0, 0, tiled=True)
    returned = returned.reshape(2 * blocks, seqs * tok_rows)
    everyone = lax.all_to_all(
        jnp.broadcast_to(returned[None], (lax.axis_size("x"), *returned.shape)), "x", 0, 0, tiled=True
    )
    everyone = lax.all_gather(everyone, "core", axis=1)
    everyone = everyone.reshape(-1, seqs * tok_rows)
    result = jnp.einsum("ct,cd->td", everyone, w_output, preferred_element_type=F32)
    return result.astype(BF).reshape(seqs, tok_rows, -1)


def solution(mesh):
    torus = Mesh(mesh.devices.reshape(8, 8, 4, 2), ("row_0", "row_1", "x", "core"))
    in_specs = (
        P(None, ROW, None),
        P(None, COL),
        P(None, COL),
        P(None, COL),
        P(None, None, COL),
        P(),
        P(),
        P(None, None, None, COL),
        P(COL),
        P(None, COL),
        P(None, COL),
    )
    out_specs = P(None, ROW, COL)
    return jax.shard_map(
        on_device, mesh=torus, in_specs=in_specs, out_specs=out_specs, check_vma=False
    )
```

```python
import functools
import math

import jax
import jax.numpy as jnp
import numpy as np
from jax import lax
from jax.experimental import pallas as pl
from jax.experimental.pallas import tpu as pltpu
from jax.sharding import Mesh
from jax.sharding import PartitionSpec as P

ROW = ("row_0", "row_1")
COL = ("x", "core")
SIDE = 128
HALF = SIDE // 2
CHUNK = 4096
BF = jnp.bfloat16
F32 = jnp.float32


def halves(table):
    table = np.asarray(table, np.float32)
    top = table.astype(jnp.bfloat16)
    return top, (table - top.astype(np.float32)).astype(jnp.bfloat16)


@functools.lru_cache(None)
def tables(length, feats):
    bands = (feats - 1) // 2
    freq = np.linspace(0.0001, bands - 1, bands)[:, None] * (2.0 * math.pi / length)
    coarse, near = freq * np.arange(SIDE) * SIDE, freq * np.arange(SIDE)
    waves = np.stack([np.cos(coarse), np.sin(coarse), np.cos(near), np.sin(near)])
    index = np.arange(SIDE)
    turn = 2.0 * math.pi / SIDE * (index[:, None] * index[None, :] % SIDE)
    cos, sin = np.cos(turn), np.sin(turn)
    fine = 2.0 * math.pi / (SIDE * SIDE) * (index[:, None] * index[None, :])
    pair_in = np.block([[cos[:, :HALF], sin[:, :HALF]], [-sin[:, :HALF], cos[:, :HALF]]])
    right = np.block([[cos, -sin], [sin, cos]])
    in_hi, in_lo = halves(pair_in)
    out_hi, out_lo = halves(pair_in.T)
    right_hi, right_lo = halves(right)
    back_hi, back_lo = halves(right.T)
    real_hi, real_lo = in_hi[:, :HALF], in_lo[:, :HALF]
    real_all = np.concatenate([real_hi, real_lo, real_hi, np.zeros_like(real_hi)], axis=1)
    rights = np.concatenate([right_hi, right_lo])
    backs = np.concatenate([back_hi, back_lo])
    ends = np.concatenate([np.concatenate([in_hi, in_lo], axis=1), out_hi, out_lo])
    turns = np.concatenate([np.cos(fine), np.sin(fine)]).astype(np.float32)
    return np.concatenate(waves).astype(np.float32), turns, real_all, rights, backs, ends


def hi_lo(value):
    top = value.astype(BF)
    return top, (value - top.astype(F32)).astype(BF)


def mm(a, b, dims=(((1,), (0,)), ((), ()))):
    return lax.dot_general(a, b, dims, preferred_element_type=F32)


def left_const(const_hi, const_lo, value):
    top, low = hi_lo(value)
    return mm(const_hi, top) + mm(const_lo, top) + mm(const_hi, low)


def right_const(value, const_hi, const_lo):
    top, low = hi_lo(value)
    return mm(top, const_hi) + mm(low, const_hi) + mm(top, const_lo)


def sine_of_turns(moved):
    moved = moved - jnp.round(moved)
    quarter = 0.25 - jnp.abs(moved)
    square = quarter * quarter
    poly = -70.98993302 * square + 81.34038614
    poly = poly * square - 41.33713041
    poly = poly * square + 6.28316395
    return poly * quarter


def project_kernel(
    steps, tok_hbm, a_hbm, b_hbm, c_hbm, o_ref, tok, weights, sum_ref, sems
):
    depth = tok.shape[1] // steps

    def group_of(step, cut):
        group = []
        for s in range(2):
            group.append((tok_hbm.at[s, :, cut], tok.at[pl.ds(s * SIDE, SIDE), cut]))
        for p, source in enumerate((a_hbm, b_hbm, c_hbm)):
            group.append((source.at[cut, :], weights.at[cut, pl.ds(p * SIDE, SIDE)]))
        return [
            pltpu.make_async_copy(near, far, sems.at[step, k]) for k, (near, far) in enumerate(group)
        ]

    for step in range(steps):
        for copy in group_of(step, pl.ds(step * depth, depth)):
            copy.start()
    for step in range(steps):
        for copy in group_of(step, pl.ds(step * depth, depth)):
            copy.wait()
        cut = slice(step * depth, (step + 1) * depth)
        part = mm(tok[:, cut], weights[cut, :])
        if step < steps - 1:
            sum_ref[...] = part if step == 0 else sum_ref[...] + part
    part += sum_ref[...]
    for p in range(3):
        cut = slice(p * SIDE, (p + 1) * SIDE)
        for s in range(2):
            turned = part[s * SIDE : (s + 1) * SIDE, cut].T
            o_ref[:, 2 * s : 2 * s + 2, cut] = turned.astype(BF).reshape(HALF, 2, SIDE)


def network_kernel(
    waves_ref, in_ref, mid_ref, out_ref, rate_ref, rows_ref, factor_ref, side_ref
):
    length = HALF * SIDE
    device = lax.axis_index("row_0") * lax.axis_size("row_1") + lax.axis_index("row_1")
    lane = lax.broadcasted_iota(jnp.int32, (8, SIDE), 1)
    row = lax.broadcasted_iota(jnp.int32, (8, SIDE), 0)
    mine = lane == 2 * device + row % 2
    last = (((1,), (1,)), ((), ()))
    first = (((0,), (0,)), ((), ()))
    units = mid_ref.shape[0]
    out_hi = jnp.zeros((8, units), F32)
    out_lo = jnp.zeros((8, units), F32)
    for pair in range(4):
        pick = jnp.where(mine & (row // 2 == pair), 1.0, 0.0).astype(BF)
        top, low = hi_lo(out_ref[pl.ds(pair, units, stride=4), :])
        out_hi += mm(pick, top, last)
        out_lo += mm(pick, low, last)
    out_hi, out_lo = out_hi.astype(BF), out_lo.astype(BF)
    out_all = jnp.concatenate([out_hi, out_lo, out_hi], axis=1)
    rate = jnp.sum(jnp.where(mine, rate_ref[...], 0.0), axis=1, keepdims=True)
    scale = 1.0 / (2.0 * math.pi)
    side_ref[...] = jnp.zeros_like(side_ref)
    ramp_hi, ramp_lo = hi_lo(in_ref[0:1, :] * scale)
    side_ref[0:1, :] = ramp_hi.astype(F32)
    side_ref[1:2, :] = ramp_lo.astype(F32)
    side_ref[2:3, :] = ramp_hi.astype(F32)
    side_ref[3:4, :] = jnp.full((1, units), -0.25, F32)
    side_ref[16:17, :] = jnp.full((1, units), -0.25, F32)
    in_hi, in_lo = hi_lo(in_ref[1:33, :] * scale)
    in_all = jnp.concatenate([in_hi, in_lo, in_hi, side_ref[0:16, :].astype(BF)], axis=0)
    mid_hi, mid_lo = hi_lo(mid_ref[...] * scale)
    mid_all = jnp.concatenate([mid_hi, mid_lo, mid_hi, side_ref[16:32, :].astype(BF)], axis=0)
    chunk = CHUNK
    cos_far, sin_far, cos_near, sin_near = (
        waves_ref[16 * k : 16 * (k + 1), :] for k in range(4)
    )
    ones = jnp.ones((16, chunk), BF)
    sign = jnp.where(row < 4, 1.0, -1.0)
    squares = jnp.zeros((8, SIDE), F32)
    blocks = chunk // SIDE
    for start in range(0, HALF, blocks):
        pieces, sides = [], []
        for block in range(start, start + blocks):
            far_c, far_s = cos_far[:, block : block + 1], sin_far[:, block : block + 1]
            pieces.append(
                jnp.concatenate(
                    [
                        far_c * cos_near - far_s * sin_near,
                        -(far_s * cos_near + far_c * sin_near),
                    ],
                    axis=0,
                )
            )
            ramp = (lane + block * SIDE).astype(F32) * (1.0 / (length - 1))
            ramp_top = ramp.astype(BF).astype(F32)
            ramp = jnp.where(row == 2, ramp - ramp_top, jnp.where(row < 2, ramp_top, 1.0))
            sides.append(jnp.concatenate([ramp, jnp.zeros_like(ramp)], axis=0).astype(BF))
        top, low = hi_lo(jnp.concatenate(pieces, axis=1))
        side = jnp.concatenate(sides, axis=1)
        moved = mm(in_all, jnp.concatenate([top, top, low, side], axis=0), first)
        top, low = hi_lo(sine_of_turns(moved))
        moved = mm(mid_all, jnp.concatenate([top, top, low, ones], axis=0), first)
        top, low = hi_lo(sine_of_turns(moved))
        shaped = mm(out_all, jnp.concatenate([top, top, low], axis=0))
        for piece in range(blocks):
            block = start + piece
            lag = lane + block * SIDE
            part = shaped[:, piece * SIDE : (piece + 1) * SIDE] * jnp.exp(-rate * lag.astype(F32))
            if block == 0:
                part = jnp.where((row >= 4) & (lag == 0), 0.0, part)
            squares += part * part
            rows_ref[block * 8 : (block + 1) * 8, :] = pltpu.roll(part, 4, 0) + part * sign
    total = jnp.sum(squares + pltpu.roll(squares, 4, 0), axis=1, keepdims=True)
    factor = lax.rsqrt(total + 1e-06) * (1.0 / (SIDE * SIDE))
    factor_ref[...] = jnp.broadcast_to(factor, factor_ref.shape)


def spectra_kernel(
    rows_ref, factor_ref, turns_ref, real_ref, right_ref, taps_ref, gain_ref,
    spec_re_ref, spec_im_ref, coef_ref,
):
    device = lax.axis_index("row_0") * lax.axis_size("row_1") + lax.axis_index("row_1")
    sources = [(tap, taps_ref[tap], 0) for tap in range(3)] + [(3, gain_ref[...], 1)]
    for c in range(2):
        for at, source, shift in sources:
            count = source.shape[0]
            at_lane = lax.broadcasted_iota(jnp.int32, (count, SIDE), 1) == 2 * device + c
            value = jnp.sum(jnp.where(at_lane, source, 0.0), axis=1, keepdims=True)
            value = jnp.broadcast_to(value, (count, SIDE))
            for k in range(count):
                coef_ref[k + shift, at : at + 1, c * SIDE : (c + 1) * SIDE] = value[k : k + 1]
    pieces = []
    for j in range(8):
        pieces.append(rows_ref[pl.ds(j, HALF, stride=8), :] * factor_ref[j : j + 1, :])
    top, low = hi_lo(jnp.concatenate(pieces, axis=1))
    grid = mm(real_ref[:, : 3 * HALF], jnp.concatenate([top, top, low], axis=0))
    cos, sin = turns_ref[:SIDE, :], turns_ref[SIDE:, :]

    def turned(j):
        real = grid[:SIDE, j * SIDE : (j + 1) * SIDE]
        imag = grid[SIDE:, j * SIDE : (j + 1) * SIDE]
        return jnp.concatenate([real * cos + imag * sin, imag * cos - real * sin], axis=1)

    for j in range(4):
        rows = pl.ds(j % 2 * SIDE, SIDE)
        spec_re_ref[j // 2, rows, :] = right_const(
            turned(j), right_ref[: 2 * SIDE, :SIDE], right_ref[2 * SIDE :, :SIDE]
        )
        spec_im_ref[j // 2, rows, :] = right_const(
            turned(j + 4), right_ref[: 2 * SIDE, SIDE:], right_ref[2 * SIDE :, SIDE:]
        )


def conv_kernel(
    x_ref, coef_ref, spec_re_ref, spec_im_ref, turns_ref, right_ref, back_ref, ends_ref,
    o_ref, rows_ref,
):
    for p in range(3):
        for s in range(2):
            piece = x_ref[:, 2 * s : 2 * s + 2, p * SIDE : (p + 1) * SIDE]
            rows_ref[2 * p + s] = piece.reshape(SIDE, SIDE).astype(F32)
    row = lax.broadcasted_iota(jnp.int32, (HALF, SIDE), 0)
    lane = lax.broadcasted_iota(jnp.int32, (HALF, SIDE), 1)

    def smoothed(p):
        seqs = []
        for s in range(2):
            chans = []
            for c in range(2):
                here = rows_ref[2 * p + s, pl.ds(c, HALF, stride=2), :]
                moved = pltpu.roll(here, 1, 1)
                prev = jnp.where(lane == 0, pltpu.roll(moved, 1, 0), moved)
                prev = jnp.where((lane == 0) & (row == 0), 0.0, prev)
                moved = pltpu.roll(here, SIDE - 1, 1)
                after = jnp.where(lane == SIDE - 1, pltpu.roll(moved, HALF - 1, 0), moved)
                after = jnp.where((lane == SIDE - 1) & (row == HALF - 1), 0.0, after)
                first, second, third = (
                    coef_ref[p, tap : tap + 1, c * SIDE : (c + 1) * SIDE] for tap in range(3)
                )
                chans.append(first * prev + second * here + third * after)
            seqs.append(jnp.concatenate(chans, axis=1))
        return jnp.concatenate(seqs, axis=0)

    cos, sin = turns_ref[:SIDE, :], turns_ref[SIDE:, :]
    cos2, sin2 = jnp.concatenate([cos, cos], axis=1), jnp.concatenate([sin, sin], axis=1)

    def one_order(order, state):
        grid = left_const(ends_ref[: 2 * SIDE, :SIDE], ends_ref[: 2 * SIDE, SIDE:], state)
        real, imag = grid[:SIDE], grid[SIDE:]
        real, imag = real * cos2 + imag * sin2, imag * cos2 - real * sin2
        grid = jnp.concatenate(
            [
                jnp.concatenate([real[:, :SIDE], imag[:, :SIDE]], axis=1),
                jnp.concatenate([real[:, SIDE:], imag[:, SIDE:]], axis=1),
            ],
            axis=0,
        )
        grid = right_const(grid, right_ref[: 2 * SIDE, :], right_ref[2 * SIDE :, :])
        real, imag = grid[:, :SIDE], grid[:, SIDE:]
        k_re, k_im = spec_re_ref[order], spec_im_ref[order]
        grid = jnp.concatenate([real * k_re - imag * k_im, real * k_im + imag * k_re], axis=1)
        grid = right_const(grid, back_ref[: 2 * SIDE, :], back_ref[2 * SIDE :, :])
        real = jnp.concatenate([grid[:SIDE, :SIDE], grid[SIDE:, :SIDE]], axis=1)
        imag = jnp.concatenate([grid[:SIDE, SIDE:], grid[SIDE:, SIDE:]], axis=1)
        grid = jnp.concatenate([real * cos2 - imag * sin2, real * sin2 + imag * cos2], axis=0)
        reach = left_const(ends_ref[2 * SIDE : 3 * SIDE, :], ends_ref[3 * SIDE :, :], grid)
        return smoothed(order + 1) * (reach + coef_ref[order + 1, 3:4, :] * state)

    state = lax.fori_loop(0, 2, one_order, smoothed(0))
    for s in range(2):
        for c in range(2):
            rows_ref[s, pl.ds(c, HALF, stride=2), :] = state[
                s * HALF : (s + 1) * HALF, c * SIDE : (c + 1) * SIDE
            ]
        o_ref[:, :, s * SIDE : (s + 1) * SIDE] = rows_ref[s].astype(BF).reshape(HALF, 2, SIDE)


def on_device(
    tokens,
    w_value,
    w_first,
    w_second,
    short_taps,
    filter_in,
    filter_mid,
    filter_out,
    decay_rate,
    skip_gain,
    w_output,
):
    seqs, tok_rows, _ = tokens.shape
    blocks = lax.axis_size(ROW)
    length = tok_rows * blocks
    feats = filter_in.shape[0]
    waves, turns, real_all, rights, backs, ends = (jnp.asarray(t) for t in tables(length, feats))
    far = pl.BlockSpec(memory_space=pltpu.HBM)
    vmem = pl.BlockSpec(memory_space=pltpu.VMEM)
    steps = 2
    pieces = pl.pallas_call(
        functools.partial(project_kernel, steps),
        out_shape=jax.ShapeDtypeStruct((blocks, 4, 3 * tok_rows), BF),
        in_specs=[far] * 4,
        out_specs=vmem,
        scratch_shapes=[
            pltpu.VMEM((seqs * tok_rows, tokens.shape[2]), BF),
            pltpu.VMEM((tokens.shape[2], 3 * SIDE), BF),
            pltpu.VMEM((seqs * tok_rows, 3 * SIDE), F32),
            pltpu.SemaphoreType.DMA((steps, 5)),
        ],
        compiler_params=pltpu.CompilerParams(vmem_limit_bytes=66_700_000),
        name="project",
    )(tokens, w_value, w_first, w_second)
    arrived = lax.all_to_all(pieces, ROW, 0, 0, tiled=True)

    spec = jax.ShapeDtypeStruct((2, 2 * SIDE, SIDE), F32)
    units = filter_in.shape[1]
    rows, factor = pl.pallas_call(
        network_kernel,
        out_shape=(
            jax.ShapeDtypeStruct((8 * HALF, SIDE), F32),
            jax.ShapeDtypeStruct((8, SIDE), F32),
        ),
        in_specs=[vmem] * 5,
        out_specs=(vmem, vmem),
        scratch_shapes=[pltpu.VMEM((32, units), F32)],
        compiler_params=pltpu.CompilerParams(vmem_limit_bytes=16 * 2**20),
        cost_estimate=pl.CostEstimate(
            flops=4_000_000_000, bytes_accessed=1_000_000, transcendentals=0
        ),
        name="network",
    )(
        waves,
        filter_in,
        filter_mid,
        filter_out.reshape(4 * units, -1),
        decay_rate.reshape(1, -1),
    )
    spec_re, spec_im, coef = pl.pallas_call(
        spectra_kernel,
        out_shape=(spec, spec, jax.ShapeDtypeStruct((3, 8, 2 * SIDE), F32)),
        in_specs=[vmem] * 7,
        out_specs=(vmem,) * 3,
        compiler_params=pltpu.CompilerParams(vmem_limit_bytes=16 * 2**20),
        cost_estimate=pl.CostEstimate(
            flops=1_000_000_000, bytes_accessed=2_000_000, transcendentals=0
        ),
        name="spectra",
    )(rows, factor, turns, real_all, rights, short_taps, skip_gain)
    gated = pl.pallas_call(
        conv_kernel,
        out_shape=jax.ShapeDtypeStruct((blocks, 2, seqs * tok_rows), BF),
        in_specs=[vmem] * 8,
        out_specs=vmem,
        scratch_shapes=[
            pltpu.VMEM((6, SIDE, SIDE), F32),
        ],
        compiler_params=pltpu.CompilerParams(vmem_limit_bytes=16 * 2**20),
        cost_estimate=pl.CostEstimate(
            flops=4_000_000_000, bytes_accessed=2_000_000, transcendentals=0
        ),
        name="gated_conv",
    )(
        arrived,
        coef,
        spec_re,
        spec_im,
        turns,
        rights,
        backs,
        ends,
    )
    returned = lax.all_to_all(gated, ROW, 0, 0, tiled=True)
    returned = returned.reshape(2 * blocks, seqs * tok_rows)
    everyone = lax.all_to_all(
        jnp.broadcast_to(returned[None], (lax.axis_size("x"), *returned.shape)), "x", 0, 0, tiled=True
    )
    everyone = lax.all_gather(everyone, "core", axis=1)
    everyone = everyone.reshape(-1, seqs * tok_rows)
    result = jnp.einsum("ct,cd->td", everyone, w_output, preferred_element_type=F32)
    return result.astype(BF).reshape(seqs, tok_rows, -1)


def solution(mesh):
    torus = Mesh(mesh.devices.reshape(8, 8, 4, 2), ("row_0", "row_1", "x", "core"))
    in_specs = (
        P(None, ROW, None),
        P(None, COL),
        P(None, COL),
        P(None, COL),
        P(None, None, COL),
        P(),
        P(),
        P(None, None, None, COL),
        P(COL),
        P(None, COL),
        P(None, COL),
    )
    out_specs = P(None, ROW, COL)
    return jax.shard_map(
        on_device, mesh=torus, in_specs=in_specs, out_specs=out_specs, check_vma=False
    )
```

```python
import functools
import math

import jax
import jax.numpy as jnp
import numpy as np
from jax import lax
from jax.experimental import pallas as pl
from jax.experimental.pallas import tpu as pltpu
from jax.sharding import Mesh
from jax.sharding import PartitionSpec as P

ROW = ("row_0", "row_1")
COL = ("x", "core")
SIDE = 128
HALF = SIDE // 2
CHUNK = 4096
BF = jnp.bfloat16
F32 = jnp.float32


def halves(table):
    table = np.asarray(table, np.float32)
    top = table.astype(jnp.bfloat16)
    return top, (table - top.astype(np.float32)).astype(jnp.bfloat16)


@functools.lru_cache(None)
def tables(length, feats):
    bands = (feats - 1) // 2
    freq = np.linspace(0.0001, bands - 1, bands)[:, None] * (2.0 * math.pi / length)
    coarse, near = freq * np.arange(SIDE) * SIDE, freq * np.arange(SIDE)
    waves = np.stack([np.cos(coarse), np.sin(coarse), np.cos(near), np.sin(near)])
    index = np.arange(SIDE)
    turn = 2.0 * math.pi / SIDE * (index[:, None] * index[None, :] % SIDE)
    cos, sin = np.cos(turn), np.sin(turn)
    fine = 2.0 * math.pi / (SIDE * SIDE) * (index[:, None] * index[None, :])
    pair_in = np.block([[cos[:, :HALF], sin[:, :HALF]], [-sin[:, :HALF], cos[:, :HALF]]])
    right = np.block([[cos, -sin], [sin, cos]])
    in_hi, in_lo = halves(pair_in)
    out_hi, out_lo = halves(pair_in.T)
    right_hi, right_lo = halves(right)
    back_hi, back_lo = halves(right.T)
    real_hi, real_lo = in_hi[:, :HALF], in_lo[:, :HALF]
    real_all = np.concatenate([real_hi, real_lo, real_hi, np.zeros_like(real_hi)], axis=1)
    rights = np.concatenate([right_hi, right_lo])
    backs = np.concatenate([back_hi, back_lo])
    ends = np.concatenate([np.concatenate([in_hi, in_lo], axis=1), out_hi, out_lo])
    turns = np.concatenate([np.cos(fine), np.sin(fine)]).astype(np.float32)
    return np.concatenate(waves).astype(np.float32), turns, real_all, rights, backs, ends


def hi_lo(value):
    top = value.astype(BF)
    return top, (value - top.astype(F32)).astype(BF)


def mm(a, b, dims=(((1,), (0,)), ((), ()))):
    return lax.dot_general(a, b, dims, preferred_element_type=F32)


def left_const(const_hi, const_lo, value):
    top, low = hi_lo(value)
    return mm(const_hi, top) + mm(const_lo, top) + mm(const_hi, low)


def right_const(value, const_hi, const_lo):
    top, low = hi_lo(value)
    return mm(top, const_hi) + mm(low, const_hi) + mm(top, const_lo)


def sine_of_turns(moved):
    moved = moved - jnp.round(moved)
    quarter = 0.25 - jnp.abs(moved)
    square = quarter * quarter
    poly = -70.98993302 * square + 81.34038614
    poly = poly * square - 41.33713041
    poly = poly * square + 6.28316395
    return poly * quarter


def project_kernel(
    steps, tok_hbm, a_hbm, b_hbm, c_hbm, o_ref, tok, weights, sum_ref, sems
):
    depth = tok.shape[1] // steps

    def group_of(step, cut):
        group = []
        for s in range(2):
            group.append((tok_hbm.at[s, :, cut], tok.at[pl.ds(s * SIDE, SIDE), cut]))
        for p, source in enumerate((a_hbm, b_hbm, c_hbm)):
            group.append((source.at[cut, :], weights.at[cut, pl.ds(p * SIDE, SIDE)]))
        return [
            pltpu.make_async_copy(near, far, sems.at[step, k]) for k, (near, far) in enumerate(group)
        ]

    for step in range(steps):
        for copy in group_of(step, pl.ds(step * depth, depth)):
            copy.start()
    for step in range(steps):
        for copy in group_of(step, pl.ds(step * depth, depth)):
            copy.wait()
        cut = slice(step * depth, (step + 1) * depth)
        part = mm(tok[:, cut], weights[cut, :])
        if step < steps - 1:
            sum_ref[...] = part if step == 0 else sum_ref[...] + part
    part += sum_ref[...]
    for p in range(3):
        cut = slice(p * SIDE, (p + 1) * SIDE)
        for s in range(2):
            turned = part[s * SIDE : (s + 1) * SIDE, cut].T
            o_ref[:, 2 * s : 2 * s + 2, cut] = turned.astype(BF).reshape(HALF, 2, SIDE)


def network_kernel(
    waves_ref, in_ref, mid_ref, out_ref, rate_ref, rows_ref, factor_ref, side_ref
):
    length = HALF * SIDE
    device = lax.axis_index("row_0") * lax.axis_size("row_1") + lax.axis_index("row_1")
    lane = lax.broadcasted_iota(jnp.int32, (8, SIDE), 1)
    row = lax.broadcasted_iota(jnp.int32, (8, SIDE), 0)
    mine = lane == 2 * device + row % 2
    last = (((1,), (1,)), ((), ()))
    first = (((0,), (0,)), ((), ()))
    units = mid_ref.shape[0]
    out_hi = jnp.zeros((8, units), F32)
    out_lo = jnp.zeros((8, units), F32)
    for pair in range(4):
        pick = jnp.where(mine & (row // 2 == pair), 1.0, 0.0).astype(BF)
        top, low = hi_lo(out_ref[pl.ds(pair, units, stride=4), :])
        out_hi += mm(pick, top, last)
        out_lo += mm(pick, low, last)
    out_hi, out_lo = out_hi.astype(BF), out_lo.astype(BF)
    out_all = jnp.concatenate([out_hi, out_lo, out_hi], axis=1)
    rate = jnp.sum(jnp.where(mine, rate_ref[...], 0.0), axis=1, keepdims=True)
    scale = 1.0 / (2.0 * math.pi)
    side_ref[...] = jnp.zeros_like(side_ref)
    ramp_hi, ramp_lo = hi_lo(in_ref[0:1, :] * scale)
    side_ref[0:1, :] = ramp_hi.astype(F32)
    side_ref[1:2, :] = ramp_lo.astype(F32)
    side_ref[2:3, :] = ramp_hi.astype(F32)
    side_ref[3:4, :] = jnp.full((1, units), -0.25, F32)
    side_ref[16:17, :] = jnp.full((1, units), -0.25, F32)
    in_hi, in_lo = hi_lo(in_ref[1:33, :] * scale)
    in_all = jnp.concatenate([in_hi, in_lo, in_hi, side_ref[0:16, :].astype(BF)], axis=0)
    mid_hi, mid_lo = hi_lo(mid_ref[...] * scale)
    mid_all = jnp.concatenate([mid_hi, mid_lo, mid_hi, side_ref[16:32, :].astype(BF)], axis=0)
    chunk = CHUNK
    cos_far, sin_far, cos_near, sin_near = (
        waves_ref[16 * k : 16 * (k + 1), :] for k in range(4)
    )
    ones = jnp.ones((16, chunk), BF)
    sign = jnp.where(row < 4, 1.0, -1.0)
    squares = jnp.zeros((8, SIDE), F32)
    blocks = chunk // SIDE
    for start in range(0, HALF, blocks):
        pieces, sides = [], []
        for block in range(start, start + blocks):
            far_c, far_s = cos_far[:, block : block + 1], sin_far[:, block : block + 1]
            pieces.append(
                jnp.concatenate(
                    [
                        far_c * cos_near - far_s * sin_near,
                        -(far_s * cos_near + far_c * sin_near),
                    ],
                    axis=0,
                )
            )
            ramp = (lane + block * SIDE).astype(F32) * (1.0 / (length - 1))
            ramp_top = ramp.astype(BF).astype(F32)
            ramp = jnp.where(row == 2, ramp - ramp_top, jnp.where(row < 2, ramp_top, 1.0))
            sides.append(jnp.concatenate([ramp, jnp.zeros_like(ramp)], axis=0).astype(BF))
        top, low = hi_lo(jnp.concatenate(pieces, axis=1))
        side = jnp.concatenate(sides, axis=1)
        moved = mm(in_all, jnp.concatenate([top, top, low, side], axis=0), first)
        top, low = hi_lo(sine_of_turns(moved))
        moved = mm(mid_all, jnp.concatenate([top, top, low, ones], axis=0), first)
        top, low = hi_lo(sine_of_turns(moved))
        shaped = mm(out_all, jnp.concatenate([top, top, low], axis=0))
        for piece in range(blocks):
            block = start + piece
            lag = lane + block * SIDE
            part = shaped[:, piece * SIDE : (piece + 1) * SIDE] * jnp.exp(-rate * lag.astype(F32))
            if block == 0:
                part = jnp.where((row >= 4) & (lag == 0), 0.0, part)
            squares += part * part
            rows_ref[block * 8 : (block + 1) * 8, :] = pltpu.roll(part, 4, 0) + part * sign
    total = jnp.sum(squares + pltpu.roll(squares, 4, 0), axis=1, keepdims=True)
    factor = lax.rsqrt(total + 1e-06) * (1.0 / (SIDE * SIDE))
    factor_ref[...] = jnp.broadcast_to(factor, factor_ref.shape)


def spectra_kernel(
    rows_ref, factor_ref, turns_ref, real_ref, right_ref, taps_ref, gain_ref,
    spec_re_ref, spec_im_ref, coef_ref,
):
    device = lax.axis_index("row_0") * lax.axis_size("row_1") + lax.axis_index("row_1")
    sources = [(tap, taps_ref[tap], 0) for tap in range(3)] + [(3, gain_ref[...], 1)]
    for c in range(2):
        for at, source, shift in sources:
            count = source.shape[0]
            at_lane = lax.broadcasted_iota(jnp.int32, (count, SIDE), 1) == 2 * device + c
            value = jnp.sum(jnp.where(at_lane, source, 0.0), axis=1, keepdims=True)
            value = jnp.broadcast_to(value, (count, SIDE))
            for k in range(count):
                coef_ref[k + shift, at : at + 1, c * SIDE : (c + 1) * SIDE] = value[k : k + 1]
    pieces = []
    for j in range(8):
        pieces.append(rows_ref[pl.ds(j, HALF, stride=8), :] * factor_ref[j : j + 1, :])
    top, low = hi_lo(jnp.concatenate(pieces, axis=1))
    grid = mm(real_ref[:, : 3 * HALF], jnp.concatenate([top, top, low], axis=0))
    cos, sin = turns_ref[:SIDE, :], turns_ref[SIDE:, :]

    def turned(j):
        real = grid[:SIDE, j * SIDE : (j + 1) * SIDE]
        imag = grid[SIDE:, j * SIDE : (j + 1) * SIDE]
        return jnp.concatenate([real * cos + imag * sin, imag * cos - real * sin], axis=1)

    for j in range(4):
        rows = pl.ds(j % 2 * SIDE, SIDE)
        spec_re_ref[j // 2, rows, :] = right_const(
            turned(j), right_ref[: 2 * SIDE, :SIDE], right_ref[2 * SIDE :, :SIDE]
        )
        spec_im_ref[j // 2, rows, :] = right_const(
            turned(j + 4), right_ref[: 2 * SIDE, SIDE:], right_ref[2 * SIDE :, SIDE:]
        )


def conv_kernel(
    x_ref, coef_ref, spec_re_ref, spec_im_ref, turns_ref, right_ref, back_ref, ends_ref,
    o_ref, rows_ref,
):
    for p in range(3):
        for s in range(2):
            piece = x_ref[:, 2 * s : 2 * s + 2, p * SIDE : (p + 1) * SIDE]
            rows_ref[2 * p + s] = piece.reshape(SIDE, SIDE).astype(F32)
    row = lax.broadcasted_iota(jnp.int32, (HALF, SIDE), 0)
    lane = lax.broadcasted_iota(jnp.int32, (HALF, SIDE), 1)

    def smoothed(p):
        seqs = []
        for s in range(2):
            chans = []
            for c in range(2):
                here = rows_ref[2 * p + s, pl.ds(c, HALF, stride=2), :]
                moved = pltpu.roll(here, 1, 1)
                prev = jnp.where(lane == 0, pltpu.roll(moved, 1, 0), moved)
                prev = jnp.where((lane == 0) & (row == 0), 0.0, prev)
                moved = pltpu.roll(here, SIDE - 1, 1)
                after = jnp.where(lane == SIDE - 1, pltpu.roll(moved, HALF - 1, 0), moved)
                after = jnp.where((lane == SIDE - 1) & (row == HALF - 1), 0.0, after)
                first, second, third = (
                    coef_ref[p, tap : tap + 1, c * SIDE : (c + 1) * SIDE] for tap in range(3)
                )
                chans.append(first * prev + second * here + third * after)
            seqs.append(jnp.concatenate(chans, axis=1))
        return jnp.concatenate(seqs, axis=0)

    cos, sin = turns_ref[:SIDE, :], turns_ref[SIDE:, :]
    cos2, sin2 = jnp.concatenate([cos, cos], axis=1), jnp.concatenate([sin, sin], axis=1)

    def one_order(order, state):
        top, low = hi_lo(state)
        grid = mm(ends_ref[: 2 * SIDE, :], jnp.concatenate([top, top], axis=0))
        grid += mm(ends_ref[: 2 * SIDE, :SIDE], low)
        reals, imags = [], []
        for c in range(2):
            cut = slice(c * SIDE, (c + 1) * SIDE)
            real, imag = grid[:SIDE, cut], grid[SIDE:, cut]
            pair = jnp.concatenate([real * cos + imag * sin, imag * cos - real * sin], axis=1)
            pair = right_const(pair, right_ref[: 2 * SIDE, :], right_ref[2 * SIDE :, :])
            real, imag = pair[:, :SIDE], pair[:, SIDE:]
            k_re, k_im = spec_re_ref[order, cut, :], spec_im_ref[order, cut, :]
            pair = jnp.concatenate([real * k_re - imag * k_im, real * k_im + imag * k_re], axis=1)
            pair = right_const(pair, back_ref[: 2 * SIDE, :], back_ref[2 * SIDE :, :])
            real, imag = pair[:, :SIDE], pair[:, SIDE:]
            reals.append(real * cos - imag * sin)
            imags.append(real * sin + imag * cos)
        grid = jnp.concatenate(
            [jnp.concatenate(reals, axis=1), jnp.concatenate(imags, axis=1)], axis=0
        )
        reach = left_const(ends_ref[2 * SIDE : 3 * SIDE, :], ends_ref[3 * SIDE :, :], grid)
        return smoothed(order + 1) * (reach + coef_ref[order + 1, 3:4, :] * state)

    state = one_order(1, one_order(0, smoothed(0)))
    for s in range(2):
        for c in range(2):
            rows_ref[s, pl.ds(c, HALF, stride=2), :] = state[
                s * HALF : (s + 1) * HALF, c * SIDE : (c + 1) * SIDE
            ]
        o_ref[:, :, s * SIDE : (s + 1) * SIDE] = rows_ref[s].astype(BF).reshape(HALF, 2, SIDE)


def on_device(
    tokens,
    w_value,
    w_first,
    w_second,
    short_taps,
    filter_in,
    filter_mid,
    filter_out,
    decay_rate,
    skip_gain,
    w_output,
):
    seqs, tok_rows, _ = tokens.shape
    blocks = lax.axis_size(ROW)
    length = tok_rows * blocks
    feats = filter_in.shape[0]
    waves, turns, real_all, rights, backs, ends = (jnp.asarray(t) for t in tables(length, feats))
    far = pl.BlockSpec(memory_space=pltpu.HBM)
    vmem = pl.BlockSpec(memory_space=pltpu.VMEM)
    steps = 2
    pieces = pl.pallas_call(
        functools.partial(project_kernel, steps),
        out_shape=jax.ShapeDtypeStruct((blocks, 4, 3 * tok_rows), BF),
        in_specs=[far] * 4,
        out_specs=vmem,
        scratch_shapes=[
            pltpu.VMEM((seqs * tok_rows, tokens.shape[2]), BF),
            pltpu.VMEM((tokens.shape[2], 3 * SIDE), BF),
            pltpu.VMEM((seqs * tok_rows, 3 * SIDE), F32),
            pltpu.SemaphoreType.DMA((steps, 5)),
        ],
        compiler_params=pltpu.CompilerParams(vmem_limit_bytes=66_700_000),
        name="project",
    )(tokens, w_value, w_first, w_second)
    arrived = lax.all_to_all(pieces, ROW, 0, 0, tiled=True)

    spec = jax.ShapeDtypeStruct((2, 2 * SIDE, SIDE), F32)
    units = filter_in.shape[1]
    rows, factor = pl.pallas_call(
        network_kernel,
        out_shape=(
            jax.ShapeDtypeStruct((8 * HALF, SIDE), F32),
            jax.ShapeDtypeStruct((8, SIDE), F32),
        ),
        in_specs=[vmem] * 5,
        out_specs=(vmem, vmem),
        scratch_shapes=[pltpu.VMEM((32, units), F32)],
        compiler_params=pltpu.CompilerParams(vmem_limit_bytes=16 * 2**20),
        cost_estimate=pl.CostEstimate(
            flops=4_000_000_000, bytes_accessed=1_000_000, transcendentals=0
        ),
        name="network",
    )(
        waves,
        filter_in,
        filter_mid,
        filter_out.reshape(4 * units, -1),
        decay_rate.reshape(1, -1),
    )
    spec_re, spec_im, coef = pl.pallas_call(
        spectra_kernel,
        out_shape=(spec, spec, jax.ShapeDtypeStruct((3, 8, 2 * SIDE), F32)),
        in_specs=[vmem] * 7,
        out_specs=(vmem,) * 3,
        compiler_params=pltpu.CompilerParams(vmem_limit_bytes=16 * 2**20),
        cost_estimate=pl.CostEstimate(
            flops=1_000_000_000, bytes_accessed=2_000_000, transcendentals=0
        ),
        name="spectra",
    )(rows, factor, turns, real_all, rights, short_taps, skip_gain)
    gated = pl.pallas_call(
        conv_kernel,
        out_shape=jax.ShapeDtypeStruct((blocks, 2, seqs * tok_rows), BF),
        in_specs=[vmem] * 8,
        out_specs=vmem,
        scratch_shapes=[
            pltpu.VMEM((6, SIDE, SIDE), F32),
        ],
        compiler_params=pltpu.CompilerParams(vmem_limit_bytes=16 * 2**20),
        cost_estimate=pl.CostEstimate(
            flops=4_000_000_000, bytes_accessed=2_000_000, transcendentals=0
        ),
        name="gated_conv",
    )(
        arrived,
        coef,
        spec_re,
        spec_im,
        turns,
        rights,
        backs,
        ends,
    )
    returned = lax.all_to_all(gated, ROW, 0, 0, tiled=True)
    returned = returned.reshape(2 * blocks, seqs * tok_rows)
    everyone = lax.all_to_all(
        jnp.broadcast_to(returned[None], (lax.axis_size("x"), *returned.shape)), "x", 0, 0, tiled=True
    )
    everyone = lax.all_gather(everyone, "core", axis=1)
    everyone = everyone.reshape(-1, seqs * tok_rows)
    result = jnp.einsum("ct,cd->td", everyone, w_output, preferred_element_type=F32)
    return result.astype(BF).reshape(seqs, tok_rows, -1)


def solution(mesh):
    torus = Mesh(mesh.devices.reshape(8, 8, 4, 2), ("row_0", "row_1", "x", "core"))
    in_specs = (
        P(None, ROW, None),
        P(None, COL),
        P(None, COL),
        P(None, COL),
        P(None, None, COL),
        P(),
        P(),
        P(None, None, None, COL),
        P(COL),
        P(None, COL),
        P(None, COL),
    )
    out_specs = P(None, ROW, COL)
    return jax.shard_map(
        on_device, mesh=torus, in_specs=in_specs, out_specs=out_specs, check_vma=False
    )
```

```python
import functools
import math

import jax
import jax.numpy as jnp
import numpy as np
from jax import lax
from jax.experimental import pallas as pl
from jax.experimental.pallas import tpu as pltpu
from jax.sharding import Mesh
from jax.sharding import PartitionSpec as P

ROW = ("row_0", "row_1")
COL = ("x", "core")
SIDE = 128
HALF = SIDE // 2
CHUNK = 4096
ROOT = 44
BF = jnp.bfloat16
F32 = jnp.float32


def halves(table):
    table = np.asarray(table, np.float32)
    top = table.astype(jnp.bfloat16)
    return top, (table - top.astype(np.float32)).astype(jnp.bfloat16)


@functools.lru_cache(None)
def tables(length, feats):
    bands = (feats - 1) // 2
    freq = np.linspace(0.0001, bands - 1, bands)[:, None] * (2.0 * math.pi / length)
    coarse, near = freq * np.arange(SIDE) * SIDE, freq * np.arange(SIDE)
    waves = np.stack([np.cos(coarse), np.sin(coarse), np.cos(near), np.sin(near)])
    index = np.arange(SIDE)
    turn = 2.0 * math.pi / SIDE * (index[:, None] * index[None, :] % SIDE)
    cos, sin = np.cos(turn), np.sin(turn)
    fine = 2.0 * math.pi / (SIDE * SIDE) * (index[:, None] * index[None, :])
    pair_in = np.block([[cos[:, :HALF], sin[:, :HALF]], [-sin[:, :HALF], cos[:, :HALF]]])
    right = np.block([[cos, -sin], [sin, cos]])
    in_hi, in_lo = halves(pair_in)
    out_hi, out_lo = halves(pair_in.T)
    right_hi, right_lo = halves(right)
    back_hi, back_lo = halves(right.T)
    real_hi, real_lo = in_hi[:, :HALF], in_lo[:, :HALF]
    real_all = np.concatenate([real_hi, real_lo, real_hi, np.zeros_like(real_hi)], axis=1)
    rights = np.concatenate([right_hi, right_lo])
    backs = np.concatenate([back_hi, back_lo])
    ends = np.concatenate([np.concatenate([in_hi, in_lo], axis=1), out_hi, out_lo])
    turns = np.concatenate([np.cos(fine), np.sin(fine)]).astype(np.float32)
    return np.concatenate(waves).astype(np.float32), turns, real_all, rights, backs, ends


def hi_lo(value):
    top = value.astype(BF)
    return top, (value - top.astype(F32)).astype(BF)


def mm(a, b, dims=(((1,), (0,)), ((), ()))):
    return lax.dot_general(a, b, dims, preferred_element_type=F32)


def left_const(const_hi, const_lo, value):
    top, low = hi_lo(value)
    return mm(const_hi, top) + mm(const_lo, top) + mm(const_hi, low)


def right_const(value, const_hi, const_lo):
    top, low = hi_lo(value)
    return mm(top, const_hi) + mm(low, const_hi) + mm(top, const_lo)


def sine_of_turns(moved):
    moved = moved - jnp.round(moved)
    quarter = 0.25 - jnp.abs(moved)
    square = quarter * quarter
    poly = -70.98993302 * square + 81.34038614
    poly = poly * square - 41.33713041
    poly = poly * square + 6.28316395
    return poly * quarter


def project_kernel(
    steps, tok_hbm, a_hbm, b_hbm, c_hbm, o_ref, tok, weights, sum_ref, sems
):
    depth = tok.shape[1] // steps

    def group_of(step, cut):
        group = []
        for s in range(2):
            group.append((tok_hbm.at[s, :, cut], tok.at[pl.ds(s * SIDE, SIDE), cut]))
        for p, source in enumerate((a_hbm, b_hbm, c_hbm)):
            group.append((source.at[cut, :], weights.at[cut, pl.ds(p * SIDE, SIDE)]))
        return [
            pltpu.make_async_copy(near, far, sems.at[step, k]) for k, (near, far) in enumerate(group)
        ]

    for step in range(steps):
        for copy in group_of(step, pl.ds(step * depth, depth)):
            copy.start()
    for step in range(steps):
        for copy in group_of(step, pl.ds(step * depth, depth)):
            copy.wait()
        cut = slice(step * depth, (step + 1) * depth)
        part = mm(tok[:, cut], weights[cut, :])
        if step < steps - 1:
            sum_ref[...] = part if step == 0 else sum_ref[...] + part
    part += sum_ref[...]
    for p in range(3):
        cut = slice(p * SIDE, (p + 1) * SIDE)
        for s in range(2):
            turned = part[s * SIDE : (s + 1) * SIDE, cut].T
            o_ref[:, 2 * s : 2 * s + 2, cut] = turned.astype(BF).reshape(HALF, 2, SIDE)


def network_kernel(
    waves_ref, in_ref, mid_ref, out_ref, rate_ref, rows_ref, factor_ref, side_ref
):
    length = HALF * SIDE
    device = lax.axis_index("row_0") * lax.axis_size("row_1") + lax.axis_index("row_1")
    device = (device + (HALF - ROOT)) % HALF
    lane = lax.broadcasted_iota(jnp.int32, (8, SIDE), 1)
    row = lax.broadcasted_iota(jnp.int32, (8, SIDE), 0)
    mine = lane == 2 * device + row % 2
    last = (((1,), (1,)), ((), ()))
    first = (((0,), (0,)), ((), ()))
    units = mid_ref.shape[0]
    out_hi = jnp.zeros((8, units), F32)
    out_lo = jnp.zeros((8, units), F32)
    for pair in range(4):
        pick = jnp.where(mine & (row // 2 == pair), 1.0, 0.0).astype(BF)
        top, low = hi_lo(out_ref[pl.ds(pair, units, stride=4), :])
        out_hi += mm(pick, top, last)
        out_lo += mm(pick, low, last)
    out_hi, out_lo = out_hi.astype(BF), out_lo.astype(BF)
    out_all = jnp.concatenate([out_hi, out_lo, out_hi], axis=1)
    rate = jnp.sum(jnp.where(mine, rate_ref[...], 0.0), axis=1, keepdims=True)
    scale = 1.0 / (2.0 * math.pi)
    side_ref[...] = jnp.zeros_like(side_ref)
    ramp_hi, ramp_lo = hi_lo(in_ref[0:1, :] * scale)
    side_ref[0:1, :] = ramp_hi.astype(F32)
    side_ref[1:2, :] = ramp_lo.astype(F32)
    side_ref[2:3, :] = ramp_hi.astype(F32)
    side_ref[3:4, :] = jnp.full((1, units), -0.25, F32)
    side_ref[16:17, :] = jnp.full((1, units), -0.25, F32)
    in_hi, in_lo = hi_lo(in_ref[1:33, :] * scale)
    in_all = jnp.concatenate([in_hi, in_lo, in_hi, side_ref[0:16, :].astype(BF)], axis=0)
    mid_hi, mid_lo = hi_lo(mid_ref[...] * scale)
    mid_all = jnp.concatenate([mid_hi, mid_lo, mid_hi, side_ref[16:32, :].astype(BF)], axis=0)
    chunk = CHUNK
    cos_far, sin_far, cos_near, sin_near = (
        waves_ref[16 * k : 16 * (k + 1), :] for k in range(4)
    )
    ones = jnp.ones((16, chunk), BF)
    sign = jnp.where(row < 4, 1.0, -1.0)
    squares = jnp.zeros((8, SIDE), F32)
    blocks = chunk // SIDE
    for start in range(0, HALF, blocks):
        pieces, sides = [], []
        for block in range(start, start + blocks):
            far_c, far_s = cos_far[:, block : block + 1], sin_far[:, block : block + 1]
            pieces.append(
                jnp.concatenate(
                    [
                        far_c * cos_near - far_s * sin_near,
                        -(far_s * cos_near + far_c * sin_near),
                    ],
                    axis=0,
                )
            )
            ramp = (lane + block * SIDE).astype(F32) * (1.0 / (length - 1))
            ramp_top = ramp.astype(BF).astype(F32)
            ramp = jnp.where(row == 2, ramp - ramp_top, jnp.where(row < 2, ramp_top, 1.0))
            sides.append(jnp.concatenate([ramp, jnp.zeros_like(ramp)], axis=0).astype(BF))
        top, low = hi_lo(jnp.concatenate(pieces, axis=1))
        side = jnp.concatenate(sides, axis=1)
        moved = mm(in_all, jnp.concatenate([top, top, low, side], axis=0), first)
        top, low = hi_lo(sine_of_turns(moved))
        moved = mm(mid_all, jnp.concatenate([top, top, low, ones], axis=0), first)
        top, low = hi_lo(sine_of_turns(moved))
        shaped = mm(out_all, jnp.concatenate([top, top, low], axis=0))
        for piece in range(blocks):
            block = start + piece
            lag = lane + block * SIDE
            part = shaped[:, piece * SIDE : (piece + 1) * SIDE] * jnp.exp(-rate * lag.astype(F32))
            if block == 0:
                part = jnp.where((row >= 4) & (lag == 0), 0.0, part)
            squares += part * part
            rows_ref[block * 8 : (block + 1) * 8, :] = pltpu.roll(part, 4, 0) + part * sign
    total = jnp.sum(squares + pltpu.roll(squares, 4, 0), axis=1, keepdims=True)
    factor = lax.rsqrt(total + 1e-06) * (1.0 / (SIDE * SIDE))
    factor_ref[...] = jnp.broadcast_to(factor, factor_ref.shape)


def spectra_kernel(
    rows_ref, factor_ref, turns_ref, real_ref, right_ref, taps_ref, gain_ref,
    spec_re_ref, spec_im_ref, coef_ref,
):
    device = lax.axis_index("row_0") * lax.axis_size("row_1") + lax.axis_index("row_1")
    device = (device + (HALF - ROOT)) % HALF
    sources = [(tap, taps_ref[tap], 0) for tap in range(3)] + [(3, gain_ref[...], 1)]
    for c in range(2):
        for at, source, shift in sources:
            count = source.shape[0]
            at_lane = lax.broadcasted_iota(jnp.int32, (count, SIDE), 1) == 2 * device + c
            value = jnp.sum(jnp.where(at_lane, source, 0.0), axis=1, keepdims=True)
            value = jnp.broadcast_to(value, (count, SIDE))
            for k in range(count):
                coef_ref[k + shift, at : at + 1, c * SIDE : (c + 1) * SIDE] = value[k : k + 1]
    pieces = []
    for j in range(8):
        pieces.append(rows_ref[pl.ds(j, HALF, stride=8), :] * factor_ref[j : j + 1, :])
    top, low = hi_lo(jnp.concatenate(pieces, axis=1))
    grid = mm(real_ref[:, : 3 * HALF], jnp.concatenate([top, top, low], axis=0))
    cos, sin = turns_ref[:SIDE, :], turns_ref[SIDE:, :]

    def turned(j):
        real = grid[:SIDE, j * SIDE : (j + 1) * SIDE]
        imag = grid[SIDE:, j * SIDE : (j + 1) * SIDE]
        return jnp.concatenate([real * cos + imag * sin, imag * cos - real * sin], axis=1)

    for j in range(4):
        rows = pl.ds(j % 2 * SIDE, SIDE)
        spec_re_ref[j // 2, rows, :] = right_const(
            turned(j), right_ref[: 2 * SIDE, :SIDE], right_ref[2 * SIDE :, :SIDE]
        )
        spec_im_ref[j // 2, rows, :] = right_const(
            turned(j + 4), right_ref[: 2 * SIDE, SIDE:], right_ref[2 * SIDE :, SIDE:]
        )


def conv_kernel(
    x_ref, coef_ref, spec_re_ref, spec_im_ref, turns_ref, right_ref, back_ref, ends_ref,
    o_ref, rows_ref,
):
    for p in range(3):
        for s in range(2):
            piece = x_ref[:, 2 * s : 2 * s + 2, p * SIDE : (p + 1) * SIDE]
            piece = jnp.concatenate([piece[HALF - ROOT :], piece[: HALF - ROOT]], axis=0)
            rows_ref[2 * p + s] = piece.reshape(SIDE, SIDE).astype(F32)
    row = lax.broadcasted_iota(jnp.int32, (HALF, SIDE), 0)
    lane = lax.broadcasted_iota(jnp.int32, (HALF, SIDE), 1)

    def smoothed(p):
        seqs = []
        for s in range(2):
            chans = []
            for c in range(2):
                here = rows_ref[2 * p + s, pl.ds(c, HALF, stride=2), :]
                moved = pltpu.roll(here, 1, 1)
                prev = jnp.where(lane == 0, pltpu.roll(moved, 1, 0), moved)
                prev = jnp.where((lane == 0) & (row == 0), 0.0, prev)
                moved = pltpu.roll(here, SIDE - 1, 1)
                after = jnp.where(lane == SIDE - 1, pltpu.roll(moved, HALF - 1, 0), moved)
                after = jnp.where((lane == SIDE - 1) & (row == HALF - 1), 0.0, after)
                first, second, third = (
                    coef_ref[p, tap : tap + 1, c * SIDE : (c + 1) * SIDE] for tap in range(3)
                )
                chans.append(first * prev + second * here + third * after)
            seqs.append(jnp.concatenate(chans, axis=1))
        return jnp.concatenate(seqs, axis=0)

    cos, sin = turns_ref[:SIDE, :], turns_ref[SIDE:, :]
    cos2, sin2 = jnp.concatenate([cos, cos], axis=1), jnp.concatenate([sin, sin], axis=1)

    def one_order(order, state):
        top, low = hi_lo(state)
        grid = mm(ends_ref[: 2 * SIDE, :], jnp.concatenate([top, top], axis=0))
        grid += mm(ends_ref[: 2 * SIDE, :SIDE], low)
        reals, imags = [], []
        for c in range(2):
            cut = slice(c * SIDE, (c + 1) * SIDE)
            real, imag = grid[:SIDE, cut], grid[SIDE:, cut]
            pair = jnp.concatenate([real * cos + imag * sin, imag * cos - real * sin], axis=1)
            pair = right_const(pair, right_ref[: 2 * SIDE, :], right_ref[2 * SIDE :, :])
            real, imag = pair[:, :SIDE], pair[:, SIDE:]
            k_re, k_im = spec_re_ref[order, cut, :], spec_im_ref[order, cut, :]
            pair = jnp.concatenate([real * k_re - imag * k_im, real * k_im + imag * k_re], axis=1)
            pair = right_const(pair, back_ref[: 2 * SIDE, :], back_ref[2 * SIDE :, :])
            real, imag = pair[:, :SIDE], pair[:, SIDE:]
            reals.append(real * cos - imag * sin)
            imags.append(real * sin + imag * cos)
        grid = jnp.concatenate(
            [jnp.concatenate(reals, axis=1), jnp.concatenate(imags, axis=1)], axis=0
        )
        reach = left_const(ends_ref[2 * SIDE : 3 * SIDE, :], ends_ref[3 * SIDE :, :], grid)
        return smoothed(order + 1) * (reach + coef_ref[order + 1, 3:4, :] * state)

    state = one_order(1, one_order(0, smoothed(0)))
    for s in range(2):
        for c in range(2):
            rows_ref[s, pl.ds(c, HALF, stride=2), :] = state[
                s * HALF : (s + 1) * HALF, c * SIDE : (c + 1) * SIDE
            ]
        piece = rows_ref[s].astype(BF).reshape(HALF, 2, SIDE)
        piece = jnp.concatenate([piece[ROOT:], piece[:ROOT]], axis=0)
        o_ref[:, :, s * SIDE : (s + 1) * SIDE] = piece


def on_device(
    tokens,
    w_value,
    w_first,
    w_second,
    short_taps,
    filter_in,
    filter_mid,
    filter_out,
    decay_rate,
    skip_gain,
    w_output,
):
    seqs, tok_rows, _ = tokens.shape
    blocks = lax.axis_size(ROW)
    length = tok_rows * blocks
    feats = filter_in.shape[0]
    waves, turns, real_all, rights, backs, ends = (jnp.asarray(t) for t in tables(length, feats))
    far = pl.BlockSpec(memory_space=pltpu.HBM)
    vmem = pl.BlockSpec(memory_space=pltpu.VMEM)
    steps = 2
    pieces = pl.pallas_call(
        functools.partial(project_kernel, steps),
        out_shape=jax.ShapeDtypeStruct((blocks, 4, 3 * tok_rows), BF),
        in_specs=[far] * 4,
        out_specs=vmem,
        scratch_shapes=[
            pltpu.VMEM((seqs * tok_rows, tokens.shape[2]), BF),
            pltpu.VMEM((tokens.shape[2], 3 * SIDE), BF),
            pltpu.VMEM((seqs * tok_rows, 3 * SIDE), F32),
            pltpu.SemaphoreType.DMA((steps, 5)),
        ],
        compiler_params=pltpu.CompilerParams(vmem_limit_bytes=66_700_000),
        name="project",
    )(tokens, w_value, w_first, w_second)
    members = [[(i + ROOT) % blocks for i in range(blocks)]]
    arrived = lax.all_to_all(pieces, ROW, 0, 0, tiled=True, axis_index_groups=members)

    spec = jax.ShapeDtypeStruct((2, 2 * SIDE, SIDE), F32)
    units = filter_in.shape[1]
    rows, factor = pl.pallas_call(
        network_kernel,
        out_shape=(
            jax.ShapeDtypeStruct((8 * HALF, SIDE), F32),
            jax.ShapeDtypeStruct((8, SIDE), F32),
        ),
        in_specs=[vmem] * 5,
        out_specs=(vmem, vmem),
        scratch_shapes=[pltpu.VMEM((32, units), F32)],
        compiler_params=pltpu.CompilerParams(vmem_limit_bytes=16 * 2**20),
        cost_estimate=pl.CostEstimate(
            flops=4_000_000_000, bytes_accessed=1_000_000, transcendentals=0
        ),
        name="network",
    )(
        waves,
        filter_in,
        filter_mid,
        filter_out.reshape(4 * units, -1),
        decay_rate.reshape(1, -1),
    )
    spec_re, spec_im, coef = pl.pallas_call(
        spectra_kernel,
        out_shape=(spec, spec, jax.ShapeDtypeStruct((3, 8, 2 * SIDE), F32)),
        in_specs=[vmem] * 7,
        out_specs=(vmem,) * 3,
        compiler_params=pltpu.CompilerParams(vmem_limit_bytes=16 * 2**20),
        cost_estimate=pl.CostEstimate(
            flops=1_000_000_000, bytes_accessed=2_000_000, transcendentals=0
        ),
        name="spectra",
    )(rows, factor, turns, real_all, rights, short_taps, skip_gain)
    gated = pl.pallas_call(
        conv_kernel,
        out_shape=jax.ShapeDtypeStruct((blocks, 2, seqs * tok_rows), BF),
        in_specs=[vmem] * 8,
        out_specs=vmem,
        scratch_shapes=[
            pltpu.VMEM((6, SIDE, SIDE), F32),
        ],
        compiler_params=pltpu.CompilerParams(vmem_limit_bytes=16 * 2**20),
        cost_estimate=pl.CostEstimate(
            flops=4_000_000_000, bytes_accessed=2_000_000, transcendentals=0
        ),
        name="gated_conv",
    )(
        arrived,
        coef,
        spec_re,
        spec_im,
        turns,
        rights,
        backs,
        ends,
    )
    returned = lax.all_to_all(gated, ROW, 0, 0, tiled=True, axis_index_groups=members)
    returned = returned.reshape(2 * blocks, seqs * tok_rows)
    everyone = lax.all_to_all(
        jnp.broadcast_to(returned[None], (lax.axis_size("x"), *returned.shape)), "x", 0, 0, tiled=True
    )
    everyone = lax.all_gather(everyone, "core", axis=1)
    everyone = everyone.reshape(-1, seqs * tok_rows)
    result = jnp.einsum("ct,cd->td", everyone, w_output, preferred_element_type=F32)
    return result.astype(BF).reshape(seqs, tok_rows, -1)


def solution(mesh):
    torus = Mesh(mesh.devices.reshape(8, 8, 4, 2), ("row_0", "row_1", "x", "core"))
    in_specs = (
        P(None, ROW, None),
        P(None, COL),
        P(None, COL),
        P(None, COL),
        P(None, None, COL),
        P(),
        P(),
        P(None, None, None, COL),
        P(COL),
        P(None, COL),
        P(None, COL),
    )
    out_specs = P(None, ROW, COL)
    return jax.shard_map(
        on_device, mesh=torus, in_specs=in_specs, out_specs=out_specs, check_vma=False
    )
```

```python
import functools
import math

import jax
import jax.numpy as jnp
import numpy as np
from jax import lax
from jax.experimental import pallas as pl
from jax.experimental.pallas import tpu as pltpu
from jax.sharding import Mesh
from jax.sharding import PartitionSpec as P

ROW = ("row_0", "row_1")
COL = ("x", "core")
SIDE = 128
HALF = SIDE // 2
CHUNK = 4096
PLANE = 2
ROOT = 44
BF = jnp.bfloat16
F32 = jnp.float32


def halves(table):
    table = np.asarray(table, np.float32)
    top = table.astype(jnp.bfloat16)
    return top, (table - top.astype(np.float32)).astype(jnp.bfloat16)


@functools.lru_cache(None)
def tables(length, feats):
    bands = (feats - 1) // 2
    freq = np.linspace(0.0001, bands - 1, bands)[:, None] * (2.0 * math.pi / length)
    coarse, near = freq * np.arange(SIDE) * SIDE, freq * np.arange(SIDE)
    waves = np.stack([np.cos(coarse), np.sin(coarse), np.cos(near), np.sin(near)])
    index = np.arange(SIDE)
    turn = 2.0 * math.pi / SIDE * (index[:, None] * index[None, :] % SIDE)
    cos, sin = np.cos(turn), np.sin(turn)
    fine = 2.0 * math.pi / (SIDE * SIDE) * (index[:, None] * index[None, :])
    pair_in = np.block([[cos[:, :HALF], sin[:, :HALF]], [-sin[:, :HALF], cos[:, :HALF]]])
    right = np.block([[cos, -sin], [sin, cos]])
    in_hi, in_lo = halves(pair_in)
    out_hi, out_lo = halves(pair_in.T)
    right_hi, right_lo = halves(right)
    back_hi, back_lo = halves(right.T)
    real_hi, real_lo = in_hi[:, :HALF], in_lo[:, :HALF]
    real_all = np.concatenate([real_hi, real_lo, real_hi, np.zeros_like(real_hi)], axis=1)
    rights = np.concatenate([right_hi, right_lo])
    backs = np.concatenate([back_hi, back_lo])
    ends = np.concatenate([np.concatenate([in_hi, in_lo], axis=1), out_hi, out_lo])
    turns = np.concatenate([np.cos(fine), np.sin(fine)]).astype(np.float32)
    return np.concatenate(waves).astype(np.float32), turns, real_all, rights, backs, ends


def hi_lo(value):
    top = value.astype(BF)
    return top, (value - top.astype(F32)).astype(BF)


def mm(a, b, dims=(((1,), (0,)), ((), ()))):
    return lax.dot_general(a, b, dims, preferred_element_type=F32)


def left_const(const_hi, const_lo, value):
    top, low = hi_lo(value)
    return mm(const_hi, top) + mm(const_lo, top) + mm(const_hi, low)


def right_const(value, const_hi, const_lo):
    top, low = hi_lo(value)
    return mm(top, const_hi) + mm(low, const_hi) + mm(top, const_lo)


def sine_of_turns(moved):
    moved = moved - jnp.round(moved)
    quarter = 0.25 - jnp.abs(moved)
    square = quarter * quarter
    poly = -70.98993302 * square + 81.34038614
    poly = poly * square - 41.33713041
    poly = poly * square + 6.28316395
    return poly * quarter


def project_kernel(
    steps, tok_hbm, a_hbm, b_hbm, c_hbm, o_ref, tok, weights, sum_ref, sems
):
    depth = tok.shape[1] // steps

    def group_of(step, cut):
        group = []
        for s in range(2):
            group.append((tok_hbm.at[s, :, cut], tok.at[pl.ds(s * SIDE, SIDE), cut]))
        for p, source in enumerate((a_hbm, b_hbm, c_hbm)):
            group.append((source.at[cut, :], weights.at[cut, pl.ds(p * SIDE, SIDE)]))
        return [
            pltpu.make_async_copy(near, far, sems.at[step, k]) for k, (near, far) in enumerate(group)
        ]

    for step in range(steps):
        for copy in group_of(step, pl.ds(step * depth, depth)):
            copy.start()
    for step in range(steps):
        for copy in group_of(step, pl.ds(step * depth, depth)):
            copy.wait()
        cut = slice(step * depth, (step + 1) * depth)
        part = mm(tok[:, cut], weights[cut, :])
        if step < steps - 1:
            sum_ref[...] = part if step == 0 else sum_ref[...] + part
    part += sum_ref[...]
    for p in range(3):
        cut = slice(p * SIDE, (p + 1) * SIDE)
        for s in range(2):
            turned = part[s * SIDE : (s + 1) * SIDE, cut].T
            o_ref[:, 2 * s : 2 * s + 2, cut] = turned.astype(BF).reshape(HALF, 2, SIDE)


def network_kernel(
    waves_ref, in_ref, mid_ref, out_ref, rate_ref, rows_ref, factor_ref, side_ref
):
    length = HALF * SIDE
    device = lax.axis_index("row_0") * lax.axis_size("row_1") + lax.axis_index("row_1")
    device = (device + (HALF - ROOT)) % HALF
    lane = lax.broadcasted_iota(jnp.int32, (8, SIDE), 1)
    row = lax.broadcasted_iota(jnp.int32, (8, SIDE), 0)
    mine = lane == 2 * device + row % 2
    last = (((1,), (1,)), ((), ()))
    first = (((0,), (0,)), ((), ()))
    units = mid_ref.shape[0]
    out_hi = jnp.zeros((8, units), F32)
    out_lo = jnp.zeros((8, units), F32)
    for pair in range(4):
        pick = jnp.where(mine & (row // 2 == pair), 1.0, 0.0).astype(BF)
        top, low = hi_lo(out_ref[pl.ds(pair, units, stride=4), :])
        out_hi += mm(pick, top, last)
        out_lo += mm(pick, low, last)
    out_hi, out_lo = out_hi.astype(BF), out_lo.astype(BF)
    out_all = jnp.concatenate([out_hi, out_lo, out_hi], axis=1)
    rate = jnp.sum(jnp.where(mine, rate_ref[...], 0.0), axis=1, keepdims=True)
    scale = 1.0 / (2.0 * math.pi)
    side_ref[...] = jnp.zeros_like(side_ref)
    ramp_hi, ramp_lo = hi_lo(in_ref[0:1, :] * scale)
    side_ref[0:1, :] = ramp_hi.astype(F32)
    side_ref[1:2, :] = ramp_lo.astype(F32)
    side_ref[2:3, :] = ramp_hi.astype(F32)
    side_ref[3:4, :] = jnp.full((1, units), -0.25, F32)
    side_ref[16:17, :] = jnp.full((1, units), -0.25, F32)
    in_hi, in_lo = hi_lo(in_ref[1:33, :] * scale)
    in_all = jnp.concatenate([in_hi, in_lo, in_hi, side_ref[0:16, :].astype(BF)], axis=0)
    mid_hi, mid_lo = hi_lo(mid_ref[...] * scale)
    mid_all = jnp.concatenate([mid_hi, mid_lo, mid_hi, side_ref[16:32, :].astype(BF)], axis=0)
    chunk = CHUNK
    cos_far, sin_far, cos_near, sin_near = (
        waves_ref[16 * k : 16 * (k + 1), :] for k in range(4)
    )
    ones = jnp.ones((16, chunk), BF)
    sign = jnp.where(row < 4, 1.0, -1.0)
    squares = jnp.zeros((8, SIDE), F32)
    blocks = chunk // SIDE
    for start in range(0, HALF, blocks):
        pieces, sides = [], []
        for block in range(start, start + blocks):
            far_c, far_s = cos_far[:, block : block + 1], sin_far[:, block : block + 1]
            pieces.append(
                jnp.concatenate(
                    [
                        far_c * cos_near - far_s * sin_near,
                        -(far_s * cos_near + far_c * sin_near),
                    ],
                    axis=0,
                )
            )
            ramp = (lane + block * SIDE).astype(F32) * (1.0 / (length - 1))
            ramp_top = ramp.astype(BF).astype(F32)
            ramp = jnp.where(row == 2, ramp - ramp_top, jnp.where(row < 2, ramp_top, 1.0))
            sides.append(jnp.concatenate([ramp, jnp.zeros_like(ramp)], axis=0).astype(BF))
        top, low = hi_lo(jnp.concatenate(pieces, axis=1))
        side = jnp.concatenate(sides, axis=1)
        moved = mm(in_all, jnp.concatenate([top, top, low, side], axis=0), first)
        top, low = hi_lo(sine_of_turns(moved))
        moved = mm(mid_all, jnp.concatenate([top, top, low, ones], axis=0), first)
        top, low = hi_lo(sine_of_turns(moved))
        shaped = mm(out_all, jnp.concatenate([top, top, low], axis=0))
        for piece in range(blocks):
            block = start + piece
            lag = lane + block * SIDE
            part = shaped[:, piece * SIDE : (piece + 1) * SIDE] * jnp.exp(-rate * lag.astype(F32))
            if block == 0:
                part = jnp.where((row >= 4) & (lag == 0), 0.0, part)
            squares += part * part
            rows_ref[block * 8 : (block + 1) * 8, :] = pltpu.roll(part, 4, 0) + part * sign
    total = jnp.sum(squares + pltpu.roll(squares, 4, 0), axis=1, keepdims=True)
    factor = lax.rsqrt(total + 1e-06) * (1.0 / (SIDE * SIDE))
    factor_ref[...] = jnp.broadcast_to(factor, factor_ref.shape)


def spectra_kernel(
    rows_ref, factor_ref, turns_ref, real_ref, right_ref, taps_ref, gain_ref,
    spec_re_ref, spec_im_ref, coef_ref,
):
    device = lax.axis_index("row_0") * lax.axis_size("row_1") + lax.axis_index("row_1")
    device = (device + (HALF - ROOT)) % HALF
    sources = [(tap, taps_ref[tap], 0) for tap in range(3)] + [(3, gain_ref[...], 1)]
    for c in range(2):
        for at, source, shift in sources:
            count = source.shape[0]
            at_lane = lax.broadcasted_iota(jnp.int32, (count, SIDE), 1) == 2 * device + c
            value = jnp.sum(jnp.where(at_lane, source, 0.0), axis=1, keepdims=True)
            value = jnp.broadcast_to(value, (count, SIDE))
            for k in range(count):
                coef_ref[k + shift, at : at + 1, c * SIDE : (c + 1) * SIDE] = value[k : k + 1]
    pieces = []
    for j in range(8):
        pieces.append(rows_ref[pl.ds(j, HALF, stride=8), :] * factor_ref[j : j + 1, :])
    top, low = hi_lo(jnp.concatenate(pieces, axis=1))
    grid = mm(real_ref[:, : 3 * HALF], jnp.concatenate([top, top, low], axis=0))
    cos, sin = turns_ref[:SIDE, :], turns_ref[SIDE:, :]

    def turned(j):
        real = grid[:SIDE, j * SIDE : (j + 1) * SIDE]
        imag = grid[SIDE:, j * SIDE : (j + 1) * SIDE]
        return jnp.concatenate([real * cos + imag * sin, imag * cos - real * sin], axis=1)

    for j in range(4):
        rows = pl.ds(j % 2 * SIDE, SIDE)
        spec_re_ref[j // 2, rows, :] = right_const(
            turned(j), right_ref[: 2 * SIDE, :SIDE], right_ref[2 * SIDE :, :SIDE]
        )
        spec_im_ref[j // 2, rows, :] = right_const(
            turned(j + 4), right_ref[: 2 * SIDE, SIDE:], right_ref[2 * SIDE :, SIDE:]
        )


def conv_kernel(
    x_ref, coef_ref, spec_re_ref, spec_im_ref, turns_ref, right_ref, back_ref, ends_ref,
    o_ref, rows_ref,
):
    for p in range(3):
        for s in range(2):
            piece = x_ref[:, 2 * s : 2 * s + 2, p * SIDE : (p + 1) * SIDE]
            piece = jnp.concatenate([piece[HALF - ROOT :], piece[: HALF - ROOT]], axis=0)
            rows_ref[2 * p + s] = piece.reshape(SIDE, SIDE).astype(F32)
    row = lax.broadcasted_iota(jnp.int32, (HALF, SIDE), 0)
    lane = lax.broadcasted_iota(jnp.int32, (HALF, SIDE), 1)

    def smoothed(p):
        seqs = []
        for s in range(2):
            chans = []
            for c in range(2):
                here = rows_ref[2 * p + s, pl.ds(c, HALF, stride=2), :]
                moved = pltpu.roll(here, 1, 1)
                prev = jnp.where(lane == 0, pltpu.roll(moved, 1, 0), moved)
                prev = jnp.where((lane == 0) & (row == 0), 0.0, prev)
                moved = pltpu.roll(here, SIDE - 1, 1)
                after = jnp.where(lane == SIDE - 1, pltpu.roll(moved, HALF - 1, 0), moved)
                after = jnp.where((lane == SIDE - 1) & (row == HALF - 1), 0.0, after)
                first, second, third = (
                    coef_ref[p, tap : tap + 1, c * SIDE : (c + 1) * SIDE] for tap in range(3)
                )
                chans.append(first * prev + second * here + third * after)
            seqs.append(jnp.concatenate(chans, axis=1))
        return jnp.concatenate(seqs, axis=0)

    cos, sin = turns_ref[:SIDE, :], turns_ref[SIDE:, :]
    cos2, sin2 = jnp.concatenate([cos, cos], axis=1), jnp.concatenate([sin, sin], axis=1)

    def one_order(order, state):
        top, low = hi_lo(state)
        grid = mm(ends_ref[: 2 * SIDE, :], jnp.concatenate([top, top], axis=0))
        grid += mm(ends_ref[: 2 * SIDE, :SIDE], low)
        reals, imags = [], []
        for c in range(2):
            cut = slice(c * SIDE, (c + 1) * SIDE)
            real, imag = grid[:SIDE, cut], grid[SIDE:, cut]
            pair = jnp.concatenate([real * cos + imag * sin, imag * cos - real * sin], axis=1)
            pair = right_const(pair, right_ref[: 2 * SIDE, :], right_ref[2 * SIDE :, :])
            real, imag = pair[:, :SIDE], pair[:, SIDE:]
            k_re, k_im = spec_re_ref[order, cut, :], spec_im_ref[order, cut, :]
            pair = jnp.concatenate([real * k_re - imag * k_im, real * k_im + imag * k_re], axis=1)
            pair = right_const(pair, back_ref[: 2 * SIDE, :], back_ref[2 * SIDE :, :])
            real, imag = pair[:, :SIDE], pair[:, SIDE:]
            reals.append(real * cos - imag * sin)
            imags.append(real * sin + imag * cos)
        grid = jnp.concatenate(
            [jnp.concatenate(reals, axis=1), jnp.concatenate(imags, axis=1)], axis=0
        )
        reach = left_const(ends_ref[2 * SIDE : 3 * SIDE, :], ends_ref[3 * SIDE :, :], grid)
        return smoothed(order + 1) * (reach + coef_ref[order + 1, 3:4, :] * state)

    state = one_order(1, one_order(0, smoothed(0)))
    for s in range(2):
        for c in range(2):
            rows_ref[s, pl.ds(c, HALF, stride=2), :] = state[
                s * HALF : (s + 1) * HALF, c * SIDE : (c + 1) * SIDE
            ]
        piece = rows_ref[s].astype(BF).reshape(HALF, 2, SIDE)
        piece = jnp.concatenate([piece[ROOT:], piece[:ROOT]], axis=0)
        o_ref[:, :, s * SIDE : (s + 1) * SIDE] = piece


def on_device(
    tokens,
    w_value,
    w_first,
    w_second,
    short_taps,
    filter_in,
    filter_mid,
    filter_out,
    decay_rate,
    skip_gain,
    w_output,
):
    seqs, tok_rows, _ = tokens.shape
    blocks = lax.axis_size(ROW)
    length = tok_rows * blocks
    feats = filter_in.shape[0]
    waves, turns, real_all, rights, backs, ends = (jnp.asarray(t) for t in tables(length, feats))
    far = pl.BlockSpec(memory_space=pltpu.HBM)
    vmem = pl.BlockSpec(memory_space=pltpu.VMEM)
    steps = 2
    pieces = pl.pallas_call(
        functools.partial(project_kernel, steps),
        out_shape=jax.ShapeDtypeStruct((blocks, 4, 3 * tok_rows), BF),
        in_specs=[far] * 4,
        out_specs=vmem,
        scratch_shapes=[
            pltpu.VMEM((seqs * tok_rows, tokens.shape[2]), BF),
            pltpu.VMEM((tokens.shape[2], 3 * SIDE), BF),
            pltpu.VMEM((seqs * tok_rows, 3 * SIDE), F32),
            pltpu.SemaphoreType.DMA((steps, 5)),
        ],
        compiler_params=pltpu.CompilerParams(vmem_limit_bytes=66_700_000),
        name="project",
    )(tokens, w_value, w_first, w_second)
    members = [[(i + ROOT) % blocks for i in range(blocks)]]
    arrived = lax.all_to_all(pieces, ROW, 0, 0, tiled=True, axis_index_groups=members)

    spec = jax.ShapeDtypeStruct((2, 2 * SIDE, SIDE), F32)
    units = filter_in.shape[1]
    rows, factor = pl.pallas_call(
        network_kernel,
        out_shape=(
            jax.ShapeDtypeStruct((8 * HALF, SIDE), F32),
            jax.ShapeDtypeStruct((8, SIDE), F32),
        ),
        in_specs=[vmem] * 5,
        out_specs=(vmem, vmem),
        scratch_shapes=[pltpu.VMEM((32, units), F32)],
        compiler_params=pltpu.CompilerParams(vmem_limit_bytes=16 * 2**20),
        cost_estimate=pl.CostEstimate(
            flops=4_000_000_000, bytes_accessed=1_000_000, transcendentals=0
        ),
        name="network",
    )(
        waves,
        filter_in,
        filter_mid,
        filter_out.reshape(4 * units, -1),
        decay_rate.reshape(1, -1),
    )
    spec_re, spec_im, coef = pl.pallas_call(
        spectra_kernel,
        out_shape=(spec, spec, jax.ShapeDtypeStruct((3, 8, 2 * SIDE), F32)),
        in_specs=[vmem] * 7,
        out_specs=(vmem,) * 3,
        compiler_params=pltpu.CompilerParams(vmem_limit_bytes=16 * 2**20),
        cost_estimate=pl.CostEstimate(
            flops=1_000_000_000, bytes_accessed=2_000_000, transcendentals=0
        ),
        name="spectra",
    )(rows, factor, turns, real_all, rights, short_taps, skip_gain)
    planes = lax.axis_size("x")
    cut = PLANE * (w_output.shape[0] // planes)
    w_turned = jnp.concatenate([w_output[cut:], w_output[:cut]], axis=0)
    coef, w_turned = lax.optimization_barrier((coef, w_turned))
    gated = pl.pallas_call(
        conv_kernel,
        out_shape=jax.ShapeDtypeStruct((blocks, 2, seqs * tok_rows), BF),
        in_specs=[vmem] * 8,
        out_specs=vmem,
        scratch_shapes=[
            pltpu.VMEM((6, SIDE, SIDE), F32),
        ],
        compiler_params=pltpu.CompilerParams(vmem_limit_bytes=16 * 2**20),
        cost_estimate=pl.CostEstimate(
            flops=4_000_000_000, bytes_accessed=2_000_000, transcendentals=0
        ),
        name="gated_conv",
    )(
        arrived,
        coef,
        spec_re,
        spec_im,
        turns,
        rights,
        backs,
        ends,
    )
    returned = lax.all_to_all(gated, ROW, 0, 0, tiled=True, axis_index_groups=members)
    returned = returned.reshape(2 * blocks, seqs * tok_rows)
    turned = [[(i + PLANE) % planes for i in range(planes)]]
    everyone = lax.all_to_all(
        jnp.broadcast_to(returned[None], (planes, *returned.shape)),
        "x", 0, 0, tiled=True, axis_index_groups=turned,
    )
    everyone = lax.all_gather(everyone, "core", axis=1)
    everyone = everyone.reshape(-1, seqs * tok_rows)
    result = jnp.einsum("ct,cd->td", everyone, w_turned, preferred_element_type=F32)
    return result.astype(BF).reshape(seqs, tok_rows, -1)


def solution(mesh):
    torus = Mesh(mesh.devices.reshape(8, 8, 4, 2), ("row_0", "row_1", "x", "core"))
    in_specs = (
        P(None, ROW, None),
        P(None, COL),
        P(None, COL),
        P(None, COL),
        P(None, None, COL),
        P(),
        P(),
        P(None, None, None, COL),
        P(COL),
        P(None, COL),
        P(None, COL),
    )
    out_specs = P(None, ROW, COL)
    return jax.shard_map(
        on_device, mesh=torus, in_specs=in_specs, out_specs=out_specs, check_vma=False
    )
```

```python
import functools
import math

import jax
import jax.numpy as jnp
import numpy as np
from jax import lax
from jax.experimental import pallas as pl
from jax.experimental.pallas import tpu as pltpu
from jax.sharding import Mesh
from jax.sharding import PartitionSpec as P

ROW = ("row_0", "row_1")
COL = ("x", "core")
SIDE = 128
HALF = SIDE // 2
CHUNK = 4096
PLANE = 2
ROOT = 44
BF = jnp.bfloat16
F32 = jnp.float32


def halves(table):
    table = np.asarray(table, np.float32)
    top = table.astype(jnp.bfloat16)
    return top, (table - top.astype(np.float32)).astype(jnp.bfloat16)


@functools.lru_cache(None)
def tables(length, feats):
    bands = (feats - 1) // 2
    freq = np.linspace(0.0001, bands - 1, bands)[:, None] * (2.0 * math.pi / length)
    coarse, near = freq * np.arange(SIDE) * SIDE, freq * np.arange(SIDE)
    waves = np.stack([np.cos(coarse), np.sin(coarse), np.cos(near), np.sin(near)])
    index = np.arange(SIDE)
    turn = 2.0 * math.pi / SIDE * (index[:, None] * index[None, :] % SIDE)
    cos, sin = np.cos(turn), np.sin(turn)
    fine = 2.0 * math.pi / (SIDE * SIDE) * (index[:, None] * index[None, :])
    pair_in = np.block([[cos[:, :HALF], sin[:, :HALF]], [-sin[:, :HALF], cos[:, :HALF]]])
    right = np.block([[cos, -sin], [sin, cos]])
    in_hi, in_lo = halves(pair_in)
    out_hi, out_lo = halves(pair_in.T)
    right_hi, right_lo = halves(right)
    back_hi, back_lo = halves(right.T)
    real_hi, real_lo = in_hi[:, :HALF], in_lo[:, :HALF]
    real_all = np.concatenate([real_hi, real_lo, real_hi, np.zeros_like(real_hi)], axis=1)
    rights = np.concatenate([right_hi, right_lo])
    backs = np.concatenate([back_hi, back_lo])
    ends = np.concatenate([np.concatenate([in_hi, in_lo], axis=1), out_hi, out_lo])
    turns = np.concatenate([np.cos(fine), np.sin(fine)]).astype(np.float32)
    return np.concatenate(waves).astype(np.float32), turns, real_all, rights, backs, ends


def hi_lo(value):
    top = value.astype(BF)
    return top, (value - top.astype(F32)).astype(BF)


def mm(a, b, dims=(((1,), (0,)), ((), ()))):
    return lax.dot_general(a, b, dims, preferred_element_type=F32)


def left_const(const_hi, const_lo, value):
    top, low = hi_lo(value)
    return mm(const_hi, top) + mm(const_lo, top) + mm(const_hi, low)


def right_const(value, const_hi, const_lo):
    top, low = hi_lo(value)
    return mm(top, const_hi) + mm(low, const_hi) + mm(top, const_lo)


def sine_of_turns(moved):
    moved = moved - jnp.round(moved)
    quarter = 0.25 - jnp.abs(moved)
    square = quarter * quarter
    poly = -70.98993302 * square + 81.34038614
    poly = poly * square - 41.33713041
    poly = poly * square + 6.28316395
    return poly * quarter


def project_kernel(
    steps, tok_hbm, a_hbm, b_hbm, c_hbm, o_ref, tok, weights, sum_ref, sems
):
    depth = tok.shape[1] // steps

    def group_of(step, cut):
        group = []
        for s in range(2):
            group.append((tok_hbm.at[s, :, cut], tok.at[pl.ds(s * SIDE, SIDE), cut]))
        for p, source in enumerate((a_hbm, b_hbm, c_hbm)):
            group.append((source.at[cut, :], weights.at[cut, pl.ds(p * SIDE, SIDE)]))
        return [
            pltpu.make_async_copy(near, far, sems.at[step, k]) for k, (near, far) in enumerate(group)
        ]

    for step in range(steps):
        for copy in group_of(step, pl.ds(step * depth, depth)):
            copy.start()
    for step in range(steps):
        for copy in group_of(step, pl.ds(step * depth, depth)):
            copy.wait()
        cut = slice(step * depth, (step + 1) * depth)
        part = mm(tok[:, cut], weights[cut, :])
        if step < steps - 1:
            sum_ref[...] = part if step == 0 else sum_ref[...] + part
    part += sum_ref[...]
    for p in range(3):
        cut = slice(p * SIDE, (p + 1) * SIDE)
        for s in range(2):
            turned = part[s * SIDE : (s + 1) * SIDE, cut].T
            o_ref[:, 2 * s : 2 * s + 2, cut] = turned.astype(BF).reshape(HALF, 2, SIDE)


def network_kernel(
    waves_ref, in_ref, mid_ref, out_ref, rate_ref, rows_ref, factor_ref, side_ref
):
    length = HALF * SIDE
    device = lax.axis_index("row_0") * lax.axis_size("row_1") + lax.axis_index("row_1")
    device = (device + (HALF - ROOT)) % HALF
    lane = lax.broadcasted_iota(jnp.int32, (8, SIDE), 1)
    row = lax.broadcasted_iota(jnp.int32, (8, SIDE), 0)
    mine = lane == 2 * device + row % 2
    last = (((1,), (1,)), ((), ()))
    first = (((0,), (0,)), ((), ()))
    units = mid_ref.shape[0]
    out_hi = jnp.zeros((8, units), F32)
    out_lo = jnp.zeros((8, units), F32)
    for pair in range(4):
        pick = jnp.where(mine & (row // 2 == pair), 1.0, 0.0).astype(BF)
        top, low = hi_lo(out_ref[pl.ds(pair, units, stride=4), :])
        out_hi += mm(pick, top, last)
        out_lo += mm(pick, low, last)
    out_hi, out_lo = out_hi.astype(BF), out_lo.astype(BF)
    out_all = jnp.concatenate([out_hi, out_lo, out_hi], axis=1)
    rate = jnp.sum(jnp.where(mine, rate_ref[...], 0.0), axis=1, keepdims=True)
    scale = 1.0 / (2.0 * math.pi)
    side_ref[...] = jnp.zeros_like(side_ref)
    ramp_hi, ramp_lo = hi_lo(in_ref[0:1, :] * scale)
    side_ref[0:1, :] = ramp_hi.astype(F32)
    side_ref[1:2, :] = ramp_lo.astype(F32)
    side_ref[2:3, :] = ramp_hi.astype(F32)
    side_ref[3:4, :] = jnp.full((1, units), -0.25, F32)
    side_ref[16:17, :] = jnp.full((1, units), -0.25, F32)
    in_hi, in_lo = hi_lo(in_ref[1:33, :] * scale)
    in_all = jnp.concatenate([in_hi, in_lo, in_hi, side_ref[0:16, :].astype(BF)], axis=0)
    mid_hi, mid_lo = hi_lo(mid_ref[...] * scale)
    mid_all = jnp.concatenate([mid_hi, mid_lo, mid_hi, side_ref[16:32, :].astype(BF)], axis=0)
    chunk = CHUNK
    cos_far, sin_far, cos_near, sin_near = (
        waves_ref[16 * k : 16 * (k + 1), :] for k in range(4)
    )
    ones = jnp.ones((16, chunk), BF)
    sign = jnp.where(row < 4, 1.0, -1.0)
    squares = jnp.zeros((8, SIDE), F32)
    blocks = chunk // SIDE
    for start in range(0, HALF, blocks):
        pieces, sides = [], []
        for block in range(start, start + blocks):
            far_c, far_s = cos_far[:, block : block + 1], sin_far[:, block : block + 1]
            pieces.append(
                jnp.concatenate(
                    [
                        far_c * cos_near - far_s * sin_near,
                        -(far_s * cos_near + far_c * sin_near),
                    ],
                    axis=0,
                )
            )
            ramp = (lane + block * SIDE).astype(F32) * (1.0 / (length - 1))
            ramp_top = ramp.astype(BF).astype(F32)
            ramp = jnp.where(row == 2, ramp - ramp_top, jnp.where(row < 2, ramp_top, 1.0))
            sides.append(jnp.concatenate([ramp, jnp.zeros_like(ramp)], axis=0).astype(BF))
        top, low = hi_lo(jnp.concatenate(pieces, axis=1))
        side = jnp.concatenate(sides, axis=1)
        moved = mm(in_all, jnp.concatenate([top, top, low, side], axis=0), first)
        top, low = hi_lo(sine_of_turns(moved))
        moved = mm(mid_all, jnp.concatenate([top, top, low, ones], axis=0), first)
        top, low = hi_lo(sine_of_turns(moved))
        shaped = mm(out_all, jnp.concatenate([top, top, low], axis=0))
        for piece in range(blocks):
            block = start + piece
            lag = lane + block * SIDE
            part = shaped[:, piece * SIDE : (piece + 1) * SIDE] * jnp.exp(-rate * lag.astype(F32))
            if block == 0:
                part = jnp.where((row >= 4) & (lag == 0), 0.0, part)
            squares += part * part
            rows_ref[block * 8 : (block + 1) * 8, :] = pltpu.roll(part, 4, 0) + part * sign
    total = jnp.sum(squares + pltpu.roll(squares, 4, 0), axis=1, keepdims=True)
    factor = lax.rsqrt(total + 1e-06) * (1.0 / (SIDE * SIDE))
    factor_ref[...] = jnp.broadcast_to(factor, factor_ref.shape)


def spectra_kernel(
    rows_ref, factor_ref, turns_ref, real_ref, right_ref, taps_ref, gain_ref,
    spec_re_ref, spec_im_ref, coef_ref,
):
    device = lax.axis_index("row_0") * lax.axis_size("row_1") + lax.axis_index("row_1")
    device = (device + (HALF - ROOT)) % HALF
    sources = [(tap, taps_ref[tap], 0) for tap in range(3)] + [(3, gain_ref[...], 1)]
    for c in range(2):
        for at, source, shift in sources:
            count = source.shape[0]
            at_lane = lax.broadcasted_iota(jnp.int32, (count, SIDE), 1) == 2 * device + c
            value = jnp.sum(jnp.where(at_lane, source, 0.0), axis=1, keepdims=True)
            value = jnp.broadcast_to(value, (count, SIDE))
            for k in range(count):
                coef_ref[k + shift, at : at + 1, c * SIDE : (c + 1) * SIDE] = value[k : k + 1]
    pieces = []
    for j in range(8):
        pieces.append(rows_ref[pl.ds(j, HALF, stride=8), :] * factor_ref[j : j + 1, :])
    top, low = hi_lo(jnp.concatenate(pieces, axis=1))
    grid = mm(real_ref[:, : 3 * HALF], jnp.concatenate([top, top, low], axis=0))
    cos, sin = turns_ref[:SIDE, :], turns_ref[SIDE:, :]

    def turned(j):
        real = grid[:SIDE, j * SIDE : (j + 1) * SIDE]
        imag = grid[SIDE:, j * SIDE : (j + 1) * SIDE]
        return jnp.concatenate([real * cos + imag * sin, imag * cos - real * sin], axis=1)

    for j in range(4):
        rows = pl.ds(j % 2 * SIDE, SIDE)
        spec_re_ref[j // 2, rows, :] = right_const(
            turned(j), right_ref[: 2 * SIDE, :SIDE], right_ref[2 * SIDE :, :SIDE]
        )
        spec_im_ref[j // 2, rows, :] = right_const(
            turned(j + 4), right_ref[: 2 * SIDE, SIDE:], right_ref[2 * SIDE :, SIDE:]
        )


def conv_kernel(
    x_ref, coef_ref, spec_re_ref, spec_im_ref, turns_ref, right_ref, back_ref, ends_ref,
    o_ref, rows_ref,
):
    for p in range(3):
        for s in range(2):
            piece = x_ref[:, 2 * s : 2 * s + 2, p * SIDE : (p + 1) * SIDE]
            piece = jnp.concatenate([piece[HALF - ROOT :], piece[: HALF - ROOT]], axis=0)
            rows_ref[2 * p + s] = piece.reshape(SIDE, SIDE).astype(F32)
    row = lax.broadcasted_iota(jnp.int32, (HALF, SIDE), 0)
    lane = lax.broadcasted_iota(jnp.int32, (HALF, SIDE), 1)

    def smoothed(p):
        seqs = []
        for s in range(2):
            chans = []
            for c in range(2):
                here = rows_ref[2 * p + s, pl.ds(c, HALF, stride=2), :]
                moved = pltpu.roll(here, 1, 1)
                prev = jnp.where(lane == 0, pltpu.roll(moved, 1, 0), moved)
                prev = jnp.where((lane == 0) & (row == 0), 0.0, prev)
                moved = pltpu.roll(here, SIDE - 1, 1)
                after = jnp.where(lane == SIDE - 1, pltpu.roll(moved, HALF - 1, 0), moved)
                after = jnp.where((lane == SIDE - 1) & (row == HALF - 1), 0.0, after)
                first, second, third = (
                    coef_ref[p, tap : tap + 1, c * SIDE : (c + 1) * SIDE] for tap in range(3)
                )
                chans.append(first * prev + second * here + third * after)
            seqs.append(jnp.concatenate(chans, axis=1))
        return jnp.concatenate(seqs, axis=0)

    cos, sin = turns_ref[:SIDE, :], turns_ref[SIDE:, :]
    cos2, sin2 = jnp.concatenate([cos, cos], axis=1), jnp.concatenate([sin, sin], axis=1)

    def one_order(order, state):
        top, low = hi_lo(state)
        grid = mm(ends_ref[: 2 * SIDE, :], jnp.concatenate([top, top], axis=0))
        grid += mm(ends_ref[: 2 * SIDE, :SIDE], low)
        reals, imags = [], []
        for c in range(2):
            cut = slice(c * SIDE, (c + 1) * SIDE)
            real, imag = grid[:SIDE, cut], grid[SIDE:, cut]
            pair = jnp.concatenate([real * cos + imag * sin, imag * cos - real * sin], axis=1)
            pair = right_const(pair, right_ref[: 2 * SIDE, :], right_ref[2 * SIDE :, :])
            real, imag = pair[:, :SIDE], pair[:, SIDE:]
            k_re, k_im = spec_re_ref[order, cut, :], spec_im_ref[order, cut, :]
            pair = jnp.concatenate([real * k_re - imag * k_im, real * k_im + imag * k_re], axis=1)
            pair = right_const(pair, back_ref[: 2 * SIDE, :], back_ref[2 * SIDE :, :])
            real, imag = pair[:, :SIDE], pair[:, SIDE:]
            reals.append(real * cos - imag * sin)
            imags.append(real * sin + imag * cos)
        grid = jnp.concatenate(
            [jnp.concatenate(reals, axis=1), jnp.concatenate(imags, axis=1)], axis=0
        )
        reach = left_const(ends_ref[2 * SIDE : 3 * SIDE, :], ends_ref[3 * SIDE :, :], grid)
        return smoothed(order + 1) * (reach + coef_ref[order + 1, 3:4, :] * state)

    state = one_order(1, one_order(0, smoothed(0)))
    for s in range(2):
        for c in range(2):
            rows_ref[s, pl.ds(c, HALF, stride=2), :] = state[
                s * HALF : (s + 1) * HALF, c * SIDE : (c + 1) * SIDE
            ]
        piece = rows_ref[s].astype(BF).reshape(HALF, 2, SIDE)
        piece = jnp.concatenate([piece[ROOT:], piece[:ROOT]], axis=0)
        o_ref[:, :, s * SIDE : (s + 1) * SIDE] = piece


def output_kernel(all_ref, w_ref, o_ref):
    rows = all_ref.shape[0]
    cut = PLANE * (rows // 4)
    first = (((0,), (0,)), ((), ()))
    total = mm(all_ref[: rows - cut, :], w_ref[cut:, :], first)
    total += mm(all_ref[rows - cut :, :], w_ref[:cut, :], first)
    o_ref[...] = total.astype(BF)


def on_device(
    tokens,
    w_value,
    w_first,
    w_second,
    short_taps,
    filter_in,
    filter_mid,
    filter_out,
    decay_rate,
    skip_gain,
    w_output,
):
    seqs, tok_rows, _ = tokens.shape
    blocks = lax.axis_size(ROW)
    length = tok_rows * blocks
    feats = filter_in.shape[0]
    waves, turns, real_all, rights, backs, ends = (jnp.asarray(t) for t in tables(length, feats))
    far = pl.BlockSpec(memory_space=pltpu.HBM)
    vmem = pl.BlockSpec(memory_space=pltpu.VMEM)
    steps = 2
    pieces = pl.pallas_call(
        functools.partial(project_kernel, steps),
        out_shape=jax.ShapeDtypeStruct((blocks, 4, 3 * tok_rows), BF),
        in_specs=[far] * 4,
        out_specs=vmem,
        scratch_shapes=[
            pltpu.VMEM((seqs * tok_rows, tokens.shape[2]), BF),
            pltpu.VMEM((tokens.shape[2], 3 * SIDE), BF),
            pltpu.VMEM((seqs * tok_rows, 3 * SIDE), F32),
            pltpu.SemaphoreType.DMA((steps, 5)),
        ],
        compiler_params=pltpu.CompilerParams(vmem_limit_bytes=66_700_000),
        name="project",
    )(tokens, w_value, w_first, w_second)
    members = [[(i + ROOT) % blocks for i in range(blocks)]]
    arrived = lax.all_to_all(pieces, ROW, 0, 0, tiled=True, axis_index_groups=members)

    spec = jax.ShapeDtypeStruct((2, 2 * SIDE, SIDE), F32)
    units = filter_in.shape[1]
    rows, factor = pl.pallas_call(
        network_kernel,
        out_shape=(
            jax.ShapeDtypeStruct((8 * HALF, SIDE), F32),
            jax.ShapeDtypeStruct((8, SIDE), F32),
        ),
        in_specs=[vmem] * 5,
        out_specs=(vmem, vmem),
        scratch_shapes=[pltpu.VMEM((32, units), F32)],
        compiler_params=pltpu.CompilerParams(vmem_limit_bytes=16 * 2**20),
        cost_estimate=pl.CostEstimate(
            flops=4_000_000_000, bytes_accessed=1_000_000, transcendentals=0
        ),
        name="network",
    )(
        waves,
        filter_in,
        filter_mid,
        filter_out.reshape(4 * units, -1),
        decay_rate.reshape(1, -1),
    )
    spec_re, spec_im, coef = pl.pallas_call(
        spectra_kernel,
        out_shape=(spec, spec, jax.ShapeDtypeStruct((3, 8, 2 * SIDE), F32)),
        in_specs=[vmem] * 7,
        out_specs=(vmem,) * 3,
        compiler_params=pltpu.CompilerParams(vmem_limit_bytes=16 * 2**20),
        cost_estimate=pl.CostEstimate(
            flops=1_000_000_000, bytes_accessed=2_000_000, transcendentals=0
        ),
        name="spectra",
    )(rows, factor, turns, real_all, rights, short_taps, skip_gain)
    planes = lax.axis_size("x")
    gated = pl.pallas_call(
        conv_kernel,
        out_shape=jax.ShapeDtypeStruct((blocks, 2, seqs * tok_rows), BF),
        in_specs=[vmem] * 8,
        out_specs=vmem,
        scratch_shapes=[
            pltpu.VMEM((6, SIDE, SIDE), F32),
        ],
        compiler_params=pltpu.CompilerParams(vmem_limit_bytes=16 * 2**20),
        cost_estimate=pl.CostEstimate(
            flops=4_000_000_000, bytes_accessed=2_000_000, transcendentals=0
        ),
        name="gated_conv",
    )(
        arrived,
        coef,
        spec_re,
        spec_im,
        turns,
        rights,
        backs,
        ends,
    )
    returned = lax.all_to_all(gated, ROW, 0, 0, tiled=True, axis_index_groups=members)
    returned = returned.reshape(2 * blocks, seqs * tok_rows)
    turned = [[(i + PLANE) % planes for i in range(planes)]]
    everyone = lax.all_to_all(
        jnp.broadcast_to(returned[None], (planes, *returned.shape)),
        "x", 0, 0, tiled=True, axis_index_groups=turned,
    )
    everyone = lax.all_gather(everyone, "core", axis=1)
    everyone = everyone.reshape(-1, seqs * tok_rows)
    result = pl.pallas_call(
        output_kernel,
        out_shape=jax.ShapeDtypeStruct((seqs * tok_rows, w_output.shape[1]), BF),
        in_specs=[vmem] * 2,
        out_specs=vmem,
        compiler_params=pltpu.CompilerParams(vmem_limit_bytes=16 * 2**20),
        cost_estimate=pl.CostEstimate(
            flops=134_217_728, bytes_accessed=1_200_000, transcendentals=0
        ),
        name="output_map",
    )(everyone, w_output)
    return result.reshape(seqs, tok_rows, -1)


def solution(mesh):
    torus = Mesh(mesh.devices.reshape(8, 8, 4, 2), ("row_0", "row_1", "x", "core"))
    in_specs = (
        P(None, ROW, None),
        P(None, COL),
        P(None, COL),
        P(None, COL),
        P(None, None, COL),
        P(),
        P(),
        P(None, None, None, COL),
        P(COL),
        P(None, COL),
        P(None, COL),
    )
    out_specs = P(None, ROW, COL)
    return jax.shard_map(
        on_device, mesh=torus, in_specs=in_specs, out_specs=out_specs, check_vma=False
    )
```

```python
import functools
import math

import jax
import jax.numpy as jnp
import numpy as np
from jax import lax
from jax.experimental import pallas as pl
from jax.experimental.pallas import tpu as pltpu
from jax.sharding import Mesh
from jax.sharding import PartitionSpec as P

ROW = ("row_0", "row_1")
COL = ("x", "core")
SIDE = 128
HALF = SIDE // 2
CHUNK = 4096
PLANE = 2
ROOT = 44
BF = jnp.bfloat16
F32 = jnp.float32


def halves(table):
    table = np.asarray(table, np.float32)
    top = table.astype(jnp.bfloat16)
    return top, (table - top.astype(np.float32)).astype(jnp.bfloat16)


@functools.lru_cache(None)
def tables(length, feats):
    bands = (feats - 1) // 2
    freq = np.linspace(0.0001, bands - 1, bands)[:, None] * (2.0 * math.pi / length)
    coarse, near = freq * np.arange(SIDE) * SIDE, freq * np.arange(SIDE)
    waves = np.stack([np.cos(coarse), np.sin(coarse), np.cos(near), np.sin(near)])
    index = np.arange(SIDE)
    turn = 2.0 * math.pi / SIDE * (index[:, None] * index[None, :] % SIDE)
    cos, sin = np.cos(turn), np.sin(turn)
    fine = 2.0 * math.pi / (SIDE * SIDE) * (index[:, None] * index[None, :])
    pair_in = np.block([[cos[:, :HALF], sin[:, :HALF]], [-sin[:, :HALF], cos[:, :HALF]]])
    right = np.block([[cos, -sin], [sin, cos]])
    in_hi, in_lo = halves(pair_in)
    out_hi, out_lo = halves(pair_in.T)
    right_hi, right_lo = halves(right)
    back_hi, back_lo = halves(right.T)
    real_hi, real_lo = in_hi[:, :HALF], in_lo[:, :HALF]
    real_all = np.concatenate([real_hi, real_lo, real_hi, np.zeros_like(real_hi)], axis=1)
    rights = np.concatenate([right_hi, right_lo])
    backs = np.concatenate([back_hi, back_lo])
    ends = np.concatenate([np.concatenate([in_hi, in_lo], axis=1), out_hi, out_lo])
    turns = np.concatenate([np.cos(fine), np.sin(fine)]).astype(np.float32)
    return np.concatenate(waves).astype(np.float32), turns, real_all, rights, backs, ends


def hi_lo(value):
    top = value.astype(BF)
    return top, (value - top.astype(F32)).astype(BF)


def mm(a, b, dims=(((1,), (0,)), ((), ()))):
    return lax.dot_general(a, b, dims, preferred_element_type=F32)


def left_const(const_hi, const_lo, value):
    top, low = hi_lo(value)
    return mm(const_hi, top) + mm(const_lo, top) + mm(const_hi, low)


def right_const(value, const_hi, const_lo):
    top, low = hi_lo(value)
    return mm(top, const_hi) + mm(low, const_hi) + mm(top, const_lo)


def sine_of_turns(moved):
    moved = moved - jnp.round(moved)
    quarter = 0.25 - jnp.abs(moved)
    square = quarter * quarter
    poly = -70.98993302 * square + 81.34038614
    poly = poly * square - 41.33713041
    poly = poly * square + 6.28316395
    return poly * quarter


def project_kernel(
    steps, tok_hbm, a_hbm, b_hbm, c_hbm, o_ref, tok, weights, sum_ref, sems
):
    depth = tok.shape[1] // steps

    def group_of(step, cut):
        group = []
        for s in range(2):
            group.append((tok_hbm.at[s, :, cut], tok.at[pl.ds(s * SIDE, SIDE), cut]))
        for p, source in enumerate((a_hbm, b_hbm, c_hbm)):
            group.append((source.at[cut, :], weights.at[cut, pl.ds(p * SIDE, SIDE)]))
        return [
            pltpu.make_async_copy(near, far, sems.at[step, k]) for k, (near, far) in enumerate(group)
        ]

    for step in range(steps):
        for copy in group_of(step, pl.ds(step * depth, depth)):
            copy.start()
    for step in range(steps):
        for copy in group_of(step, pl.ds(step * depth, depth)):
            copy.wait()
        cut = slice(step * depth, (step + 1) * depth)
        part = mm(tok[:, cut], weights[cut, :])
        if step < steps - 1:
            sum_ref[...] = part if step == 0 else sum_ref[...] + part
    part += sum_ref[...]
    for p in range(3):
        cut = slice(p * SIDE, (p + 1) * SIDE)
        for s in range(2):
            turned = part[s * SIDE : (s + 1) * SIDE, cut].T
            o_ref[:, 2 * s : 2 * s + 2, cut] = turned.astype(BF).reshape(HALF, 2, SIDE)


def network_kernel(
    waves_ref, in_ref, mid_ref, out_ref, rate_ref, rows_ref, factor_ref, side_ref
):
    length = HALF * SIDE
    device = lax.axis_index("row_0") * lax.axis_size("row_1") + lax.axis_index("row_1")
    device = (device + (HALF - ROOT)) % HALF
    lane = lax.broadcasted_iota(jnp.int32, (8, SIDE), 1)
    row = lax.broadcasted_iota(jnp.int32, (8, SIDE), 0)
    mine = lane == 2 * device + row % 2
    last = (((1,), (1,)), ((), ()))
    first = (((0,), (0,)), ((), ()))
    units = mid_ref.shape[0]
    out_hi = jnp.zeros((8, units), F32)
    out_lo = jnp.zeros((8, units), F32)
    for pair in range(4):
        pick = jnp.where(mine & (row // 2 == pair), 1.0, 0.0).astype(BF)
        top, low = hi_lo(out_ref[pl.ds(pair, units, stride=4), :])
        out_hi += mm(pick, top, last)
        out_lo += mm(pick, low, last)
    out_hi, out_lo = out_hi.astype(BF), out_lo.astype(BF)
    out_all = jnp.concatenate([out_hi, out_lo, out_hi], axis=1)
    rate = jnp.sum(jnp.where(mine, rate_ref[...], 0.0), axis=1, keepdims=True)
    scale = 1.0 / (2.0 * math.pi)
    side_ref[...] = jnp.zeros_like(side_ref)
    ramp_hi, ramp_lo = hi_lo(in_ref[0:1, :] * scale)
    side_ref[0:1, :] = ramp_hi.astype(F32)
    side_ref[1:2, :] = ramp_lo.astype(F32)
    side_ref[2:3, :] = ramp_hi.astype(F32)
    side_ref[3:4, :] = jnp.full((1, units), -0.25, F32)
    side_ref[16:17, :] = jnp.full((1, units), -0.25, F32)
    in_hi, in_lo = hi_lo(in_ref[1:33, :] * scale)
    in_all = jnp.concatenate([in_hi, in_lo, in_hi, side_ref[0:16, :].astype(BF)], axis=0)
    mid_hi, mid_lo = hi_lo(mid_ref[...] * scale)
    mid_all = jnp.concatenate([mid_hi, mid_lo, mid_hi, side_ref[16:32, :].astype(BF)], axis=0)
    chunk = CHUNK
    cos_far, sin_far, cos_near, sin_near = (
        waves_ref[16 * k : 16 * (k + 1), :] for k in range(4)
    )
    ones = jnp.ones((16, chunk), BF)
    sign = jnp.where(row < 4, 1.0, -1.0)
    squares = jnp.zeros((8, SIDE), F32)
    blocks = chunk // SIDE
    for start in range(0, HALF, blocks):
        pieces, sides = [], []
        for block in range(start, start + blocks):
            far_c, far_s = cos_far[:, block : block + 1], sin_far[:, block : block + 1]
            pieces.append(
                jnp.concatenate(
                    [
                        far_c * cos_near - far_s * sin_near,
                        -(far_s * cos_near + far_c * sin_near),
                    ],
                    axis=0,
                )
            )
            ramp = (lane + block * SIDE).astype(F32) * (1.0 / (length - 1))
            ramp_top = ramp.astype(BF).astype(F32)
            ramp = jnp.where(row == 2, ramp - ramp_top, jnp.where(row < 2, ramp_top, 1.0))
            sides.append(jnp.concatenate([ramp, jnp.zeros_like(ramp)], axis=0).astype(BF))
        top, low = hi_lo(jnp.concatenate(pieces, axis=1))
        side = jnp.concatenate(sides, axis=1)
        moved = mm(in_all, jnp.concatenate([top, top, low, side], axis=0), first)
        top, low = hi_lo(sine_of_turns(moved))
        moved = mm(mid_all, jnp.concatenate([top, top, low, ones], axis=0), first)
        top, low = hi_lo(sine_of_turns(moved))
        shaped = mm(out_all, jnp.concatenate([top, top, low], axis=0))
        for piece in range(blocks):
            block = start + piece
            lag = lane + block * SIDE
            part = shaped[:, piece * SIDE : (piece + 1) * SIDE] * jnp.exp(-rate * lag.astype(F32))
            if block == 0:
                part = jnp.where((row >= 4) & (lag == 0), 0.0, part)
            squares += part * part
            rows_ref[block * 8 : (block + 1) * 8, :] = pltpu.roll(part, 4, 0) + part * sign
    total = jnp.sum(squares + pltpu.roll(squares, 4, 0), axis=1, keepdims=True)
    factor = lax.rsqrt(total + 1e-06) * (1.0 / (SIDE * SIDE))
    factor_ref[...] = jnp.broadcast_to(factor, factor_ref.shape)


def spectra_kernel(
    rows_ref, factor_ref, turns_ref, real_ref, right_ref, taps_ref, gain_ref,
    spec_re_ref, spec_im_ref, coef_ref,
):
    device = lax.axis_index("row_0") * lax.axis_size("row_1") + lax.axis_index("row_1")
    device = (device + (HALF - ROOT)) % HALF
    sources = [(tap, taps_ref[tap], 0) for tap in range(3)] + [(3, gain_ref[...], 1)]
    for c in range(2):
        for at, source, shift in sources:
            count = source.shape[0]
            at_lane = lax.broadcasted_iota(jnp.int32, (count, SIDE), 1) == 2 * device + c
            value = jnp.sum(jnp.where(at_lane, source, 0.0), axis=1, keepdims=True)
            value = jnp.broadcast_to(value, (count, SIDE))
            for k in range(count):
                coef_ref[k + shift, at : at + 1, c * SIDE : (c + 1) * SIDE] = value[k : k + 1]
    pieces = []
    for j in range(8):
        pieces.append(rows_ref[pl.ds(j, HALF, stride=8), :] * factor_ref[j : j + 1, :])
    top, low = hi_lo(jnp.concatenate(pieces, axis=1))
    grid = mm(real_ref[:, : 3 * HALF], jnp.concatenate([top, top, low], axis=0))
    cos, sin = turns_ref[:SIDE, :], turns_ref[SIDE:, :]

    def turned(j):
        real = grid[:SIDE, j * SIDE : (j + 1) * SIDE]
        imag = grid[SIDE:, j * SIDE : (j + 1) * SIDE]
        return jnp.concatenate([real * cos + imag * sin, imag * cos - real * sin], axis=1)

    for j in range(4):
        rows = pl.ds(j % 2 * SIDE, SIDE)
        spec_re_ref[j // 2, rows, :] = right_const(
            turned(j), right_ref[: 2 * SIDE, :SIDE], right_ref[2 * SIDE :, :SIDE]
        )
        spec_im_ref[j // 2, rows, :] = right_const(
            turned(j + 4), right_ref[: 2 * SIDE, SIDE:], right_ref[2 * SIDE :, SIDE:]
        )


def conv_kernel(
    x_ref, coef_ref, spec_re_ref, spec_im_ref, turns_ref, right_ref, back_ref, ends_ref,
    o_ref, rows_ref,
):
    for p in range(3):
        for s in range(2):
            piece = x_ref[:, 2 * s : 2 * s + 2, p * SIDE : (p + 1) * SIDE]
            piece = jnp.concatenate([piece[HALF - ROOT :], piece[: HALF - ROOT]], axis=0)
            rows_ref[2 * p + s] = piece.reshape(SIDE, SIDE).astype(F32)
    row = lax.broadcasted_iota(jnp.int32, (HALF, SIDE), 0)
    lane = lax.broadcasted_iota(jnp.int32, (HALF, SIDE), 1)

    def smoothed(p):
        seqs = []
        for s in range(2):
            chans = []
            for c in range(2):
                here = rows_ref[2 * p + s, pl.ds(c, HALF, stride=2), :]
                moved = pltpu.roll(here, 1, 1)
                prev = jnp.where(lane == 0, pltpu.roll(moved, 1, 0), moved)
                prev = jnp.where((lane == 0) & (row == 0), 0.0, prev)
                moved = pltpu.roll(here, SIDE - 1, 1)
                after = jnp.where(lane == SIDE - 1, pltpu.roll(moved, HALF - 1, 0), moved)
                after = jnp.where((lane == SIDE - 1) & (row == HALF - 1), 0.0, after)
                first, second, third = (
                    coef_ref[p, tap : tap + 1, c * SIDE : (c + 1) * SIDE] for tap in range(3)
                )
                chans.append(first * prev + second * here + third * after)
            seqs.append(jnp.concatenate(chans, axis=1))
        return jnp.concatenate(seqs, axis=0)

    cos, sin = turns_ref[:SIDE, :], turns_ref[SIDE:, :]
    cos2, sin2 = jnp.concatenate([cos, cos], axis=1), jnp.concatenate([sin, sin], axis=1)

    def one_order(order, state):
        top, low = hi_lo(state)
        grid = mm(ends_ref[: 2 * SIDE, :], jnp.concatenate([top, top], axis=0))
        grid += mm(ends_ref[: 2 * SIDE, :SIDE], low)
        reals, imags = [], []
        for c in range(2):
            cut = slice(c * SIDE, (c + 1) * SIDE)
            real, imag = grid[:SIDE, cut], grid[SIDE:, cut]
            pair = jnp.concatenate([real * cos + imag * sin, imag * cos - real * sin], axis=1)
            pair = right_const(pair, right_ref[: 2 * SIDE, :], right_ref[2 * SIDE :, :])
            real, imag = pair[:, :SIDE], pair[:, SIDE:]
            k_re, k_im = spec_re_ref[order, cut, :], spec_im_ref[order, cut, :]
            pair = jnp.concatenate([real * k_re - imag * k_im, real * k_im + imag * k_re], axis=1)
            pair = right_const(pair, back_ref[: 2 * SIDE, :], back_ref[2 * SIDE :, :])
            real, imag = pair[:, :SIDE], pair[:, SIDE:]
            reals.append(real * cos - imag * sin)
            imags.append(real * sin + imag * cos)
        grid = jnp.concatenate(
            [jnp.concatenate(reals, axis=1), jnp.concatenate(imags, axis=1)], axis=0
        )
        reach = left_const(ends_ref[2 * SIDE : 3 * SIDE, :], ends_ref[3 * SIDE :, :], grid)
        return smoothed(order + 1) * (reach + coef_ref[order + 1, 3:4, :] * state)

    state = one_order(1, one_order(0, smoothed(0)))
    for s in range(2):
        for c in range(2):
            rows_ref[s, pl.ds(c, HALF, stride=2), :] = state[
                s * HALF : (s + 1) * HALF, c * SIDE : (c + 1) * SIDE
            ]
        piece = rows_ref[s].astype(BF).reshape(HALF, 2, SIDE)
        piece = jnp.concatenate([piece[ROOT:], piece[:ROOT]], axis=0)
        for plane in range(o_ref.shape[0]):
            o_ref[plane, :, :, s * SIDE : (s + 1) * SIDE] = piece


def output_kernel(all_ref, w_ref, o_ref):
    rows = all_ref.shape[0]
    cut = PLANE * (rows // 4)
    first = (((0,), (0,)), ((), ()))
    total = mm(all_ref[: rows - cut, :], w_ref[cut:, :], first)
    total += mm(all_ref[rows - cut :, :], w_ref[:cut, :], first)
    o_ref[...] = total.astype(BF)


def on_device(
    tokens,
    w_value,
    w_first,
    w_second,
    short_taps,
    filter_in,
    filter_mid,
    filter_out,
    decay_rate,
    skip_gain,
    w_output,
):
    seqs, tok_rows, _ = tokens.shape
    blocks = lax.axis_size(ROW)
    length = tok_rows * blocks
    feats = filter_in.shape[0]
    waves, turns, real_all, rights, backs, ends = (jnp.asarray(t) for t in tables(length, feats))
    far = pl.BlockSpec(memory_space=pltpu.HBM)
    vmem = pl.BlockSpec(memory_space=pltpu.VMEM)
    steps = 2
    pieces = pl.pallas_call(
        functools.partial(project_kernel, steps),
        out_shape=jax.ShapeDtypeStruct((blocks, 4, 3 * tok_rows), BF),
        in_specs=[far] * 4,
        out_specs=vmem,
        scratch_shapes=[
            pltpu.VMEM((seqs * tok_rows, tokens.shape[2]), BF),
            pltpu.VMEM((tokens.shape[2], 3 * SIDE), BF),
            pltpu.VMEM((seqs * tok_rows, 3 * SIDE), F32),
            pltpu.SemaphoreType.DMA((steps, 5)),
        ],
        compiler_params=pltpu.CompilerParams(vmem_limit_bytes=66_700_000),
        name="project",
    )(tokens, w_value, w_first, w_second)
    members = [[(i + ROOT) % blocks for i in range(blocks)]]
    arrived = lax.all_to_all(pieces, ROW, 0, 0, tiled=True, axis_index_groups=members)

    spec = jax.ShapeDtypeStruct((2, 2 * SIDE, SIDE), F32)
    units = filter_in.shape[1]
    rows, factor = pl.pallas_call(
        network_kernel,
        out_shape=(
            jax.ShapeDtypeStruct((8 * HALF, SIDE), F32),
            jax.ShapeDtypeStruct((8, SIDE), F32),
        ),
        in_specs=[vmem] * 5,
        out_specs=(vmem, vmem),
        scratch_shapes=[pltpu.VMEM((32, units), F32)],
        compiler_params=pltpu.CompilerParams(vmem_limit_bytes=16 * 2**20),
        cost_estimate=pl.CostEstimate(
            flops=4_000_000_000, bytes_accessed=1_000_000, transcendentals=0
        ),
        name="network",
    )(
        waves,
        filter_in,
        filter_mid,
        filter_out.reshape(4 * units, -1),
        decay_rate.reshape(1, -1),
    )
    spec_re, spec_im, coef = pl.pallas_call(
        spectra_kernel,
        out_shape=(spec, spec, jax.ShapeDtypeStruct((3, 8, 2 * SIDE), F32)),
        in_specs=[vmem] * 7,
        out_specs=(vmem,) * 3,
        compiler_params=pltpu.CompilerParams(vmem_limit_bytes=16 * 2**20),
        cost_estimate=pl.CostEstimate(
            flops=1_000_000_000, bytes_accessed=2_000_000, transcendentals=0
        ),
        name="spectra",
    )(rows, factor, turns, real_all, rights, short_taps, skip_gain)
    planes = lax.axis_size("x")
    gated = pl.pallas_call(
        conv_kernel,
        out_shape=jax.ShapeDtypeStruct((planes, blocks, 2, seqs * tok_rows), BF),
        in_specs=[vmem] * 8,
        out_specs=vmem,
        scratch_shapes=[
            pltpu.VMEM((6, SIDE, SIDE), F32),
        ],
        compiler_params=pltpu.CompilerParams(vmem_limit_bytes=16 * 2**20),
        cost_estimate=pl.CostEstimate(
            flops=4_000_000_000, bytes_accessed=2_000_000, transcendentals=0
        ),
        name="gated_conv",
    )(
        arrived,
        coef,
        spec_re,
        spec_im,
        turns,
        rights,
        backs,
        ends,
    )
    turned = [
        [((i // blocks + PLANE) % planes) * blocks + (i + ROOT) % blocks for i in range(planes * blocks)]
    ]
    everyone = lax.all_to_all(
        gated.reshape(planes * blocks, *gated.shape[2:]),
        ("x", *ROW), 0, 0, tiled=True, axis_index_groups=turned,
    )
    everyone = everyone.reshape(planes, 2 * blocks, seqs * tok_rows)
    everyone = lax.all_gather(everyone, "core", axis=1)
    everyone = everyone.reshape(-1, seqs * tok_rows)
    result = pl.pallas_call(
        output_kernel,
        out_shape=jax.ShapeDtypeStruct((seqs * tok_rows, w_output.shape[1]), BF),
        in_specs=[vmem] * 2,
        out_specs=vmem,
        compiler_params=pltpu.CompilerParams(vmem_limit_bytes=16 * 2**20),
        cost_estimate=pl.CostEstimate(
            flops=134_217_728, bytes_accessed=1_200_000, transcendentals=0
        ),
        name="output_map",
    )(everyone, w_output)
    return result.reshape(seqs, tok_rows, -1)


def solution(mesh):
    torus = Mesh(mesh.devices.reshape(8, 8, 4, 2), ("row_0", "row_1", "x", "core"))
    in_specs = (
        P(None, ROW, None),
        P(None, COL),
        P(None, COL),
        P(None, COL),
        P(None, None, COL),
        P(),
        P(),
        P(None, None, None, COL),
        P(COL),
        P(None, COL),
        P(None, COL),
    )
    out_specs = P(None, ROW, COL)
    return jax.shard_map(
        on_device, mesh=torus, in_specs=in_specs, out_specs=out_specs, check_vma=False
    )
```

```python
import functools
import math

import jax
import jax.numpy as jnp
import numpy as np
from jax import lax
from jax.experimental import pallas as pl
from jax.experimental.pallas import tpu as pltpu
from jax.sharding import Mesh
from jax.sharding import PartitionSpec as P

ROW = ("row_0", "row_1")
COL = ("x", "core")
SIDE = 128
HALF = SIDE // 2
CHUNK = 4096
PLANE = 2
ROOT = 44
BF = jnp.bfloat16
F32 = jnp.float32


def halves(table):
    table = np.asarray(table, np.float32)
    top = table.astype(jnp.bfloat16)
    return top, (table - top.astype(np.float32)).astype(jnp.bfloat16)


@functools.lru_cache(None)
def tables(length, feats):
    bands = (feats - 1) // 2
    freq = np.linspace(0.0001, bands - 1, bands)[:, None] * (2.0 * math.pi / length)
    coarse, near = freq * np.arange(SIDE) * SIDE, freq * np.arange(SIDE)
    waves = np.stack([np.cos(coarse), np.sin(coarse), np.cos(near), np.sin(near)])
    index = np.arange(SIDE)
    turn = 2.0 * math.pi / SIDE * (index[:, None] * index[None, :] % SIDE)
    cos, sin = np.cos(turn), np.sin(turn)
    fine = 2.0 * math.pi / (SIDE * SIDE) * (index[:, None] * index[None, :])
    pair_in = np.block([[cos[:, :HALF], sin[:, :HALF]], [-sin[:, :HALF], cos[:, :HALF]]])
    right = np.block([[cos, -sin], [sin, cos]])
    in_hi, in_lo = halves(pair_in)
    out_hi, out_lo = halves(pair_in.T)
    right_hi, right_lo = halves(right)
    back_hi, back_lo = halves(right.T)
    real_hi, real_lo = in_hi[:, :HALF], in_lo[:, :HALF]
    real_all = np.concatenate([real_hi, real_lo, real_hi, np.zeros_like(real_hi)], axis=1)
    rights = np.concatenate([right_hi, right_lo])
    backs = np.concatenate([back_hi, back_lo])
    ends = np.concatenate([np.concatenate([in_hi, in_lo], axis=1), out_hi, out_lo])
    turns = np.concatenate([np.cos(fine), np.sin(fine)]).astype(np.float32)
    return np.concatenate(waves).astype(np.float32), turns, real_all, rights, backs, ends


def hi_lo(value):
    top = value.astype(BF)
    return top, (value - top.astype(F32)).astype(BF)


def three_parts(value):
    top = value.astype(BF)
    rest = value - top.astype(F32)
    low = rest.astype(BF)
    return top, low, (rest - low.astype(F32)).astype(BF)


def mm(a, b, dims=(((1,), (0,)), ((), ()))):
    return lax.dot_general(a, b, dims, preferred_element_type=F32)


def left_const(const_hi, const_lo, value):
    top, low = hi_lo(value)
    return mm(const_hi, top) + mm(const_lo, top) + mm(const_hi, low)


def right_const(value, const_hi, const_lo):
    top, low = hi_lo(value)
    return mm(top, const_hi) + mm(low, const_hi) + mm(top, const_lo)


def sine_of_turns(moved):
    moved = moved - jnp.round(moved)
    quarter = 0.25 - jnp.abs(moved)
    square = quarter * quarter
    poly = -70.98993302 * square + 81.34038614
    poly = poly * square - 41.33713041
    poly = poly * square + 6.28316395
    return poly * quarter


def project_kernel(
    steps, tok_hbm, a_hbm, b_hbm, c_hbm, o_ref, tok, weights, sum_ref, sems
):
    depth = tok.shape[1] // steps

    def group_of(step, cut):
        group = []
        for s in range(2):
            group.append((tok_hbm.at[s, :, cut], tok.at[pl.ds(s * SIDE, SIDE), cut]))
        for p, source in enumerate((a_hbm, b_hbm, c_hbm)):
            group.append((source.at[cut, :], weights.at[cut, pl.ds(p * SIDE, SIDE)]))
        return [
            pltpu.make_async_copy(near, far, sems.at[step, k]) for k, (near, far) in enumerate(group)
        ]

    for step in range(steps):
        for copy in group_of(step, pl.ds(step * depth, depth)):
            copy.start()
    for step in range(steps):
        for copy in group_of(step, pl.ds(step * depth, depth)):
            copy.wait()
        cut = slice(step * depth, (step + 1) * depth)
        part = mm(tok[:, cut], weights[cut, :])
        if step < steps - 1:
            sum_ref[...] = part if step == 0 else sum_ref[...] + part
    part += sum_ref[...]
    for p in range(3):
        cut = slice(p * SIDE, (p + 1) * SIDE)
        for s in range(2):
            turned = part[s * SIDE : (s + 1) * SIDE, cut].T
            o_ref[:, 2 * s : 2 * s + 2, cut] = turned.astype(BF).reshape(HALF, 2, SIDE)


def network_kernel(
    waves_ref, in_ref, mid_ref, out_ref, rate_ref, rows_ref, factor_ref, side_ref
):
    length = HALF * SIDE
    device = lax.axis_index("row_0") * lax.axis_size("row_1") + lax.axis_index("row_1")
    device = (device + (HALF - ROOT)) % HALF
    lane = lax.broadcasted_iota(jnp.int32, (8, SIDE), 1)
    row = lax.broadcasted_iota(jnp.int32, (8, SIDE), 0)
    mine = lane == 2 * device + row % 2
    last = (((1,), (1,)), ((), ()))
    first = (((0,), (0,)), ((), ()))
    units = mid_ref.shape[0]
    out_hi = jnp.zeros((8, units), F32)
    out_lo = jnp.zeros((8, units), F32)
    for pair in range(4):
        pick = jnp.where(mine & (row // 2 == pair), 1.0, 0.0).astype(BF)
        top, low = hi_lo(out_ref[pl.ds(pair, units, stride=4), :])
        out_hi += mm(pick, top, last)
        out_lo += mm(pick, low, last)
    out_hi, out_lo = out_hi.astype(BF), out_lo.astype(BF)
    out_all = jnp.concatenate([out_hi, out_lo, out_hi], axis=1)
    rate = jnp.sum(jnp.where(mine, rate_ref[...], 0.0), axis=1, keepdims=True)
    scale = 1.0 / (2.0 * math.pi)
    side_ref[...] = jnp.zeros_like(side_ref)
    ramp_hi, ramp_lo = hi_lo(in_ref[0:1, :] * scale)
    side_ref[0:1, :] = ramp_hi.astype(F32)
    side_ref[1:2, :] = ramp_lo.astype(F32)
    side_ref[2:3, :] = ramp_hi.astype(F32)
    side_ref[3:4, :] = jnp.full((1, units), -0.25, F32)
    side_ref[16:17, :] = jnp.full((1, units), -0.25, F32)
    in_hi, in_lo, in_end = three_parts(in_ref[1:33, :] * scale)
    in_all = jnp.concatenate(
        [in_hi, in_lo, in_hi, in_lo, in_hi, in_end, side_ref[0:16, :].astype(BF)], axis=0
    )
    mid_hi, mid_lo = hi_lo(mid_ref[...] * scale)
    mid_all = jnp.concatenate([mid_hi, mid_lo, mid_hi, side_ref[16:32, :].astype(BF)], axis=0)
    chunk = CHUNK
    cos_far, sin_far, cos_near, sin_near = (
        waves_ref[16 * k : 16 * (k + 1), :] for k in range(4)
    )
    ones = jnp.ones((16, chunk), BF)
    sign = jnp.where(row < 4, 1.0, -1.0)
    squares = jnp.zeros((8, SIDE), F32)
    blocks = chunk // SIDE
    for start in range(0, HALF, blocks):
        pieces, sides = [], []
        for block in range(start, start + blocks):
            far_c, far_s = cos_far[:, block : block + 1], sin_far[:, block : block + 1]
            pieces.append(
                jnp.concatenate(
                    [
                        far_c * cos_near - far_s * sin_near,
                        -(far_s * cos_near + far_c * sin_near),
                    ],
                    axis=0,
                )
            )
            ramp = (lane + block * SIDE).astype(F32) * (1.0 / (length - 1))
            ramp_top = ramp.astype(BF).astype(F32)
            ramp = jnp.where(row == 2, ramp - ramp_top, jnp.where(row < 2, ramp_top, 1.0))
            sides.append(jnp.concatenate([ramp, jnp.zeros_like(ramp)], axis=0).astype(BF))
        top, low, end = three_parts(jnp.concatenate(pieces, axis=1))
        side = jnp.concatenate(sides, axis=1)
        moved = mm(in_all, jnp.concatenate([top, top, low, low, end, top, side], axis=0), first)
        top, low = hi_lo(sine_of_turns(moved))
        moved = mm(mid_all, jnp.concatenate([top, top, low, ones], axis=0), first)
        top, low = hi_lo(sine_of_turns(moved))
        shaped = mm(out_all, jnp.concatenate([top, top, low], axis=0))
        for piece in range(blocks):
            block = start + piece
            lag = lane + block * SIDE
            part = shaped[:, piece * SIDE : (piece + 1) * SIDE] * jnp.exp(-rate * lag.astype(F32))
            if block == 0:
                part = jnp.where((row >= 4) & (lag == 0), 0.0, part)
            squares += part * part
            rows_ref[block * 8 : (block + 1) * 8, :] = pltpu.roll(part, 4, 0) + part * sign
    total = jnp.sum(squares + pltpu.roll(squares, 4, 0), axis=1, keepdims=True)
    factor = lax.rsqrt(total + 1e-06) * (1.0 / (SIDE * SIDE))
    factor_ref[...] = jnp.broadcast_to(factor, factor_ref.shape)


def spectra_kernel(
    rows_ref, factor_ref, turns_ref, real_ref, right_ref, taps_ref, gain_ref,
    spec_re_ref, spec_im_ref, coef_ref,
):
    device = lax.axis_index("row_0") * lax.axis_size("row_1") + lax.axis_index("row_1")
    device = (device + (HALF - ROOT)) % HALF
    sources = [(tap, taps_ref[tap], 0) for tap in range(3)] + [(3, gain_ref[...], 1)]
    for c in range(2):
        for at, source, shift in sources:
            count = source.shape[0]
            at_lane = lax.broadcasted_iota(jnp.int32, (count, SIDE), 1) == 2 * device + c
            value = jnp.sum(jnp.where(at_lane, source, 0.0), axis=1, keepdims=True)
            value = jnp.broadcast_to(value, (count, SIDE))
            for k in range(count):
                coef_ref[k + shift, at : at + 1, c * SIDE : (c + 1) * SIDE] = value[k : k + 1]
    pieces = []
    for j in range(8):
        pieces.append(rows_ref[pl.ds(j, HALF, stride=8), :] * factor_ref[j : j + 1, :])
    top, low = hi_lo(jnp.concatenate(pieces, axis=1))
    grid = mm(real_ref[:, : 3 * HALF], jnp.concatenate([top, top, low], axis=0))
    cos, sin = turns_ref[:SIDE, :], turns_ref[SIDE:, :]

    def turned(j):
        real = grid[:SIDE, j * SIDE : (j + 1) * SIDE]
        imag = grid[SIDE:, j * SIDE : (j + 1) * SIDE]
        return jnp.concatenate([real * cos + imag * sin, imag * cos - real * sin], axis=1)

    for j in range(4):
        rows = pl.ds(j % 2 * SIDE, SIDE)
        spec_re_ref[j // 2, rows, :] = right_const(
            turned(j), right_ref[: 2 * SIDE, :SIDE], right_ref[2 * SIDE :, :SIDE]
        )
        spec_im_ref[j // 2, rows, :] = right_const(
            turned(j + 4), right_ref[: 2 * SIDE, SIDE:], right_ref[2 * SIDE :, SIDE:]
        )


def conv_kernel(
    x_ref, coef_ref, spec_re_ref, spec_im_ref, turns_ref, right_ref, back_ref, ends_ref,
    o_ref, rows_ref,
):
    for p in range(3):
        for s in range(2):
            piece = x_ref[:, 2 * s : 2 * s + 2, p * SIDE : (p + 1) * SIDE]
            piece = jnp.concatenate([piece[HALF - ROOT :], piece[: HALF - ROOT]], axis=0)
            rows_ref[2 * p + s] = piece.reshape(SIDE, SIDE).astype(F32)
    row = lax.broadcasted_iota(jnp.int32, (HALF, SIDE), 0)
    lane = lax.broadcasted_iota(jnp.int32, (HALF, SIDE), 1)

    def smoothed(p):
        seqs = []
        for s in range(2):
            chans = []
            for c in range(2):
                here = rows_ref[2 * p + s, pl.ds(c, HALF, stride=2), :]
                moved = pltpu.roll(here, 1, 1)
                prev = jnp.where(lane == 0, pltpu.roll(moved, 1, 0), moved)
                prev = jnp.where((lane == 0) & (row == 0), 0.0, prev)
                moved = pltpu.roll(here, SIDE - 1, 1)
                after = jnp.where(lane == SIDE - 1, pltpu.roll(moved, HALF - 1, 0), moved)
                after = jnp.where((lane == SIDE - 1) & (row == HALF - 1), 0.0, after)
                first, second, third = (
                    coef_ref[p, tap : tap + 1, c * SIDE : (c + 1) * SIDE] for tap in range(3)
                )
                chans.append(first * prev + second * here + third * after)
            seqs.append(jnp.concatenate(chans, axis=1))
        return jnp.concatenate(seqs, axis=0)

    cos, sin = turns_ref[:SIDE, :], turns_ref[SIDE:, :]
    cos2, sin2 = jnp.concatenate([cos, cos], axis=1), jnp.concatenate([sin, sin], axis=1)

    def one_order(order, state):
        top, low = hi_lo(state)
        grid = mm(ends_ref[: 2 * SIDE, :], jnp.concatenate([top, top], axis=0))
        grid += mm(ends_ref[: 2 * SIDE, :SIDE], low)
        reals, imags = [], []
        for c in range(2):
            cut = slice(c * SIDE, (c + 1) * SIDE)
            real, imag = grid[:SIDE, cut], grid[SIDE:, cut]
            pair = jnp.concatenate([real * cos + imag * sin, imag * cos - real * sin], axis=1)
            pair = right_const(pair, right_ref[: 2 * SIDE, :], right_ref[2 * SIDE :, :])
            real, imag = pair[:, :SIDE], pair[:, SIDE:]
            k_re, k_im = spec_re_ref[order, cut, :], spec_im_ref[order, cut, :]
            pair = jnp.concatenate([real * k_re - imag * k_im, real * k_im + imag * k_re], axis=1)
            pair = right_const(pair, back_ref[: 2 * SIDE, :], back_ref[2 * SIDE :, :])
            real, imag = pair[:, :SIDE], pair[:, SIDE:]
            reals.append(real * cos - imag * sin)
            imags.append(real * sin + imag * cos)
        grid = jnp.concatenate(
            [jnp.concatenate(reals, axis=1), jnp.concatenate(imags, axis=1)], axis=0
        )
        reach = left_const(ends_ref[2 * SIDE : 3 * SIDE, :], ends_ref[3 * SIDE :, :], grid)
        return smoothed(order + 1) * (reach + coef_ref[order + 1, 3:4, :] * state)

    state = one_order(1, one_order(0, smoothed(0)))
    for s in range(2):
        for c in range(2):
            rows_ref[s, pl.ds(c, HALF, stride=2), :] = state[
                s * HALF : (s + 1) * HALF, c * SIDE : (c + 1) * SIDE
            ]
        piece = rows_ref[s].astype(BF).reshape(HALF, 2, SIDE)
        piece = jnp.concatenate([piece[ROOT:], piece[:ROOT]], axis=0)
        for plane in range(o_ref.shape[0]):
            o_ref[plane, :, :, s * SIDE : (s + 1) * SIDE] = piece


def output_kernel(all_ref, w_ref, o_ref):
    rows = all_ref.shape[0]
    cut = PLANE * (rows // 4)
    first = (((0,), (0,)), ((), ()))
    total = mm(all_ref[: rows - cut, :], w_ref[cut:, :], first)
    total += mm(all_ref[rows - cut :, :], w_ref[:cut, :], first)
    o_ref[...] = total.astype(BF)


def on_device(
    tokens,
    w_value,
    w_first,
    w_second,
    short_taps,
    filter_in,
    filter_mid,
    filter_out,
    decay_rate,
    skip_gain,
    w_output,
):
    seqs, tok_rows, _ = tokens.shape
    blocks = lax.axis_size(ROW)
    length = tok_rows * blocks
    feats = filter_in.shape[0]
    waves, turns, real_all, rights, backs, ends = (jnp.asarray(t) for t in tables(length, feats))
    far = pl.BlockSpec(memory_space=pltpu.HBM)
    vmem = pl.BlockSpec(memory_space=pltpu.VMEM)
    steps = 2
    pieces = pl.pallas_call(
        functools.partial(project_kernel, steps),
        out_shape=jax.ShapeDtypeStruct((blocks, 4, 3 * tok_rows), BF),
        in_specs=[far] * 4,
        out_specs=vmem,
        scratch_shapes=[
            pltpu.VMEM((seqs * tok_rows, tokens.shape[2]), BF),
            pltpu.VMEM((tokens.shape[2], 3 * SIDE), BF),
            pltpu.VMEM((seqs * tok_rows, 3 * SIDE), F32),
            pltpu.SemaphoreType.DMA((steps, 5)),
        ],
        compiler_params=pltpu.CompilerParams(vmem_limit_bytes=66_700_000),
        name="project",
    )(tokens, w_value, w_first, w_second)
    members = [[(i + ROOT) % blocks for i in range(blocks)]]
    arrived = lax.all_to_all(pieces, ROW, 0, 0, tiled=True, axis_index_groups=members)

    spec = jax.ShapeDtypeStruct((2, 2 * SIDE, SIDE), F32)
    units = filter_in.shape[1]
    rows, factor = pl.pallas_call(
        network_kernel,
        out_shape=(
            jax.ShapeDtypeStruct((8 * HALF, SIDE), F32),
            jax.ShapeDtypeStruct((8, SIDE), F32),
        ),
        in_specs=[vmem] * 5,
        out_specs=(vmem, vmem),
        scratch_shapes=[pltpu.VMEM((32, units), F32)],
        compiler_params=pltpu.CompilerParams(vmem_limit_bytes=16 * 2**20),
        cost_estimate=pl.CostEstimate(
            flops=4_000_000_000, bytes_accessed=1_000_000, transcendentals=0
        ),
        name="network",
    )(
        waves,
        filter_in,
        filter_mid,
        filter_out.reshape(4 * units, -1),
        decay_rate.reshape(1, -1),
    )
    spec_re, spec_im, coef = pl.pallas_call(
        spectra_kernel,
        out_shape=(spec, spec, jax.ShapeDtypeStruct((3, 8, 2 * SIDE), F32)),
        in_specs=[vmem] * 7,
        out_specs=(vmem,) * 3,
        compiler_params=pltpu.CompilerParams(vmem_limit_bytes=16 * 2**20),
        cost_estimate=pl.CostEstimate(
            flops=1_000_000_000, bytes_accessed=2_000_000, transcendentals=0
        ),
        name="spectra",
    )(rows, factor, turns, real_all, rights, short_taps, skip_gain)
    planes = lax.axis_size("x")
    gated = pl.pallas_call(
        conv_kernel,
        out_shape=jax.ShapeDtypeStruct((planes, blocks, 2, seqs * tok_rows), BF),
        in_specs=[vmem] * 8,
        out_specs=vmem,
        scratch_shapes=[
            pltpu.VMEM((6, SIDE, SIDE), F32),
        ],
        compiler_params=pltpu.CompilerParams(vmem_limit_bytes=16 * 2**20),
        cost_estimate=pl.CostEstimate(
            flops=4_000_000_000, bytes_accessed=2_000_000, transcendentals=0
        ),
        name="gated_conv",
    )(
        arrived,
        coef,
        spec_re,
        spec_im,
        turns,
        rights,
        backs,
        ends,
    )
    turned = [
        [((i // blocks + PLANE) % planes) * blocks + (i + ROOT) % blocks for i in range(planes * blocks)]
    ]
    everyone = lax.all_to_all(
        gated.reshape(planes * blocks, *gated.shape[2:]),
        ("x", *ROW), 0, 0, tiled=True, axis_index_groups=turned,
    )
    everyone = everyone.reshape(planes, 2 * blocks, seqs * tok_rows)
    everyone = lax.all_gather(everyone, "core", axis=1)
    everyone = everyone.reshape(-1, seqs * tok_rows)
    result = pl.pallas_call(
        output_kernel,
        out_shape=jax.ShapeDtypeStruct((seqs * tok_rows, w_output.shape[1]), BF),
        in_specs=[vmem] * 2,
        out_specs=vmem,
        compiler_params=pltpu.CompilerParams(vmem_limit_bytes=16 * 2**20),
        cost_estimate=pl.CostEstimate(
            flops=134_217_728, bytes_accessed=1_200_000, transcendentals=0
        ),
        name="output_map",
    )(everyone, w_output)
    return result.reshape(seqs, tok_rows, -1)


def solution(mesh):
    torus = Mesh(mesh.devices.reshape(8, 8, 4, 2), ("row_0", "row_1", "x", "core"))
    in_specs = (
        P(None, ROW, None),
        P(None, COL),
        P(None, COL),
        P(None, COL),
        P(None, None, COL),
        P(),
        P(),
        P(None, None, None, COL),
        P(COL),
        P(None, COL),
        P(None, COL),
    )
    out_specs = P(None, ROW, COL)
    return jax.shard_map(
        on_device, mesh=torus, in_specs=in_specs, out_specs=out_specs, check_vma=False
    )
```

```python
import functools
import math

import jax
import jax.numpy as jnp
import numpy as np
from jax import lax
from jax.experimental import pallas as pl
from jax.experimental.pallas import tpu as pltpu
from jax.sharding import Mesh
from jax.sharding import PartitionSpec as P

ROW = ("row_0", "row_1")
COL = ("x", "core")
SIDE = 128
HALF = SIDE // 2
CHUNK = 4096
PLANE = 2
ROOT = 44
BF = jnp.bfloat16
F32 = jnp.float32


def halves(table):
    table = np.asarray(table, np.float32)
    top = table.astype(jnp.bfloat16)
    return top, (table - top.astype(np.float32)).astype(jnp.bfloat16)


@functools.lru_cache(None)
def tables(length, feats):
    bands = (feats - 1) // 2
    freq = np.linspace(0.0001, bands - 1, bands)[:, None] * (2.0 * math.pi / length)
    coarse, near = freq * np.arange(SIDE) * SIDE, freq * np.arange(SIDE)
    waves = np.stack([np.cos(coarse), np.sin(coarse), np.cos(near), np.sin(near)])
    index = np.arange(SIDE)
    turn = 2.0 * math.pi / SIDE * (index[:, None] * index[None, :] % SIDE)
    cos, sin = np.cos(turn), np.sin(turn)
    fine = 2.0 * math.pi / (SIDE * SIDE) * (index[:, None] * index[None, :])
    pair_in = np.block([[cos[:, :HALF], sin[:, :HALF]], [-sin[:, :HALF], cos[:, :HALF]]])
    right = np.block([[cos, -sin], [sin, cos]])
    in_hi, in_lo = halves(pair_in)
    out_hi, out_lo = halves(pair_in.T)
    right_hi, right_lo = halves(right)
    back_hi, back_lo = halves(right.T)
    real_hi, real_lo = in_hi[:, :HALF], in_lo[:, :HALF]
    real_all = np.concatenate([real_hi, real_lo, real_hi, np.zeros_like(real_hi)], axis=1)
    rights = np.concatenate([right_hi, right_lo])
    backs = np.concatenate([back_hi, back_lo])
    ends = np.concatenate([np.concatenate([in_hi, in_lo], axis=1), out_hi, out_lo])
    turns = np.concatenate([np.cos(fine), np.sin(fine)]).astype(np.float32)
    return np.concatenate(waves).astype(np.float32), turns, real_all, rights, backs, ends


def hi_lo(value):
    top = value.astype(BF)
    return top, (value - top.astype(F32)).astype(BF)


def three_parts(value):
    top = value.astype(BF)
    rest = value - top.astype(F32)
    low = rest.astype(BF)
    return top, low, (rest - low.astype(F32)).astype(BF)


def mm(a, b, dims=(((1,), (0,)), ((), ()))):
    return lax.dot_general(a, b, dims, preferred_element_type=F32)


def left_const(const_hi, const_lo, value):
    top, low = hi_lo(value)
    return mm(const_hi, top) + mm(const_lo, top) + mm(const_hi, low)


def right_const(value, const_hi, const_lo):
    top, low = hi_lo(value)
    return mm(top, const_hi) + mm(low, const_hi) + mm(top, const_lo)


def sine_of_turns(moved):
    moved = moved - jnp.round(moved)
    quarter = 0.25 - jnp.abs(moved)
    square = quarter * quarter
    poly = -70.98993302 * square + 81.34038614
    poly = poly * square - 41.33713041
    poly = poly * square + 6.28316395
    return poly * quarter


def project_kernel(
    steps, tok_hbm, a_hbm, b_hbm, c_hbm, o_ref, tok, weights, sum_ref, sems
):
    depth = tok.shape[1] // steps

    def group_of(step, cut):
        group = []
        for s in range(2):
            group.append((tok_hbm.at[s, :, cut], tok.at[pl.ds(s * SIDE, SIDE), cut]))
        for p, source in enumerate((a_hbm, b_hbm, c_hbm)):
            group.append((source.at[cut, :], weights.at[cut, pl.ds(p * SIDE, SIDE)]))
        return [
            pltpu.make_async_copy(near, far, sems.at[step, k]) for k, (near, far) in enumerate(group)
        ]

    for step in range(steps):
        for copy in group_of(step, pl.ds(step * depth, depth)):
            copy.start()
    for step in range(steps):
        for copy in group_of(step, pl.ds(step * depth, depth)):
            copy.wait()
        cut = slice(step * depth, (step + 1) * depth)
        part = mm(tok[:, cut], weights[cut, :])
        if step < steps - 1:
            sum_ref[...] = part if step == 0 else sum_ref[...] + part
    part += sum_ref[...]
    for p in range(3):
        cut = slice(p * SIDE, (p + 1) * SIDE)
        for s in range(2):
            turned = part[s * SIDE : (s + 1) * SIDE, cut].T
            o_ref[:, 2 * s : 2 * s + 2, cut] = turned.astype(BF).reshape(HALF, 2, SIDE)


def network_kernel(
    waves_ref, in_ref, mid_ref, out_ref, rate_ref, rows_ref, factor_ref, side_ref
):
    length = HALF * SIDE
    device = lax.axis_index("row_0") * lax.axis_size("row_1") + lax.axis_index("row_1")
    device = (device + (HALF - ROOT)) % HALF
    lane = lax.broadcasted_iota(jnp.int32, (8, SIDE), 1)
    row = lax.broadcasted_iota(jnp.int32, (8, SIDE), 0)
    mine = lane == 2 * device + row % 2
    last = (((1,), (1,)), ((), ()))
    first = (((0,), (0,)), ((), ()))
    units = mid_ref.shape[0]
    out_hi = jnp.zeros((8, units), F32)
    out_lo = jnp.zeros((8, units), F32)
    for pair in range(4):
        pick = jnp.where(mine & (row // 2 == pair), 1.0, 0.0).astype(BF)
        top, low = hi_lo(out_ref[pl.ds(pair, units, stride=4), :])
        out_hi += mm(pick, top, last)
        out_lo += mm(pick, low, last)
    out_hi, out_lo = out_hi.astype(BF), out_lo.astype(BF)
    out_all = jnp.concatenate([out_hi, out_lo, out_hi], axis=1)
    rate = jnp.sum(jnp.where(mine, rate_ref[...], 0.0), axis=1, keepdims=True)
    scale = 1.0 / (2.0 * math.pi)
    side_ref[...] = jnp.zeros_like(side_ref)
    ramp_hi, ramp_lo = hi_lo(in_ref[0:1, :] * scale)
    side_ref[0:1, :] = ramp_hi.astype(F32)
    side_ref[1:2, :] = ramp_lo.astype(F32)
    side_ref[2:3, :] = ramp_hi.astype(F32)
    side_ref[3:4, :] = jnp.full((1, units), -0.25, F32)
    side_ref[16:17, :] = jnp.full((1, units), -0.25, F32)
    in_hi, in_lo, in_end = three_parts(in_ref[1:33, :] * scale)
    in_all = jnp.concatenate(
        [in_hi, in_lo, in_hi, in_lo, in_hi, in_end, side_ref[0:16, :].astype(BF)], axis=0
    )
    mid_hi, mid_lo = hi_lo(mid_ref[...] * scale)
    mid_all = jnp.concatenate([mid_hi, mid_lo, mid_hi, side_ref[16:32, :].astype(BF)], axis=0)
    chunk = CHUNK
    cos_far, sin_far, cos_near, sin_near = (
        waves_ref[16 * k : 16 * (k + 1), :] for k in range(4)
    )
    ones = jnp.ones((16, chunk), BF)
    sign = jnp.where(row < 4, 1.0, -1.0)
    squares = jnp.zeros((8, SIDE), F32)
    blocks = chunk // SIDE
    for start in range(0, HALF, blocks):
        pieces, sides = [], []
        for block in range(start, start + blocks):
            far_c, far_s = cos_far[:, block : block + 1], sin_far[:, block : block + 1]
            pieces.append(
                jnp.concatenate(
                    [
                        far_c * cos_near - far_s * sin_near,
                        -(far_s * cos_near + far_c * sin_near),
                    ],
                    axis=0,
                )
            )
            ramp = (lane + block * SIDE).astype(F32) * (1.0 / (length - 1))
            ramp_top = ramp.astype(BF).astype(F32)
            ramp = jnp.where(row == 2, ramp - ramp_top, jnp.where(row < 2, ramp_top, 1.0))
            sides.append(jnp.concatenate([ramp, jnp.zeros_like(ramp)], axis=0).astype(BF))
        top, low, end = three_parts(jnp.concatenate(pieces, axis=1))
        side = jnp.concatenate(sides, axis=1)
        moved = mm(in_all, jnp.concatenate([top, top, low, low, end, top, side], axis=0), first)
        top, low = hi_lo(sine_of_turns(moved))
        moved = mm(mid_all, jnp.concatenate([top, top, low, ones], axis=0), first)
        top, low = hi_lo(sine_of_turns(moved))
        shaped = mm(out_all, jnp.concatenate([top, top, low], axis=0))
        for piece in range(blocks):
            block = start + piece
            lag = lane + block * SIDE
            part = shaped[:, piece * SIDE : (piece + 1) * SIDE] * jnp.exp(-rate * lag.astype(F32))
            if block == 0:
                part = jnp.where((row >= 4) & (lag == 0), 0.0, part)
            squares += part * part
            rows_ref[block * 8 : (block + 1) * 8, :] = pltpu.roll(part, 4, 0) + part * sign
    total = jnp.sum(squares + pltpu.roll(squares, 4, 0), axis=1, keepdims=True)
    factor = lax.rsqrt(total + 1e-06) * (1.0 / (SIDE * SIDE))
    factor_ref[...] = jnp.broadcast_to(factor, factor_ref.shape)


def spectra_kernel(
    rows_ref, factor_ref, turns_ref, real_ref, right_ref, taps_ref, gain_ref,
    spec_re_ref, spec_im_ref, coef_ref,
):
    device = lax.axis_index("row_0") * lax.axis_size("row_1") + lax.axis_index("row_1")
    device = (device + (HALF - ROOT)) % HALF
    sources = [(tap, taps_ref[tap], 0) for tap in range(3)] + [(3, gain_ref[...], 1)]
    for c in range(2):
        for at, source, shift in sources:
            count = source.shape[0]
            at_lane = lax.broadcasted_iota(jnp.int32, (count, SIDE), 1) == 2 * device + c
            value = jnp.sum(jnp.where(at_lane, source, 0.0), axis=1, keepdims=True)
            value = jnp.broadcast_to(value, (count, SIDE))
            for k in range(count):
                coef_ref[k + shift, at : at + 1, c * SIDE : (c + 1) * SIDE] = value[k : k + 1]
    pieces = []
    for j in range(8):
        pieces.append(rows_ref[pl.ds(j, HALF, stride=8), :] * factor_ref[j : j + 1, :])
    top, low = hi_lo(jnp.concatenate(pieces, axis=1))
    grid = mm(real_ref[:, : 3 * HALF], jnp.concatenate([top, top, low], axis=0))
    cos, sin = turns_ref[:SIDE, :], turns_ref[SIDE:, :]

    def turned(j):
        real = grid[:SIDE, j * SIDE : (j + 1) * SIDE]
        imag = grid[SIDE:, j * SIDE : (j + 1) * SIDE]
        return jnp.concatenate([real * cos + imag * sin, imag * cos - real * sin], axis=1)

    for j in range(4):
        rows = pl.ds(j % 2 * SIDE, SIDE)
        spec_re_ref[j // 2, rows, :] = right_const(
            turned(j), right_ref[: 2 * SIDE, :SIDE], right_ref[2 * SIDE :, :SIDE]
        )
        spec_im_ref[j // 2, rows, :] = right_const(
            turned(j + 4), right_ref[: 2 * SIDE, SIDE:], right_ref[2 * SIDE :, SIDE:]
        )


def conv_kernel(
    x_ref, coef_ref, spec_re_ref, spec_im_ref, turns_ref, right_ref, back_ref, ends_ref,
    o_ref, rows_ref,
):
    for p in range(3):
        for s in range(2):
            piece = x_ref[:, 2 * s : 2 * s + 2, p * SIDE : (p + 1) * SIDE]
            piece = jnp.concatenate([piece[HALF - ROOT :], piece[: HALF - ROOT]], axis=0)
            rows_ref[2 * p + s] = piece.reshape(SIDE, SIDE).astype(F32)
    row = lax.broadcasted_iota(jnp.int32, (HALF, SIDE), 0)
    lane = lax.broadcasted_iota(jnp.int32, (HALF, SIDE), 1)

    def smoothed(p):
        seqs = []
        for s in range(2):
            chans = []
            for c in range(2):
                here = rows_ref[2 * p + s, pl.ds(c, HALF, stride=2), :]
                moved = pltpu.roll(here, 1, 1)
                prev = jnp.where(lane == 0, pltpu.roll(moved, 1, 0), moved)
                prev = jnp.where((lane == 0) & (row == 0), 0.0, prev)
                moved = pltpu.roll(here, SIDE - 1, 1)
                after = jnp.where(lane == SIDE - 1, pltpu.roll(moved, HALF - 1, 0), moved)
                after = jnp.where((lane == SIDE - 1) & (row == HALF - 1), 0.0, after)
                first, second, third = (
                    coef_ref[p, tap : tap + 1, c * SIDE : (c + 1) * SIDE] for tap in range(3)
                )
                chans.append(first * prev + second * here + third * after)
            seqs.append(jnp.concatenate(chans, axis=1))
        return jnp.concatenate(seqs, axis=0)

    cos, sin = turns_ref[:SIDE, :], turns_ref[SIDE:, :]
    cos2, sin2 = jnp.concatenate([cos, cos], axis=1), jnp.concatenate([sin, sin], axis=1)

    def one_order(order, state):
        top, low = hi_lo(state)
        grid = mm(ends_ref[: 2 * SIDE, :], jnp.concatenate([top, top], axis=0))
        grid += mm(ends_ref[: 2 * SIDE, :SIDE], low)
        reals, imags = [], []
        for c in range(2):
            cut = slice(c * SIDE, (c + 1) * SIDE)
            real, imag = grid[:SIDE, cut], grid[SIDE:, cut]
            pair = jnp.concatenate([real * cos + imag * sin, imag * cos - real * sin], axis=1)
            pair = right_const(pair, right_ref[: 2 * SIDE, :], right_ref[2 * SIDE :, :])
            real, imag = pair[:, :SIDE], pair[:, SIDE:]
            k_re, k_im = spec_re_ref[order, cut, :], spec_im_ref[order, cut, :]
            pair = jnp.concatenate([real * k_re - imag * k_im, real * k_im + imag * k_re], axis=1)
            pair = right_const(pair, back_ref[: 2 * SIDE, :], back_ref[2 * SIDE :, :])
            real, imag = pair[:, :SIDE], pair[:, SIDE:]
            reals.append(real * cos - imag * sin)
            imags.append(real * sin + imag * cos)
        grid = jnp.concatenate(
            [jnp.concatenate(reals, axis=1), jnp.concatenate(imags, axis=1)], axis=0
        )
        reach = left_const(ends_ref[2 * SIDE : 3 * SIDE, :], ends_ref[3 * SIDE :, :], grid)
        return smoothed(order + 1) * (reach + coef_ref[order + 1, 3:4, :] * state)

    state = one_order(1, one_order(0, smoothed(0)))
    for s in range(2):
        for c in range(2):
            rows_ref[s, pl.ds(c, HALF, stride=2), :] = state[
                s * HALF : (s + 1) * HALF, c * SIDE : (c + 1) * SIDE
            ]
        piece = rows_ref[s].astype(BF).reshape(HALF, 2, SIDE)
        piece = jnp.concatenate([piece[ROOT:], piece[:ROOT]], axis=0)
        for plane in range(o_ref.shape[0]):
            o_ref[plane, :, :, s * SIDE : (s + 1) * SIDE] = piece


def output_kernel(all_ref, w_ref, o_hbm, o_ref, sems):
    rows = all_ref.shape[0]
    cut = PLANE * (rows // 4)
    first = (((0,), (0,)), ((), ()))
    copies = []
    for s in range(2):
        part = slice(s * SIDE, (s + 1) * SIDE)
        total = mm(all_ref[: rows - cut, part], w_ref[cut:, :], first)
        total += mm(all_ref[rows - cut :, part], w_ref[:cut, :], first)
        o_ref[part, :] = total.astype(BF)
        span = pl.ds(s * SIDE, SIDE)
        copy = pltpu.make_async_copy(o_ref.at[span, :], o_hbm.at[span, :], sems.at[s])
        copy.start()
        copies.append(copy)
    for copy in copies:
        copy.wait()


def on_device(
    tokens,
    w_value,
    w_first,
    w_second,
    short_taps,
    filter_in,
    filter_mid,
    filter_out,
    decay_rate,
    skip_gain,
    w_output,
):
    seqs, tok_rows, _ = tokens.shape
    blocks = lax.axis_size(ROW)
    length = tok_rows * blocks
    feats = filter_in.shape[0]
    waves, turns, real_all, rights, backs, ends = (jnp.asarray(t) for t in tables(length, feats))
    far = pl.BlockSpec(memory_space=pltpu.HBM)
    vmem = pl.BlockSpec(memory_space=pltpu.VMEM)
    steps = 2
    pieces = pl.pallas_call(
        functools.partial(project_kernel, steps),
        out_shape=jax.ShapeDtypeStruct((blocks, 4, 3 * tok_rows), BF),
        in_specs=[far] * 4,
        out_specs=vmem,
        scratch_shapes=[
            pltpu.VMEM((seqs * tok_rows, tokens.shape[2]), BF),
            pltpu.VMEM((tokens.shape[2], 3 * SIDE), BF),
            pltpu.VMEM((seqs * tok_rows, 3 * SIDE), F32),
            pltpu.SemaphoreType.DMA((steps, 5)),
        ],
        compiler_params=pltpu.CompilerParams(vmem_limit_bytes=66_700_000),
        name="project",
    )(tokens, w_value, w_first, w_second)
    members = [[(i + ROOT) % blocks for i in range(blocks)]]
    arrived = lax.all_to_all(pieces, ROW, 0, 0, tiled=True, axis_index_groups=members)

    spec = jax.ShapeDtypeStruct((2, 2 * SIDE, SIDE), F32)
    units = filter_in.shape[1]
    rows, factor = pl.pallas_call(
        network_kernel,
        out_shape=(
            jax.ShapeDtypeStruct((8 * HALF, SIDE), F32),
            jax.ShapeDtypeStruct((8, SIDE), F32),
        ),
        in_specs=[vmem] * 5,
        out_specs=(vmem, vmem),
        scratch_shapes=[pltpu.VMEM((32, units), F32)],
        compiler_params=pltpu.CompilerParams(vmem_limit_bytes=16 * 2**20),
        cost_estimate=pl.CostEstimate(
            flops=4_000_000_000, bytes_accessed=1_000_000, transcendentals=0
        ),
        name="network",
    )(
        waves,
        filter_in,
        filter_mid,
        filter_out.reshape(4 * units, -1),
        decay_rate.reshape(1, -1),
    )
    spec_re, spec_im, coef = pl.pallas_call(
        spectra_kernel,
        out_shape=(spec, spec, jax.ShapeDtypeStruct((3, 8, 2 * SIDE), F32)),
        in_specs=[vmem] * 7,
        out_specs=(vmem,) * 3,
        compiler_params=pltpu.CompilerParams(vmem_limit_bytes=16 * 2**20),
        cost_estimate=pl.CostEstimate(
            flops=1_000_000_000, bytes_accessed=2_000_000, transcendentals=0
        ),
        name="spectra",
    )(rows, factor, turns, real_all, rights, short_taps, skip_gain)
    planes = lax.axis_size("x")
    gated = pl.pallas_call(
        conv_kernel,
        out_shape=jax.ShapeDtypeStruct((planes, blocks, 2, seqs * tok_rows), BF),
        in_specs=[vmem] * 8,
        out_specs=vmem,
        scratch_shapes=[
            pltpu.VMEM((6, SIDE, SIDE), F32),
        ],
        compiler_params=pltpu.CompilerParams(vmem_limit_bytes=16 * 2**20),
        cost_estimate=pl.CostEstimate(
            flops=4_000_000_000, bytes_accessed=2_000_000, transcendentals=0
        ),
        name="gated_conv",
    )(
        arrived,
        coef,
        spec_re,
        spec_im,
        turns,
        rights,
        backs,
        ends,
    )
    turned = [
        [((i // blocks + PLANE) % planes) * blocks + (i + ROOT) % blocks for i in range(planes * blocks)]
    ]
    everyone = lax.all_to_all(
        gated.reshape(planes * blocks, *gated.shape[2:]),
        ("x", *ROW), 0, 0, tiled=True, axis_index_groups=turned,
    )
    everyone = everyone.reshape(planes, 2 * blocks, seqs * tok_rows)
    everyone = lax.all_gather(everyone, "core", axis=1)
    everyone = everyone.reshape(-1, seqs * tok_rows)
    result = pl.pallas_call(
        output_kernel,
        out_shape=jax.ShapeDtypeStruct((seqs * tok_rows, w_output.shape[1]), BF),
        in_specs=[vmem] * 2,
        out_specs=far,
        scratch_shapes=[
            pltpu.VMEM((seqs * tok_rows, w_output.shape[1]), BF),
            pltpu.SemaphoreType.DMA((2,)),
        ],
        compiler_params=pltpu.CompilerParams(vmem_limit_bytes=16 * 2**20),
        cost_estimate=pl.CostEstimate(
            flops=134_217_728, bytes_accessed=1_200_000, transcendentals=0
        ),
        name="output_map",
    )(everyone, w_output)
    return result.reshape(seqs, tok_rows, -1)


def solution(mesh):
    torus = Mesh(mesh.devices.reshape(8, 8, 4, 2), ("row_0", "row_1", "x", "core"))
    in_specs = (
        P(None, ROW, None),
        P(None, COL),
        P(None, COL),
        P(None, COL),
        P(None, None, COL),
        P(),
        P(),
        P(None, None, None, COL),
        P(COL),
        P(None, COL),
        P(None, COL),
    )
    out_specs = P(None, ROW, COL)
    return jax.shard_map(
        on_device, mesh=torus, in_specs=in_specs, out_specs=out_specs, check_vma=False
    )
```

```python
import functools
import math

import jax
import jax.numpy as jnp
import numpy as np
from jax import lax
from jax.experimental import pallas as pl
from jax.experimental.pallas import tpu as pltpu
from jax.sharding import Mesh
from jax.sharding import PartitionSpec as P

ROW = ("row_0", "row_1")
COL = ("x", "core")
SIDE = 128
HALF = SIDE // 2
CHUNK = 4096
PLANE = 2
ROOT = 36
BF = jnp.bfloat16
F32 = jnp.float32


def halves(table):
    table = np.asarray(table, np.float32)
    top = table.astype(jnp.bfloat16)
    return top, (table - top.astype(np.float32)).astype(jnp.bfloat16)


@functools.lru_cache(None)
def tables(length, feats):
    bands = (feats - 1) // 2
    freq = np.linspace(0.0001, bands - 1, bands)[:, None] * (2.0 * math.pi / length)
    coarse, near = freq * np.arange(SIDE) * SIDE, freq * np.arange(SIDE)
    waves = np.stack([np.cos(coarse), np.sin(coarse), np.cos(near), np.sin(near)])
    index = np.arange(SIDE)
    turn = 2.0 * math.pi / SIDE * (index[:, None] * index[None, :] % SIDE)
    cos, sin = np.cos(turn), np.sin(turn)
    fine = 2.0 * math.pi / (SIDE * SIDE) * (index[:, None] * index[None, :])
    pair_in = np.block([[cos[:, :HALF], sin[:, :HALF]], [-sin[:, :HALF], cos[:, :HALF]]])
    right = np.block([[cos, -sin], [sin, cos]])
    in_hi, in_lo = halves(pair_in)
    out_hi, out_lo = halves(pair_in.T)
    right_hi, right_lo = halves(right)
    back_hi, back_lo = halves(right.T)
    real_hi, real_lo = in_hi[:, :HALF], in_lo[:, :HALF]
    real_all = np.concatenate([real_hi, real_lo, real_hi, np.zeros_like(real_hi)], axis=1)
    rights = np.concatenate([right_hi, right_lo])
    backs = np.concatenate([back_hi, back_lo])
    ends = np.concatenate([np.concatenate([in_hi, in_lo], axis=1), out_hi, out_lo])
    turns = np.concatenate([np.cos(fine), np.sin(fine)]).astype(np.float32)
    return np.concatenate(waves).astype(np.float32), turns, real_all, rights, backs, ends


def hi_lo(value):
    top = value.astype(BF)
    return top, (value - top.astype(F32)).astype(BF)


def three_parts(value):
    top = value.astype(BF)
    rest = value - top.astype(F32)
    low = rest.astype(BF)
    return top, low, (rest - low.astype(F32)).astype(BF)


def mm(a, b, dims=(((1,), (0,)), ((), ()))):
    return lax.dot_general(a, b, dims, preferred_element_type=F32)


def left_const(const_hi, const_lo, value):
    top, low = hi_lo(value)
    return mm(const_hi, top) + mm(const_lo, top) + mm(const_hi, low)


def right_const(value, const_hi, const_lo):
    top, low = hi_lo(value)
    return mm(top, const_hi) + mm(low, const_hi) + mm(top, const_lo)


def sine_of_turns(moved):
    moved = moved - jnp.round(moved)
    quarter = 0.25 - jnp.abs(moved)
    square = quarter * quarter
    poly = -70.98993302 * square + 81.34038614
    poly = poly * square - 41.33713041
    poly = poly * square + 6.28316395
    return poly * quarter


def project_kernel(
    steps, tok_hbm, a_hbm, b_hbm, c_hbm, o_ref, tok, weights, sum_ref, sems
):
    depth = tok.shape[1] // steps

    def group_of(step, cut):
        group = []
        for s in range(2):
            group.append((tok_hbm.at[s, :, cut], tok.at[pl.ds(s * SIDE, SIDE), cut]))
        for p, source in enumerate((a_hbm, b_hbm, c_hbm)):
            group.append((source.at[cut, :], weights.at[cut, pl.ds(p * SIDE, SIDE)]))
        return [
            pltpu.make_async_copy(near, far, sems.at[step, k]) for k, (near, far) in enumerate(group)
        ]

    for step in range(steps):
        for copy in group_of(step, pl.ds(step * depth, depth)):
            copy.start()
    for step in range(steps):
        for copy in group_of(step, pl.ds(step * depth, depth)):
            copy.wait()
        cut = slice(step * depth, (step + 1) * depth)
        part = mm(tok[:, cut], weights[cut, :])
        if step < steps - 1:
            sum_ref[...] = part if step == 0 else sum_ref[...] + part
    part += sum_ref[...]
    for p in range(3):
        cut = slice(p * SIDE, (p + 1) * SIDE)
        for s in range(2):
            turned = part[s * SIDE : (s + 1) * SIDE, cut].T
            o_ref[:, 2 * s : 2 * s + 2, cut] = turned.astype(BF).reshape(HALF, 2, SIDE)


def network_kernel(
    waves_ref, in_ref, mid_ref, out_ref, rate_ref, rows_ref, factor_ref, side_ref
):
    length = HALF * SIDE
    device = lax.axis_index("row_0") * lax.axis_size("row_1") + lax.axis_index("row_1")
    device = (device + (HALF - ROOT)) % HALF
    lane = lax.broadcasted_iota(jnp.int32, (8, SIDE), 1)
    row = lax.broadcasted_iota(jnp.int32, (8, SIDE), 0)
    mine = lane == 2 * device + row % 2
    last = (((1,), (1,)), ((), ()))
    first = (((0,), (0,)), ((), ()))
    units = mid_ref.shape[0]
    out_hi = jnp.zeros((8, units), F32)
    out_lo = jnp.zeros((8, units), F32)
    for pair in range(4):
        pick = jnp.where(mine & (row // 2 == pair), 1.0, 0.0).astype(BF)
        top, low = hi_lo(out_ref[pl.ds(pair, units, stride=4), :])
        out_hi += mm(pick, top, last)
        out_lo += mm(pick, low, last)
    out_hi, out_lo = out_hi.astype(BF), out_lo.astype(BF)
    out_all = jnp.concatenate([out_hi, out_lo, out_hi], axis=1)
    rate = jnp.sum(jnp.where(mine, rate_ref[...], 0.0), axis=1, keepdims=True)
    scale = 1.0 / (2.0 * math.pi)
    side_ref[...] = jnp.zeros_like(side_ref)
    ramp_hi, ramp_lo = hi_lo(in_ref[0:1, :] * scale)
    side_ref[0:1, :] = ramp_hi.astype(F32)
    side_ref[1:2, :] = ramp_lo.astype(F32)
    side_ref[2:3, :] = ramp_hi.astype(F32)
    side_ref[3:4, :] = jnp.full((1, units), -0.25, F32)
    side_ref[16:17, :] = jnp.full((1, units), -0.25, F32)
    in_hi, in_lo, in_end = three_parts(in_ref[1:33, :] * scale)
    in_all = jnp.concatenate(
        [in_hi, in_lo, in_hi, in_lo, in_hi, in_end, side_ref[0:16, :].astype(BF)], axis=0
    )
    mid_hi, mid_lo = hi_lo(mid_ref[...] * scale)
    mid_all = jnp.concatenate([mid_hi, mid_lo, mid_hi, side_ref[16:32, :].astype(BF)], axis=0)
    chunk = CHUNK
    cos_far, sin_far, cos_near, sin_near = (
        waves_ref[16 * k : 16 * (k + 1), :] for k in range(4)
    )
    ones = jnp.ones((16, chunk), BF)
    sign = jnp.where(row < 4, 1.0, -1.0)
    squares = jnp.zeros((8, SIDE), F32)
    blocks = chunk // SIDE
    for start in range(0, HALF, blocks):
        pieces, sides = [], []
        for block in range(start, start + blocks):
            far_c, far_s = cos_far[:, block : block + 1], sin_far[:, block : block + 1]
            pieces.append(
                jnp.concatenate(
                    [
                        far_c * cos_near - far_s * sin_near,
                        -(far_s * cos_near + far_c * sin_near),
                    ],
                    axis=0,
                )
            )
            ramp = (lane + block * SIDE).astype(F32) * (1.0 / (length - 1))
            ramp_top = ramp.astype(BF).astype(F32)
            ramp = jnp.where(row == 2, ramp - ramp_top, jnp.where(row < 2, ramp_top, 1.0))
            sides.append(jnp.concatenate([ramp, jnp.zeros_like(ramp)], axis=0).astype(BF))
        top, low, end = three_parts(jnp.concatenate(pieces, axis=1))
        side = jnp.concatenate(sides, axis=1)
        moved = mm(in_all, jnp.concatenate([top, top, low, low, end, top, side], axis=0), first)
        top, low = hi_lo(sine_of_turns(moved))
        moved = mm(mid_all, jnp.concatenate([top, top, low, ones], axis=0), first)
        top, low = hi_lo(sine_of_turns(moved))
        shaped = mm(out_all, jnp.concatenate([top, top, low], axis=0))
        for piece in range(blocks):
            block = start + piece
            lag = lane + block * SIDE
            part = shaped[:, piece * SIDE : (piece + 1) * SIDE] * jnp.exp(-rate * lag.astype(F32))
            if block == 0:
                part = jnp.where((row >= 4) & (lag == 0), 0.0, part)
            squares += part * part
            rows_ref[block * 8 : (block + 1) * 8, :] = pltpu.roll(part, 4, 0) + part * sign
    total = jnp.sum(squares + pltpu.roll(squares, 4, 0), axis=1, keepdims=True)
    factor = lax.rsqrt(total + 1e-06) * (1.0 / (SIDE * SIDE))
    factor_ref[...] = jnp.broadcast_to(factor, factor_ref.shape)


def spectra_kernel(
    rows_ref, factor_ref, turns_ref, real_ref, right_ref, taps_ref, gain_ref,
    spec_re_ref, spec_im_ref, coef_ref,
):
    device = lax.axis_index("row_0") * lax.axis_size("row_1") + lax.axis_index("row_1")
    device = (device + (HALF - ROOT)) % HALF
    sources = [(tap, taps_ref[tap], 0) for tap in range(3)] + [(3, gain_ref[...], 1)]
    for c in range(2):
        for at, source, shift in sources:
            count = source.shape[0]
            at_lane = lax.broadcasted_iota(jnp.int32, (count, SIDE), 1) == 2 * device + c
            value = jnp.sum(jnp.where(at_lane, source, 0.0), axis=1, keepdims=True)
            value = jnp.broadcast_to(value, (count, SIDE))
            for k in range(count):
                coef_ref[k + shift, at : at + 1, c * SIDE : (c + 1) * SIDE] = value[k : k + 1]
    pieces = []
    for j in range(8):
        pieces.append(rows_ref[pl.ds(j, HALF, stride=8), :] * factor_ref[j : j + 1, :])
    top, low = hi_lo(jnp.concatenate(pieces, axis=1))
    grid = mm(real_ref[:, : 3 * HALF], jnp.concatenate([top, top, low], axis=0))
    cos, sin = turns_ref[:SIDE, :], turns_ref[SIDE:, :]

    def turned(j):
        real = grid[:SIDE, j * SIDE : (j + 1) * SIDE]
        imag = grid[SIDE:, j * SIDE : (j + 1) * SIDE]
        return jnp.concatenate([real * cos + imag * sin, imag * cos - real * sin], axis=1)

    for j in range(4):
        rows = pl.ds(j % 2 * SIDE, SIDE)
        spec_re_ref[j // 2, rows, :] = right_const(
            turned(j), right_ref[: 2 * SIDE, :SIDE], right_ref[2 * SIDE :, :SIDE]
        )
        spec_im_ref[j // 2, rows, :] = right_const(
            turned(j + 4), right_ref[: 2 * SIDE, SIDE:], right_ref[2 * SIDE :, SIDE:]
        )


def conv_kernel(
    x_ref, coef_ref, spec_re_ref, spec_im_ref, turns_ref, right_ref, back_ref, ends_ref,
    o_ref, rows_ref,
):
    for p in range(3):
        for s in range(2):
            piece = x_ref[:, 2 * s : 2 * s + 2, p * SIDE : (p + 1) * SIDE]
            piece = jnp.concatenate([piece[HALF - ROOT :], piece[: HALF - ROOT]], axis=0)
            rows_ref[2 * p + s] = piece.reshape(SIDE, SIDE).astype(F32)
    row = lax.broadcasted_iota(jnp.int32, (HALF, SIDE), 0)
    lane = lax.broadcasted_iota(jnp.int32, (HALF, SIDE), 1)

    def smoothed(p):
        seqs = []
        for s in range(2):
            chans = []
            for c in range(2):
                here = rows_ref[2 * p + s, pl.ds(c, HALF, stride=2), :]
                moved = pltpu.roll(here, 1, 1)
                prev = jnp.where(lane == 0, pltpu.roll(moved, 1, 0), moved)
                prev = jnp.where((lane == 0) & (row == 0), 0.0, prev)
                moved = pltpu.roll(here, SIDE - 1, 1)
                after = jnp.where(lane == SIDE - 1, pltpu.roll(moved, HALF - 1, 0), moved)
                after = jnp.where((lane == SIDE - 1) & (row == HALF - 1), 0.0, after)
                first, second, third = (
                    coef_ref[p, tap : tap + 1, c * SIDE : (c + 1) * SIDE] for tap in range(3)
                )
                chans.append(first * prev + second * here + third * after)
            seqs.append(jnp.concatenate(chans, axis=1))
        return jnp.concatenate(seqs, axis=0)

    cos, sin = turns_ref[:SIDE, :], turns_ref[SIDE:, :]
    cos2, sin2 = jnp.concatenate([cos, cos], axis=1), jnp.concatenate([sin, sin], axis=1)

    def one_order(order, state):
        top, low = hi_lo(state)
        grid = mm(ends_ref[: 2 * SIDE, :], jnp.concatenate([top, top], axis=0))
        grid += mm(ends_ref[: 2 * SIDE, :SIDE], low)
        reals, imags = [], []
        for c in range(2):
            cut = slice(c * SIDE, (c + 1) * SIDE)
            real, imag = grid[:SIDE, cut], grid[SIDE:, cut]
            pair = jnp.concatenate([real * cos + imag * sin, imag * cos - real * sin], axis=1)
            pair = right_const(pair, right_ref[: 2 * SIDE, :], right_ref[2 * SIDE :, :])
            real, imag = pair[:, :SIDE], pair[:, SIDE:]
            k_re, k_im = spec_re_ref[order, cut, :], spec_im_ref[order, cut, :]
            pair = jnp.concatenate([real * k_re - imag * k_im, real * k_im + imag * k_re], axis=1)
            pair = right_const(pair, back_ref[: 2 * SIDE, :], back_ref[2 * SIDE :, :])
            real, imag = pair[:, :SIDE], pair[:, SIDE:]
            reals.append(real * cos - imag * sin)
            imags.append(real * sin + imag * cos)
        grid = jnp.concatenate(
            [jnp.concatenate(reals, axis=1), jnp.concatenate(imags, axis=1)], axis=0
        )
        reach = left_const(ends_ref[2 * SIDE : 3 * SIDE, :], ends_ref[3 * SIDE :, :], grid)
        return smoothed(order + 1) * (reach + coef_ref[order + 1, 3:4, :] * state)

    state = one_order(1, one_order(0, smoothed(0)))
    for s in range(2):
        for c in range(2):
            rows_ref[s, pl.ds(c, HALF, stride=2), :] = state[
                s * HALF : (s + 1) * HALF, c * SIDE : (c + 1) * SIDE
            ]
        piece = rows_ref[s].astype(BF).reshape(HALF, 2, SIDE)
        piece = jnp.concatenate([piece[ROOT:], piece[:ROOT]], axis=0)
        for plane in range(o_ref.shape[0]):
            o_ref[plane, :, :, s * SIDE : (s + 1) * SIDE] = piece


def output_kernel(all_ref, w_ref, o_ref):
    rows = all_ref.shape[0]
    cut = PLANE * (rows // 4)
    first = (((0,), (0,)), ((), ()))
    total = mm(all_ref[: rows - cut, :], w_ref[cut:, :], first)
    total += mm(all_ref[rows - cut :, :], w_ref[:cut, :], first)
    o_ref[...] = total.astype(BF)


def on_device(
    tokens,
    w_value,
    w_first,
    w_second,
    short_taps,
    filter_in,
    filter_mid,
    filter_out,
    decay_rate,
    skip_gain,
    w_output,
):
    seqs, tok_rows, _ = tokens.shape
    blocks = lax.axis_size(ROW)
    length = tok_rows * blocks
    feats = filter_in.shape[0]
    waves, turns, real_all, rights, backs, ends = (jnp.asarray(t) for t in tables(length, feats))
    far = pl.BlockSpec(memory_space=pltpu.HBM)
    vmem = pl.BlockSpec(memory_space=pltpu.VMEM)
    steps = 2
    pieces = pl.pallas_call(
        functools.partial(project_kernel, steps),
        out_shape=jax.ShapeDtypeStruct((blocks, 4, 3 * tok_rows), BF),
        in_specs=[far] * 4,
        out_specs=vmem,
        scratch_shapes=[
            pltpu.VMEM((seqs * tok_rows, tokens.shape[2]), BF),
            pltpu.VMEM((tokens.shape[2], 3 * SIDE), BF),
            pltpu.VMEM((seqs * tok_rows, 3 * SIDE), F32),
            pltpu.SemaphoreType.DMA((steps, 5)),
        ],
        compiler_params=pltpu.CompilerParams(vmem_limit_bytes=66_700_000),
        name="project",
    )(tokens, w_value, w_first, w_second)
    members = [[(i + ROOT) % blocks for i in range(blocks)]]
    arrived = lax.all_to_all(pieces, ROW, 0, 0, tiled=True, axis_index_groups=members)

    spec = jax.ShapeDtypeStruct((2, 2 * SIDE, SIDE), F32)
    units = filter_in.shape[1]
    rows, factor = pl.pallas_call(
        network_kernel,
        out_shape=(
            jax.ShapeDtypeStruct((8 * HALF, SIDE), F32),
            jax.ShapeDtypeStruct((8, SIDE), F32),
        ),
        in_specs=[vmem] * 5,
        out_specs=(vmem, vmem),
        scratch_shapes=[pltpu.VMEM((32, units), F32)],
        compiler_params=pltpu.CompilerParams(vmem_limit_bytes=16 * 2**20),
        cost_estimate=pl.CostEstimate(
            flops=4_000_000_000, bytes_accessed=1_000_000, transcendentals=0
        ),
        name="network",
    )(
        waves,
        filter_in,
        filter_mid,
        filter_out.reshape(4 * units, -1),
        decay_rate.reshape(1, -1),
    )
    spec_re, spec_im, coef = pl.pallas_call(
        spectra_kernel,
        out_shape=(spec, spec, jax.ShapeDtypeStruct((3, 8, 2 * SIDE), F32)),
        in_specs=[vmem] * 7,
        out_specs=(vmem,) * 3,
        compiler_params=pltpu.CompilerParams(vmem_limit_bytes=16 * 2**20),
        cost_estimate=pl.CostEstimate(
            flops=1_000_000_000, bytes_accessed=2_000_000, transcendentals=0
        ),
        name="spectra",
    )(rows, factor, turns, real_all, rights, short_taps, skip_gain)
    planes = lax.axis_size("x")
    gated = pl.pallas_call(
        conv_kernel,
        out_shape=jax.ShapeDtypeStruct((planes, blocks, 2, seqs * tok_rows), BF),
        in_specs=[vmem] * 8,
        out_specs=vmem,
        scratch_shapes=[
            pltpu.VMEM((6, SIDE, SIDE), F32),
        ],
        compiler_params=pltpu.CompilerParams(vmem_limit_bytes=16 * 2**20),
        cost_estimate=pl.CostEstimate(
            flops=4_000_000_000, bytes_accessed=2_000_000, transcendentals=0
        ),
        name="gated_conv",
    )(
        arrived,
        coef,
        spec_re,
        spec_im,
        turns,
        rights,
        backs,
        ends,
    )
    turned = [
        [((i // blocks + PLANE) % planes) * blocks + (i + ROOT) % blocks for i in range(planes * blocks)]
    ]
    everyone = lax.all_to_all(
        gated.reshape(planes * blocks, *gated.shape[2:]),
        ("x", *ROW), 0, 0, tiled=True, axis_index_groups=turned,
    )
    everyone = everyone.reshape(planes, 2 * blocks, seqs * tok_rows)
    everyone = lax.all_gather(everyone, "core", axis=1)
    everyone = everyone.reshape(-1, seqs * tok_rows)
    result = pl.pallas_call(
        output_kernel,
        out_shape=jax.ShapeDtypeStruct((seqs * tok_rows, w_output.shape[1]), BF),
        in_specs=[vmem] * 2,
        out_specs=vmem,
        compiler_params=pltpu.CompilerParams(vmem_limit_bytes=16 * 2**20),
        cost_estimate=pl.CostEstimate(
            flops=134_217_728, bytes_accessed=1_200_000, transcendentals=0
        ),
        name="output_map",
    )(everyone, w_output)
    return result.reshape(seqs, tok_rows, -1)


def solution(mesh):
    torus = Mesh(mesh.devices.reshape(8, 8, 4, 2), ("row_0", "row_1", "x", "core"))
    in_specs = (
        P(None, ROW, None),
        P(None, COL),
        P(None, COL),
        P(None, COL),
        P(None, None, COL),
        P(),
        P(),
        P(None, None, None, COL),
        P(COL),
        P(None, COL),
        P(None, COL),
    )
    out_specs = P(None, ROW, COL)
    return jax.shard_map(
        on_device, mesh=torus, in_specs=in_specs, out_specs=out_specs, check_vma=False
    )
```
